128 devices in a mesh: sp: 32 (over z, y, core), tp: 4 (over x).
Axes of the slice: x: 4, y: 4, z: 4, core: 2. Of those that a mesh axis runs over, the one named last changes fastest.
Arguments:
- tokens: bfloat16 [8192, 4096], P(('sp', 'tp')), may hold values from -700 to 700
- down_query: bfloat16 [4096, 1024], replicated, may hold values from -0.09375 to 0.09375
- down_latent: bfloat16 [4096, 512], replicated, may hold values from -0.09375 to 0.09375
- down_rotary: bfloat16 [4096, 64], replicated, may hold values from -0.09375 to 0.09375
- query_gain: float32 [1024], replicated, may hold values from 0.1 to 1.9
- latent_gain: float32 [512], replicated, may hold values from 0.1 to 1.9
- up_query: bfloat16 [1024, 2048], P(None, 'tp'), may hold values from -0.1875 to 0.1875
- up_query_rotary: bfloat16 [1024, 1024], P(None, 'tp'), may hold values from -0.1875 to 0.1875
- up_key: bfloat16 [512, 2048], P(None, 'tp'), may hold values from -0.25 to 0.25
- up_value: bfloat16 [512, 2048], P(None, 'tp'), may hold values from -0.25 to 0.25
- out_weight: bfloat16 [2048, 4096], P('tp'), may hold values from -0.39648438 to 0.39648438
Outputs:
- mixed: bfloat16 [8192, 4096], P(('sp', 'tp'))
The draws below stay inside these ranges and needn't reach their ends.
All inputs are finite; a program needn't handle non-finite values.
Results may differ from the reference program's by a relative error of at most 0.03.
Values may be sent and summed in bfloat16 or wider, within the bound.
A program may use at most 192 MiB of HBM per device.

```python
import jax
import jax.numpy as jnp
from jax import lax

D = 4096
HEADS = 16
NOPE = 128
ROPE = 64
VDIM = 128
QRANK = 1024
KVRANK = 512
TOK_DEV = 256
TOKENS = 8192
N_TP = 4


def draw_tokens(key, part):
    first_key, second_key, third_key = jax.random.split(jax.random.fold_in(key, 11), 3)
    offsets = jax.random.normal(second_key, (TOKENS // TOK_DEV, D), jnp.float32) * 0.7
    shifted = jnp.repeat(offsets, TOK_DEV, axis=0)
    rough = jax.random.normal(first_key, (TOKENS, D), jnp.float32) + shifted
    return jnp.clip(rough, -700.0, 700.0).astype(jnp.bfloat16)


def shard_levels(stream_key, dims, cuts, smallest, high):
    loudness, own = 1.0, jax.random.fold_in(stream_key, 6)
    for dim, parts in cuts:
        heights = jnp.exp(jax.random.uniform(jax.random.fold_in(own, dim), (parts,), jnp.float32, smallest / len(cuts), high / len(cuts)))
        loudness = loudness * jnp.repeat(heights, dims[dim] // parts).reshape([-1 if axis == dim else 1 for axis in range(len(dims))])
    return loudness


def normal_values(rng, shape, width, bound, pieces=(), held_as=jnp.bfloat16):
    values = jax.random.normal(rng, shape, jnp.float32) * width
    if len(pieces) > 0:
        values = shard_levels(rng, shape, pieces, -0.22, 0.18) * values
    return jnp.clip(values, min=-bound, max=bound).astype(held_as)


def setup_inputs(seed: int = 0) -> dict:
    splits = jax.random.split(jax.random.key(seed), 12)
    tokens = draw_tokens(jax.random.fold_in(splits[11], 71), 0)
    down_query = normal_values(splits[1], (D, QRANK), D ** -0.5, 0.09375)
    down_latent = normal_values(splits[2], (D, KVRANK), D ** -0.5, 0.09375)
    down_rotary = normal_values(splits[3], (D, ROPE), D ** -0.5, 0.09375)
    query_gain = jnp.clip(1.0 + 0.18 * jax.random.normal(splits[4], (QRANK,), jnp.float32), 0.1, 1.9)
    latent_gain = jnp.clip(1.0 + 0.18 * jax.random.normal(splits[5], (KVRANK,), jnp.float32), 0.1, 1.9)
    up_query = normal_values(splits[6], (QRANK, HEADS * NOPE), QRANK ** -0.5, 0.1875, ((1, 4),))
    up_query_rotary = normal_values(splits[7], (QRANK, HEADS * ROPE), QRANK ** -0.5, 0.1875, ((1, 4),))
    up_key = normal_values(splits[8], (KVRANK, HEADS * NOPE), KVRANK ** -0.5, 0.25, ((1, 4),))
    up_value = normal_values(splits[9], (KVRANK, HEADS * VDIM), KVRANK ** -0.5, 0.25, ((1, 4),))
    out_weight = normal_values(splits[10], (HEADS * VDIM, D), (3.0 * (HEADS * VDIM) ** -0.5), 0.39648438, ((0, 4),))
    return dict(tokens=tokens, down_query=down_query, down_latent=down_latent, down_rotary=down_rotary, query_gain=query_gain, latent_gain=latent_gain, up_query=up_query, up_query_rotary=up_query_rotary, up_key=up_key, up_value=up_value, out_weight=out_weight)


rope_base = 500000.0
norm_eps = 1e-06
masked_score = -1e+30

def rotate_half(values, positions):
    half = values.shape[-1] // 2
    inverse = rope_base ** (-jnp.arange(0, 2 * half, 2, dtype=jnp.float32) / (2 * half))
    angles = positions.astype(jnp.float32)[:, None] * inverse
    if values.ndim == 3:
        angles = angles[:, None, :]
    cosine = jnp.cos(angles)
    sine = jnp.sin(angles)
    first = values[..., :half]
    second = values[..., half:]
    return jnp.concatenate([first * cosine - second * sine, second * cosine + first * sine], axis=-1)

def norm_rows(values, gain):
    return values * lax.rsqrt(lax.optimization_barrier(jnp.mean(values * values, axis=-1, keepdims=True)) + norm_eps) * gain

def reference(tokens, down_query, down_latent, down_rotary, query_gain, latent_gain, up_query, up_query_rotary, up_key, up_value, out_weight):
    positions = jnp.arange(TOKENS, dtype=jnp.int32)
    query_latent = norm_rows(jnp.dot(tokens, down_query, preferred_element_type=jnp.float32), query_gain).astype(jnp.bfloat16)
    kv_latent = norm_rows(jnp.dot(tokens, down_latent, preferred_element_type=jnp.float32), latent_gain).astype(jnp.bfloat16)
    key_rotary = rotate_half(jnp.dot(tokens, down_rotary, preferred_element_type=jnp.float32), positions).astype(jnp.bfloat16)
    query_plain = jnp.dot(query_latent, up_query, preferred_element_type=jnp.float32).astype(jnp.bfloat16).reshape(TOKENS, HEADS, NOPE)
    query_turned = rotate_half(jnp.dot(query_latent, up_query_rotary, preferred_element_type=jnp.float32).reshape(TOKENS, HEADS, ROPE), positions).astype(jnp.bfloat16)
    key_plain = jnp.dot(kv_latent, up_key, preferred_element_type=jnp.float32).astype(jnp.bfloat16).reshape(TOKENS, HEADS, NOPE)
    values = jnp.dot(kv_latent, up_value, preferred_element_type=jnp.float32).astype(jnp.bfloat16).reshape(TOKENS, HEADS, VDIM)
    factor = (NOPE + ROPE) ** (-0.5)
    block = 512 if TOKENS % 512 == 0 else TOKENS
    outputs = []
    for first in range(0, TOKENS, block):
        stop = first + block
        scores = jnp.einsum('qhd,khd->hqk', query_plain[first:stop].astype(jnp.float32), key_plain[:stop].astype(jnp.float32))
        scores = scores + jnp.einsum('qhr,kr->hqk', query_turned[first:stop].astype(jnp.float32), key_rotary[:stop].astype(jnp.float32))
        scores = scores * factor
        allowed = (positions[:stop][None, :] <= positions[first:stop][:, None])[None]
        scores = jnp.where(allowed, scores, masked_score)
        best = lax.optimization_barrier(jnp.max(scores, axis=-1, keepdims=True))
        weights = jnp.where(allowed, jnp.exp(scores - best), 0.0)
        total = lax.optimization_barrier(jnp.sum(weights, axis=-1))
        rounded = lax.optimization_barrier(weights.astype(jnp.bfloat16)).astype(jnp.float32)
        summed = jnp.einsum('hqk,khd->qhd', rounded, values[:stop].astype(jnp.float32))
        outputs.append((summed / jnp.transpose(total)[:, :, None]).astype(jnp.bfloat16).reshape(block, HEADS * VDIM))
    attended = jnp.concatenate(outputs, axis=0)
    group_width = HEADS * VDIM // N_TP
    mixed = jnp.zeros((TOKENS, D), jnp.float32)
    for group in range(N_TP):
        lower = group * group_width
        partial_sum = jnp.dot(attended[:, lower:lower + group_width], out_weight[lower:lower + group_width], preferred_element_type=jnp.float32)
        mixed = mixed + lax.optimization_barrier(partial_sum.astype(jnp.bfloat16)).astype(jnp.float32)
    return mixed.astype(jnp.bfloat16)
```

```python
import functools

import jax
import jax.numpy as jnp
from jax import lax
from jax.experimental import pallas as pl
from jax.experimental.pallas import tpu as pltpu
from jax.sharding import PartitionSpec as P

NOPE = 128
ROPE = 64
VDIM = 128
HEADS = 4
OWN = 64
GROUP = 256
BLOCK = 288
VROWS = 144
RING = 4

rope_base = 500000.0
norm_eps = 1e-06
masked_score = -1e30

f32 = jnp.float32
bf16 = jnp.bfloat16
MESH = pl.DeviceIdType.MESH

X_MSG, A_MSG, B_MSG, Q_MSG, QX_MSG, OX_MSG, R_MSG = 0, 4, 8, 24, 28, 29, 30
COLS = 4
N_MSG = R_MSG + 6 * COLS

UNIT_OA = ((0, 0, -1, 1, -1, 2, 0, -1), (1, 0, 2, 1, -1, 2, 1, 2))
UNIT_OB = ((0, 1, 0, 1, 1, 1, 2, 2), (0, -1, 0, -1, -1, -1, 2, 2))


def pick(index, values):
    out = jnp.int32(values[0])
    for i, v in enumerate(values[1:], 1):
        out = jnp.where(index == i, jnp.int32(v), out)
    return out


def mod4(v):
    return lax.rem(v + 8, 4)


def kernel(
    tokens,
    down_query,
    down_latent,
    down_rotary,
    query_gain,
    latent_gain,
    up_query,
    up_query_rotary,
    up_key,
    up_value,
    out_weight,
    key_cos,
    key_sin,
    query_cos,
    query_sin,
    out,
    wdl,
    wdr,
    wdq,
    wuq,
    wur,
    wuk,
    wuv,
    wout,
    lat,
    ql,
    qt,
    uvt,
    kbuf,
    vbuf,
    acc,
    best,
    xsend,
    xrecv,
    pbuf,
    r1buf,
    dbuf,
    cbuf,
    crecv,
    local_sem,
    ssem,
    rsem,
):
    sp = lax.axis_index("sp")
    x = lax.axis_index("tp")
    c = lax.rem(sp, 2)
    m = sp // 2
    y = lax.rem(m, 4)
    z = m // 4
    first = c == 0
    a = jnp.where(first, y, z)
    b = jnp.where(first, z, y)
    stride_a = jnp.where(first, 2, 8)
    stride_b = jnp.where(first, 8, 2)

    def at(aa, bb):
        return {"sp": aa * stride_a + bb * stride_b + c, "tp": x}

    xp, xm, x2 = mod4(x + 1), mod4(x - 1), mod4(x + 2)
    dev_xp = {"sp": sp, "tp": xp}
    dev_xm = {"sp": sp, "tp": xm}
    dev_ap, dev_am = at(mod4(a + 1), b), at(mod4(a - 1), b)
    dev_bp, dev_bm = at(a, mod4(b + 1)), at(a, mod4(b - 1))
    dev_core = {"sp": sp + 1 - 2 * c, "tp": x}

    def copy_in(i, src, dst):
        return pltpu.make_async_copy(src, dst, local_sem.at[i])

    K4 = 1024
    loads = []
    for k in range(4):
        rows = pl.ds(k * K4, K4)
        loads.append(copy_in(k, down_latent.at[rows], wdl.at[rows]))
    loads.append(copy_in(4, down_rotary, wdr))
    for k in range(4):
        rows = pl.ds(k * K4, K4)
        loads.append(copy_in(5 + k, down_query.at[rows], wdq.at[rows]))
    loads.append(copy_in(9, up_query, wuq))
    loads.append(copy_in(10, up_query_rotary, wur))
    loads.append(copy_in(11, up_key, wuk))
    loads.append(copy_in(12, up_value, wuv))
    loads.append(copy_in(13, out_weight, wout))
    for load in loads:
        load.start()

    barrier = pltpu.get_barrier_semaphore()
    for dev in (dev_xp, dev_xm, dev_ap, dev_am, dev_bp, dev_bm, dev_core):
        pl.semaphore_signal(barrier, inc=1, device_id=dev, device_id_type=MESH)

    def rcopy(i, src, dst, dev):
        return pltpu.make_async_remote_copy(
            src_ref=src,
            dst_ref=dst,
            send_sem=ssem.at[i],
            recv_sem=rsem.at[i],
            device_id=dev,
            device_id_type=MESH,
        )

    def same(i, ref, dev):
        return rcopy(i, ref, ref, dev)

    def group(aa, bb):
        return mod4(bb) * 4 + mod4(aa)

    s0 = group(a, b)
    lo, hi = pl.ds(0, BLOCK // 2), pl.ds(BLOCK // 2, BLOCK // 2)
    xs_lo, xs_hi = pl.ds(0, 2), pl.ds(2, 2)

    send = {}
    recv = {}

    def both(i, sent, received, dev):
        send[i] = same(i, sent, dev)
        recv[i] = same(i, received, dev)

    both(X_MSG, lat.at[s0, x], lat.at[s0, xm], dev_xp)
    both(X_MSG + 1, lat.at[s0, x], lat.at[s0, xp], dev_xm)
    both(X_MSG + 2, lat.at[s0, xm, lo], lat.at[s0, x2, lo], dev_xp)
    both(X_MSG + 3, lat.at[s0, xp, hi], lat.at[s0, x2, hi], dev_xm)
    both(A_MSG, lat.at[s0], lat.at[group(a - 1, b)], dev_ap)
    both(A_MSG + 1, lat.at[s0], lat.at[group(a + 1, b)], dev_am)
    both(A_MSG + 2, lat.at[group(a - 1, b), xs_lo], lat.at[group(a + 2, b), xs_lo], dev_ap)
    both(A_MSG + 3, lat.at[group(a + 1, b), xs_hi], lat.at[group(a + 2, b), xs_hi], dev_am)
    for k, o in enumerate((0, 1, -1, 2)):
        i = B_MSG + 4 * k
        own, lower, upper, far = (group(a + o, b + d) for d in (0, -1, 1, 2))
        both(i, lat.at[own], lat.at[lower], dev_bp)
        both(i + 1, lat.at[own], lat.at[upper], dev_bm)
        both(i + 2, lat.at[lower, xs_lo], lat.at[far, xs_lo], dev_bp)
        both(i + 3, lat.at[upper, xs_hi], lat.at[far, xs_hi], dev_bm)
    q_lo, q_hi = pl.ds(0, OWN // 2), pl.ds(OWN // 2, OWN // 2)
    both(Q_MSG, ql.at[x], ql.at[xm], dev_xp)
    both(Q_MSG + 1, ql.at[x], ql.at[xp], dev_xm)
    both(Q_MSG + 2, ql.at[xm, q_lo], ql.at[x2, q_lo], dev_xp)
    both(Q_MSG + 3, ql.at[xp, q_hi], ql.at[x2, q_hi], dev_xm)
    send[QX_MSG] = same(QX_MSG, qt.at[c], dev_core)
    recv[QX_MSG] = same(QX_MSG, qt.at[1 - c], dev_core)
    send[OX_MSG] = rcopy(OX_MSG, xsend, xrecv, dev_core)
    recv[OX_MSG] = send[OX_MSG]

    def start(*ids):
        for i in ids:
            send[i].start()

    def arrived(*ids):
        for i in ids:
            recv[i].wait_recv()

    def norm_rows(values, gain):
        return values * lax.rsqrt(jnp.mean(values * values, axis=-1, keepdims=True) + norm_eps) * gain

    latent = jnp.zeros((OWN, 512), f32)
    for k in range(4):
        loads[k].wait()
        cols = slice(k * K4, (k + 1) * K4)
        latent = latent + jnp.dot(tokens[:, cols], wdl[cols, :], preferred_element_type=f32)
    latent = norm_rows(latent, latent_gain[...]).astype(bf16)
    for t in range(4):
        lat[s0, x, t * OWN : (t + 1) * OWN, :] = latent[:, t * 128 : (t + 1) * 128]
    loads[4].wait()
    turned = jnp.dot(tokens[...], wdr[...], preferred_element_type=f32)
    turned = jnp.concatenate([turned, turned], axis=-1)
    turned = turned * key_cos[...] + pltpu.roll(turned, 32, 1) * key_sin[...]
    lane = lax.broadcasted_iota(jnp.int32, (32, 128), 1)
    lat[s0, x, 256:288, :] = jnp.where(lane < 64, turned[:32], turned[32:]).astype(bf16)

    pl.semaphore_wait(barrier, 7)
    start(X_MSG, X_MSG + 1)

    query = jnp.zeros((OWN, 1024), f32)
    for k in range(4):
        loads[5 + k].wait()
        cols = slice(k * K4, (k + 1) * K4)
        query = query + jnp.dot(tokens[:, cols], wdq[cols, :], preferred_element_type=f32)
    ql[x] = norm_rows(query, query_gain[...]).astype(bf16)

    arrived(X_MSG, X_MSG + 1)
    start(X_MSG + 2, X_MSG + 3, Q_MSG, Q_MSG + 1)
    for i in range(9, 14):
        loads[i].wait()
    uvt[...] = jnp.transpose(wuv[...].astype(f32)).astype(bf16)
    for h in range(HEADS):
        vbuf[h, VDIM:VROWS, :] = jnp.ones((VROWS - VDIM, 2 * GROUP), bf16)
    acc[...] = jnp.zeros_like(acc)
    best[...] = jnp.full(best.shape, masked_score, f32)
    arrived(X_MSG + 2, X_MSG + 3)
    start(A_MSG, A_MSG + 1, B_MSG, B_MSG + 1)
    arrived(Q_MSG, Q_MSG + 1)
    start(Q_MSG + 2, Q_MSG + 3)
    arrived(Q_MSG + 2, Q_MSG + 3)

    factor = (NOPE + ROPE) ** (-0.5) * 1.4426950408889634
    rows = ql[...].reshape(GROUP, 1024)
    plain = jnp.dot(rows, wuq[...], preferred_element_type=f32) * factor
    qt[c, 0 : HEADS * NOPE, :] = jnp.transpose(plain).astype(bf16)
    turned = jnp.transpose(jnp.dot(rows, wur[...], preferred_element_type=f32) * factor)
    cosine, sine = query_cos[...], query_sin[...]
    for h in range(HEADS):
        one = turned[h * ROPE : h * ROPE + 32]
        two = turned[h * ROPE + 32 : (h + 1) * ROPE]
        at_row = HEADS * NOPE + h * ROPE
        qt[c, at_row : at_row + 32, :] = (one * cosine - two * sine).astype(bf16)
        qt[c, at_row + 32 : at_row + 64, :] = (two * cosine + one * sine).astype(bf16)
    start(QX_MSG)
    arrived(QX_MSG)

    UNIT = 2 * GROUP

    def attend(set_one, set_two, m_one, m_two, masked):
        parts, rots = [], []
        for s in (set_one, set_two):
            tiles = [
                lat[s, :, t * OWN : (t + 1) * OWN, :].reshape(GROUP, 128) for t in range(4)
            ]
            parts.append(jnp.concatenate(tiles, axis=1))
            packed = lat[s, :, 256:288, :]
            swapped = pltpu.roll(packed.reshape(128, 128).astype(f32), 64, 1).astype(bf16)
            rots.append(
                jnp.concatenate([packed, swapped.reshape(4, 32, 128)], axis=1).reshape(GROUP, 128)
            )
        latents = jnp.concatenate(parts, axis=0)
        keys = jnp.dot(latents, wuk[...], preferred_element_type=f32).astype(bf16)
        for h in range(HEADS):
            kbuf[h, :, 0:NOPE] = keys[:, h * NOPE : (h + 1) * NOPE]
            kbuf[h, :, NOPE:256] = jnp.concatenate(rots, axis=0)
        values = lax.dot_general(
            uvt[...], latents, (((1,), (1,)), ((), ())), preferred_element_type=f32
        ).astype(bf16)
        for h in range(HEADS):
            vbuf[h, 0:VDIM, :] = values[h * VDIM : (h + 1) * VDIM]

        def head(h, carry):
            key = kbuf[h]
            value = vbuf[h]
            for j in range(2):
                at_plain = pl.multiple_of(h * NOPE, NOPE)
                at_turned = pl.multiple_of(HEADS * NOPE + h * ROPE, ROPE)
                queries = jnp.concatenate(
                    [
                        qt[j, pl.ds(at_plain, NOPE), :],
                        qt[j, pl.ds(at_turned, ROPE), :],
                        jnp.zeros((ROPE, GROUP), bf16),
                    ],
                    axis=0,
                )
                scores = jnp.dot(key, queries, preferred_element_type=f32)
                if masked:
                    row = lax.broadcasted_iota(jnp.int32, (UNIT, GROUP), 0)
                    col = lax.broadcasted_iota(jnp.int32, (UNIT, GROUP), 1)
                    base_one = (2 * m_one + c) * GROUP
                    base_two = (2 * m_two + c) * GROUP - GROUP
                    place = row + jnp.where(row < GROUP, base_one, base_two)
                    scores = jnp.where(
                        place <= col + (2 * m + j) * GROUP, scores, masked_score
                    )
                old = best[j, h]
                new = jnp.maximum(old, jnp.max(scores, axis=0, keepdims=True))
                weights = jnp.exp2(scores - new).astype(bf16)
                best[j, h] = new
                acc[j, h] = acc[j, h] * jnp.exp2(old - new) + jnp.dot(
                    value, weights, preferred_element_type=f32
                )
            return carry

        lax.fori_loop(0, HEADS, head, 0)

    def unit(u, carry):
        @pl.when(u == 0)
        def _():
            arrived(A_MSG, A_MSG + 1)
            start(A_MSG + 2, A_MSG + 3)
            start(B_MSG + 4, B_MSG + 5, B_MSG + 8, B_MSG + 9)

        @pl.when(u == 1)
        def _():
            arrived(B_MSG, B_MSG + 1)
            start(B_MSG + 2, B_MSG + 3)

        @pl.when(u == 2)
        def _():
            arrived(A_MSG + 2, A_MSG + 3)
            start(B_MSG + 12, B_MSG + 13)

        for k in (1, 2, 3):

            @pl.when(u == 2 + k)
            def _(k=k):
                arrived(B_MSG + 4 * k, B_MSG + 4 * k + 1)
                start(B_MSG + 4 * k + 2, B_MSG + 4 * k + 3)

        @pl.when(u == 6)
        def _():
            arrived(B_MSG + 2, B_MSG + 3, B_MSG + 6, B_MSG + 7)

        @pl.when(u == 7)
        def _():
            arrived(B_MSG + 10, B_MSG + 11, B_MSG + 14, B_MSG + 15)

        sets, spots = [], []
        for n in range(2):
            aa = mod4(a + pick(u, UNIT_OA[n]))
            bb = mod4(b + pick(u, UNIT_OB[n]))
            sets.append(bb * 4 + aa)
            spots.append(jnp.where(first, bb * 4 + aa, aa * 4 + bb))
        plain_unit = jnp.logical_and(spots[0] < m, spots[1] < m)
        some = jnp.logical_or(spots[0] <= m, spots[1] <= m)

        @pl.when(plain_unit)
        def _():
            attend(*sets, *spots, False)

        @pl.when(jnp.logical_and(some, jnp.logical_not(plain_unit)))
        def _():
            attend(*sets, *spots, True)

        return carry

    lax.fori_loop(0, 8, unit, 0)

    other = 1 - c
    for h in range(HEADS):
        xsend[h, 0:136, :] = acc[other, h, 0:136, :]
        xsend[h, 136:144, :] = jnp.broadcast_to(best[other, h], (8, GROUP))
    start(OX_MSG)
    arrived(OX_MSG)
    heads = []
    for h in range(HEADS):
        mine, theirs = best[c, h], xrecv[h, 136:137, :]
        top = jnp.maximum(mine, theirs)
        w_mine, w_theirs = jnp.exp2(mine - top), jnp.exp2(theirs - top)
        total = acc[c, h, 128:129, :] * w_mine + xrecv[h, 128:129, :] * w_theirs
        summed = acc[c, h, 0:128, :] * w_mine + xrecv[h, 0:128, :] * w_theirs
        heads.append(jnp.transpose(summed / total).astype(bf16))
    attended = jnp.concatenate(heads, axis=1)

    WIDE = 4096 // COLS
    top, low = pl.ds(0, 32), pl.ds(32, 32)
    for k in range(COLS):
        cols = pl.ds(k * WIDE, WIDE)
        i = R_MSG + 6 * k
        send[i] = rcopy(i, pbuf.at[x2, top, cols], r1buf.at[0, :, cols], dev_xp)
        send[i + 1] = rcopy(i + 1, pbuf.at[x2, low, cols], r1buf.at[1, :, cols], dev_xm)
        send[i + 2] = rcopy(i + 2, pbuf.at[xp, low, cols], dbuf.at[0, :, cols], dev_xp)
        send[i + 3] = rcopy(i + 3, pbuf.at[xm, top, cols], dbuf.at[1, :, cols], dev_xm)
        send[i + 4] = rcopy(i + 4, cbuf.at[0, :, cols], crecv.at[0, :, cols], dev_xp)
        send[i + 5] = rcopy(i + 5, cbuf.at[1, :, cols], crecv.at[1, :, cols], dev_xm)
        for n in range(6):
            recv[i + n] = send[i + n]
    for k in range(COLS):
        cols = slice(k * WIDE, (k + 1) * WIDE)
        part = jnp.dot(attended, wout[:, cols], preferred_element_type=f32).astype(bf16)
        pbuf[:, :, cols] = part.reshape(4, OWN, WIDE)
        start(R_MSG + 6 * k, R_MSG + 6 * k + 1)
    for k in range(COLS):
        start(R_MSG + 6 * k + 2, R_MSG + 6 * k + 3)
    for k in range(COLS):
        cols = slice(k * WIDE, (k + 1) * WIDE)
        i = R_MSG + 6 * k
        arrived(i, i + 1)
        cbuf[0, :, cols] = (
            r1buf[0, :, cols].astype(f32) + pbuf[xp, 0:32, cols].astype(f32)
        ).astype(bf16)
        cbuf[1, :, cols] = (
            r1buf[1, :, cols].astype(f32) + pbuf[xm, 32:64, cols].astype(f32)
        ).astype(bf16)
        start(i + 4, i + 5)
    for k in range(COLS):
        cols = slice(k * WIDE, (k + 1) * WIDE)
        i = R_MSG + 6 * k
        arrived(i + 2, i + 3, i + 4, i + 5)
        out[0:32, cols] = (
            pbuf[x, 0:32, cols].astype(f32)
            + crecv[0, :, cols].astype(f32)
            + dbuf[1, :, cols].astype(f32)
        ).astype(bf16)
        out[32:64, cols] = (
            pbuf[x, 32:64, cols].astype(f32)
            + crecv[1, :, cols].astype(f32)
            + dbuf[0, :, cols].astype(f32)
        ).astype(bf16)
    for i in range(N_MSG):
        send[i].wait_send()


def local(
    tokens,
    down_query,
    down_latent,
    down_rotary,
    query_gain,
    latent_gain,
    up_query,
    up_query_rotary,
    up_key,
    up_value,
    out_weight,
):
    sp = lax.axis_index("sp")
    x = lax.axis_index("tp")
    inverse = rope_base ** (-jnp.arange(0, ROPE, 2, dtype=f32) / ROPE)
    own = ((sp * RING + x) * OWN + jnp.arange(OWN, dtype=jnp.int32)).astype(f32)
    angles = own[:, None] * jnp.tile(inverse, 4)[None, :]
    sign = jnp.tile(jnp.repeat(jnp.array([-1.0, 1.0], f32), 32), 2)
    key_cos, key_sin = jnp.cos(angles), jnp.sin(angles) * sign[None, :]
    span = (sp * GROUP + jnp.arange(GROUP, dtype=jnp.int32)).astype(f32)
    angles = inverse[:, None] * span[None, :]
    query_cos, query_sin = jnp.cos(angles), jnp.sin(angles)

    vmem = pl.BlockSpec(memory_space=pltpu.VMEM)
    hbm = pl.BlockSpec(memory_space=pl.ANY)
    return pl.pallas_call(
        kernel,
        out_shape=jax.ShapeDtypeStruct((OWN, 4096), bf16),
        in_specs=[vmem, hbm, hbm, hbm, vmem, vmem, hbm, hbm, hbm, hbm, hbm, vmem, vmem, vmem, vmem],
        out_specs=vmem,
        scratch_shapes=[
            pltpu.VMEM((4096, 512), bf16),
            pltpu.VMEM((4096, 64), bf16),
            pltpu.VMEM((4096, 1024), bf16),
            pltpu.VMEM((1024, 512), bf16),
            pltpu.VMEM((1024, 256), bf16),
            pltpu.VMEM((512, 512), bf16),
            pltpu.VMEM((512, 512), bf16),
            pltpu.VMEM((512, 4096), bf16),
            pltpu.VMEM((16, 4, BLOCK, 128), bf16),
            pltpu.VMEM((4, OWN, 1024), bf16),
            pltpu.VMEM((2, HEADS * (NOPE + ROPE), GROUP), bf16),
            pltpu.VMEM((512, 512), bf16),
            pltpu.VMEM((HEADS, 2 * GROUP, 256), bf16),
            pltpu.VMEM((HEADS, VROWS, 2 * GROUP), bf16),
            pltpu.VMEM((2, HEADS, VROWS, GROUP), f32),
            pltpu.VMEM((2, HEADS, 1, GROUP), f32),
            pltpu.VMEM((HEADS, VROWS, GROUP), f32),
            pltpu.VMEM((HEADS, VROWS, GROUP), f32),
            pltpu.VMEM((4, OWN, 4096), bf16),
            pltpu.VMEM((2, 32, 4096), bf16),
            pltpu.VMEM((2, 32, 4096), bf16),
            pltpu.VMEM((2, 32, 4096), bf16),
            pltpu.VMEM((2, 32, 4096), bf16),
            pltpu.SemaphoreType.DMA((14,)),
            pltpu.SemaphoreType.DMA((N_MSG,)),
            pltpu.SemaphoreType.DMA((N_MSG,)),
        ],
        compiler_params=pltpu.CompilerParams(
            collective_id=0, has_side_effects=True, vmem_limit_bytes=62 * 1024 * 1024
        ),
    )(
        tokens,
        down_query,
        down_latent,
        down_rotary,
        query_gain.reshape(1, -1),
        latent_gain.reshape(1, -1),
        up_query,
        up_query_rotary,
        up_key,
        up_value,
        out_weight,
        key_cos,
        key_sin,
        query_cos,
        query_sin,
    )


def solution(mesh):
    return jax.shard_map(
        local,
        mesh=mesh,
        in_specs=(
            P(("sp", "tp"), None),
            P(),
            P(),
            P(),
            P(),
            P(),
            P(None, "tp"),
            P(None, "tp"),
            P(None, "tp"),
            P(None, "tp"),
            P("tp", None),
        ),
        out_specs=P(("sp", "tp"), None),
        check_vma=False,
    )
```

```python
import functools

import jax
import jax.numpy as jnp
from jax import lax
from jax.experimental import pallas as pl
from jax.experimental.pallas import tpu as pltpu
from jax.sharding import PartitionSpec as P

NOPE = 128
ROPE = 64
VDIM = 128
HEADS = 4
OWN = 64
GROUP = 256
BLOCK = 288
VROWS = 144
RING = 4

rope_base = 500000.0
norm_eps = 1e-06
masked_score = -1e30

f32 = jnp.float32
bf16 = jnp.bfloat16
MESH = pl.DeviceIdType.MESH

X_MSG, A_MSG, B_MSG, Q_MSG, QX_MSG, OX_MSG, R_MSG = 0, 4, 8, 24, 28, 29, 30
COLS = 4
N_MSG = R_MSG + 6 * COLS

UNIT_OA = ((0, 0, -1, 1, -1, 2, 0, -1), (1, 0, 2, 1, -1, 2, 1, 2))
UNIT_OB = ((0, 1, 0, 1, 1, 1, 2, 2), (0, -1, 0, -1, -1, -1, 2, 2))


def pick(index, values):
    out = jnp.int32(values[0])
    for i, v in enumerate(values[1:], 1):
        out = jnp.where(index == i, jnp.int32(v), out)
    return out


def mod4(v):
    return lax.rem(v + 8, 4)


def kernel(
    tokens,
    down_query,
    down_latent,
    down_rotary,
    query_gain,
    latent_gain,
    up_query,
    up_query_rotary,
    up_key,
    up_value,
    out_weight,
    key_cos,
    key_sin,
    query_cos,
    query_sin,
    out,
    wdl,
    wdr,
    wdq,
    wuq,
    wur,
    wuk,
    wuv,
    wout,
    lat,
    ql,
    qt,
    uvt,
    kbuf,
    vbuf,
    acc,
    best,
    qfull,
    sbuf,
    tops,
    xsend,
    xrecv,
    pbuf,
    r1buf,
    dbuf,
    cbuf,
    crecv,
    local_sem,
    ssem,
    rsem,
):
    sp = lax.axis_index("sp")
    x = lax.axis_index("tp")
    c = lax.rem(sp, 2)
    m = sp // 2
    y = lax.rem(m, 4)
    z = m // 4
    first = c == 0
    a = jnp.where(first, y, z)
    b = jnp.where(first, z, y)
    stride_a = jnp.where(first, 2, 8)
    stride_b = jnp.where(first, 8, 2)

    def at(aa, bb):
        return {"sp": aa * stride_a + bb * stride_b + c, "tp": x}

    xp, xm, x2 = mod4(x + 1), mod4(x - 1), mod4(x + 2)
    dev_xp = {"sp": sp, "tp": xp}
    dev_xm = {"sp": sp, "tp": xm}
    dev_ap, dev_am = at(mod4(a + 1), b), at(mod4(a - 1), b)
    dev_bp, dev_bm = at(a, mod4(b + 1)), at(a, mod4(b - 1))
    dev_core = {"sp": sp + 1 - 2 * c, "tp": x}

    def copy_in(i, src, dst):
        return pltpu.make_async_copy(src, dst, local_sem.at[i])

    K4 = 1024
    loads = []
    for k in range(4):
        rows = pl.ds(k * K4, K4)
        loads.append(copy_in(k, down_latent.at[rows], wdl.at[rows]))
    loads.append(copy_in(4, down_rotary, wdr))
    for k in range(4):
        rows = pl.ds(k * K4, K4)
        loads.append(copy_in(5 + k, down_query.at[rows], wdq.at[rows]))
    loads.append(copy_in(9, up_query, wuq))
    loads.append(copy_in(10, up_query_rotary, wur))
    loads.append(copy_in(11, up_key, wuk))
    loads.append(copy_in(12, up_value, wuv))
    loads.append(copy_in(13, out_weight, wout))
    for load in loads:
        load.start()

    barrier = pltpu.get_barrier_semaphore()
    for dev in (dev_xp, dev_xm, dev_ap, dev_am, dev_bp, dev_bm, dev_core):
        pl.semaphore_signal(barrier, inc=1, device_id=dev, device_id_type=MESH)

    def rcopy(i, src, dst, dev):
        return pltpu.make_async_remote_copy(
            src_ref=src,
            dst_ref=dst,
            send_sem=ssem.at[i],
            recv_sem=rsem.at[i],
            device_id=dev,
            device_id_type=MESH,
        )

    def same(i, ref, dev):
        return rcopy(i, ref, ref, dev)

    def group(aa, bb):
        return mod4(bb) * 4 + mod4(aa)

    s0 = group(a, b)
    lo, hi = pl.ds(0, BLOCK // 2), pl.ds(BLOCK // 2, BLOCK // 2)
    xs_lo, xs_hi = pl.ds(0, 2), pl.ds(2, 2)

    send = {}
    recv = {}

    def both(i, sent, received, dev):
        send[i] = same(i, sent, dev)
        recv[i] = same(i, received, dev)

    both(X_MSG, lat.at[s0, x], lat.at[s0, xm], dev_xp)
    both(X_MSG + 1, lat.at[s0, x], lat.at[s0, xp], dev_xm)
    both(X_MSG + 2, lat.at[s0, xm, lo], lat.at[s0, x2, lo], dev_xp)
    both(X_MSG + 3, lat.at[s0, xp, hi], lat.at[s0, x2, hi], dev_xm)
    both(A_MSG, lat.at[s0], lat.at[group(a - 1, b)], dev_ap)
    both(A_MSG + 1, lat.at[s0], lat.at[group(a + 1, b)], dev_am)
    both(A_MSG + 2, lat.at[group(a - 1, b), xs_lo], lat.at[group(a + 2, b), xs_lo], dev_ap)
    both(A_MSG + 3, lat.at[group(a + 1, b), xs_hi], lat.at[group(a + 2, b), xs_hi], dev_am)
    for k, o in enumerate((0, 1, -1, 2)):
        i = B_MSG + 4 * k
        own, lower, upper, far = (group(a + o, b + d) for d in (0, -1, 1, 2))
        both(i, lat.at[own], lat.at[lower], dev_bp)
        both(i + 1, lat.at[own], lat.at[upper], dev_bm)
        both(i + 2, lat.at[lower, xs_lo], lat.at[far, xs_lo], dev_bp)
        both(i + 3, lat.at[upper, xs_hi], lat.at[far, xs_hi], dev_bm)
    q_lo, q_hi = pl.ds(0, OWN // 2), pl.ds(OWN // 2, OWN // 2)
    both(Q_MSG, ql.at[x], ql.at[xm], dev_xp)
    both(Q_MSG + 1, ql.at[x], ql.at[xp], dev_xm)
    both(Q_MSG + 2, ql.at[xm, q_lo], ql.at[x2, q_lo], dev_xp)
    both(Q_MSG + 3, ql.at[xp, q_hi], ql.at[x2, q_hi], dev_xm)
    send[QX_MSG] = same(QX_MSG, qt.at[c], dev_core)
    recv[QX_MSG] = same(QX_MSG, qt.at[1 - c], dev_core)
    send[OX_MSG] = rcopy(OX_MSG, xsend, xrecv, dev_core)
    recv[OX_MSG] = send[OX_MSG]

    def start(*ids):
        for i in ids:
            send[i].start()

    def arrived(*ids):
        for i in ids:
            recv[i].wait_recv()

    def norm_rows(values, gain):
        return values * lax.rsqrt(jnp.mean(values * values, axis=-1, keepdims=True) + norm_eps) * gain

    latent = jnp.zeros((OWN, 512), f32)
    for k in range(4):
        loads[k].wait()
        cols = slice(k * K4, (k + 1) * K4)
        latent = latent + jnp.dot(tokens[:, cols], wdl[cols, :], preferred_element_type=f32)
    latent = norm_rows(latent, latent_gain[...]).astype(bf16)
    for t in range(4):
        lat[s0, x, t * OWN : (t + 1) * OWN, :] = latent[:, t * 128 : (t + 1) * 128]
    loads[4].wait()
    turned = lax.dot_general(
        tokens[...], wdr[...], (((1,), (1,)), ((), ())), preferred_element_type=f32
    )
    turned = jnp.concatenate([turned, turned], axis=-1)
    turned = turned * key_cos[...] + pltpu.roll(turned, 32, 1) * key_sin[...]
    lane = lax.broadcasted_iota(jnp.int32, (32, 128), 1)
    lat[s0, x, 256:288, :] = jnp.where(lane < 64, turned[:32], turned[32:]).astype(bf16)

    pl.semaphore_wait(barrier, 7)
    start(X_MSG, X_MSG + 1)

    query = jnp.zeros((OWN, 1024), f32)
    for k in range(4):
        loads[5 + k].wait()
        cols = slice(k * K4, (k + 1) * K4)
        query = query + jnp.dot(tokens[:, cols], wdq[cols, :], preferred_element_type=f32)
    ql[x] = norm_rows(query, query_gain[...]).astype(bf16)

    arrived(X_MSG, X_MSG + 1)
    start(X_MSG + 2, X_MSG + 3, Q_MSG, Q_MSG + 1)
    for i in range(9, 14):
        loads[i].wait()
    uvt[...] = jnp.transpose(wuv[...].astype(f32)).astype(bf16)
    for h in range(HEADS):
        vbuf[h, VDIM:VROWS, :] = jnp.ones((VROWS - VDIM, 2 * GROUP), bf16)
    acc[...] = jnp.zeros_like(acc)
    best[...] = jnp.full(best.shape, masked_score, f32)
    arrived(X_MSG + 2, X_MSG + 3)
    start(A_MSG, A_MSG + 1, B_MSG, B_MSG + 1)
    arrived(Q_MSG, Q_MSG + 1)
    start(Q_MSG + 2, Q_MSG + 3)
    arrived(Q_MSG + 2, Q_MSG + 3)

    factor = (NOPE + ROPE) ** (-0.5) * 1.4426950408889634
    rows = ql[...].reshape(GROUP, 1024)
    plain = jnp.dot(rows, wuq[...], preferred_element_type=f32) * factor
    qt[c, 0 : HEADS * NOPE, :] = jnp.transpose(plain).astype(bf16)
    turned = jnp.transpose(jnp.dot(rows, wur[...], preferred_element_type=f32) * factor)
    cosine, sine = query_cos[...], query_sin[...]
    for h in range(HEADS):
        one = turned[h * ROPE : h * ROPE + 32]
        two = turned[h * ROPE + 32 : (h + 1) * ROPE]
        at_row = HEADS * NOPE + h * ROPE
        qt[c, at_row : at_row + 32, :] = (one * cosine - two * sine).astype(bf16)
        qt[c, at_row + 32 : at_row + 64, :] = (two * cosine + one * sine).astype(bf16)
    start(QX_MSG)
    arrived(QX_MSG)
    for h in range(HEADS):
        for j in range(2):
            cols = slice(j * GROUP, (j + 1) * GROUP)
            qfull[h, 0:NOPE, cols] = qt[j, h * NOPE : (h + 1) * NOPE, :]
            at_row = HEADS * NOPE + h * ROPE
            qfull[h, NOPE : NOPE + ROPE, cols] = qt[j, at_row : at_row + ROPE, :]
        qfull[h, NOPE + ROPE :, :] = jnp.zeros((ROPE, 2 * GROUP), bf16)

    UNIT = 2 * GROUP

    def attend(set_one, set_two, m_one, m_two, masked):
        parts, rots = [], []
        for s in (set_one, set_two):
            tiles = [
                lat[s, :, t * OWN : (t + 1) * OWN, :].reshape(GROUP, 128) for t in range(4)
            ]
            parts.append(jnp.concatenate(tiles, axis=1))
            packed = lat[s, :, 256:288, :]
            swapped = pltpu.roll(packed.reshape(128, 128).astype(f32), 64, 1).astype(bf16)
            rots.append(
                jnp.concatenate([packed, swapped.reshape(4, 32, 128)], axis=1).reshape(GROUP, 128)
            )
        latents = jnp.concatenate(parts, axis=0)
        keys = jnp.dot(latents, wuk[...], preferred_element_type=f32).astype(bf16)
        for h in range(HEADS):
            kbuf[h, :, 0:NOPE] = keys[:, h * NOPE : (h + 1) * NOPE]
            kbuf[h, :, NOPE:256] = jnp.concatenate(rots, axis=0)
        values = lax.dot_general(
            uvt[...], latents, (((1,), (1,)), ((), ())), preferred_element_type=f32
        ).astype(bf16)
        for h in range(HEADS):
            vbuf[h, 0:VDIM, :] = values[h * VDIM : (h + 1) * VDIM]

        def score(h):
            scores = jnp.dot(kbuf[h], qfull[h], preferred_element_type=f32)
            if masked:
                row = lax.broadcasted_iota(jnp.int32, (UNIT, UNIT), 0)
                col = lax.broadcasted_iota(jnp.int32, (UNIT, UNIT), 1)
                base_one = (2 * m_one + c) * GROUP
                base_two = (2 * m_two + c) * GROUP - GROUP
                place = row + jnp.where(row < GROUP, base_one, base_two)
                scores = jnp.where(place <= col + 2 * m * GROUP, scores, masked_score)
            sbuf[h % 2] = scores
            tops[h % 2] = jnp.max(scores, axis=0, keepdims=True)

        score(0)
        for h in range(HEADS):
            if h + 1 < HEADS:
                score(h + 1)
            old = best[h]
            new = jnp.maximum(old, tops[h % 2])
            weights = jnp.exp2(sbuf[h % 2] - new).astype(bf16)
            best[h] = new
            acc[h] = acc[h] * jnp.exp2(old - new) + jnp.dot(
                vbuf[h], weights, preferred_element_type=f32
            )

    def unit(u, carry):
        @pl.when(u == 0)
        def _():
            arrived(A_MSG, A_MSG + 1)
            start(A_MSG + 2, A_MSG + 3)
            start(B_MSG + 4, B_MSG + 5, B_MSG + 8, B_MSG + 9)

        @pl.when(u == 1)
        def _():
            arrived(B_MSG, B_MSG + 1)
            start(B_MSG + 2, B_MSG + 3)

        @pl.when(u == 2)
        def _():
            arrived(A_MSG + 2, A_MSG + 3)
            start(B_MSG + 12, B_MSG + 13)

        for k in (1, 2, 3):

            @pl.when(u == 2 + k)
            def _(k=k):
                arrived(B_MSG + 4 * k, B_MSG + 4 * k + 1)
                start(B_MSG + 4 * k + 2, B_MSG + 4 * k + 3)

        @pl.when(u == 6)
        def _():
            arrived(B_MSG + 2, B_MSG + 3, B_MSG + 6, B_MSG + 7)

        @pl.when(u == 7)
        def _():
            arrived(B_MSG + 10, B_MSG + 11, B_MSG + 14, B_MSG + 15)

        sets, spots = [], []
        for n in range(2):
            aa = mod4(a + pick(u, UNIT_OA[n]))
            bb = mod4(b + pick(u, UNIT_OB[n]))
            sets.append(bb * 4 + aa)
            spots.append(jnp.where(first, bb * 4 + aa, aa * 4 + bb))
        plain_unit = jnp.logical_and(spots[0] < m, spots[1] < m)
        some = jnp.logical_or(spots[0] <= m, spots[1] <= m)

        @pl.when(plain_unit)
        def _():
            attend(*sets, *spots, False)

        @pl.when(jnp.logical_and(some, jnp.logical_not(plain_unit)))
        def _():
            attend(*sets, *spots, True)

        return carry

    lax.fori_loop(0, 8, unit, 0)

    mine_at = pl.ds(pl.multiple_of(c * GROUP, GROUP), GROUP)
    other_at = pl.ds(pl.multiple_of((1 - c) * GROUP, GROUP), GROUP)
    for h in range(HEADS):
        xsend[h, 0:136, :] = acc[h, 0:136, other_at]
        xsend[h, 136:144, :] = jnp.broadcast_to(best[h, :, other_at], (8, GROUP))
    start(OX_MSG)
    arrived(OX_MSG)
    heads = []
    for h in range(HEADS):
        mine, theirs = best[h, :, mine_at], xrecv[h, 136:137, :]
        top = jnp.maximum(mine, theirs)
        w_mine, w_theirs = jnp.exp2(mine - top), jnp.exp2(theirs - top)
        total = acc[h, 128:129, mine_at] * w_mine + xrecv[h, 128:129, :] * w_theirs
        summed = acc[h, 0:128, mine_at] * w_mine + xrecv[h, 0:128, :] * w_theirs
        heads.append(jnp.transpose(summed / total).astype(bf16))
    attended = jnp.concatenate(heads, axis=1)

    WIDE = 4096 // COLS
    top, low = pl.ds(0, 32), pl.ds(32, 32)
    for k in range(COLS):
        cols = pl.ds(k * WIDE, WIDE)
        i = R_MSG + 6 * k
        send[i] = rcopy(i, pbuf.at[x2, top, cols], r1buf.at[0, :, cols], dev_xp)
        send[i + 1] = rcopy(i + 1, pbuf.at[x2, low, cols], r1buf.at[1, :, cols], dev_xm)
        send[i + 2] = rcopy(i + 2, pbuf.at[xp, low, cols], dbuf.at[0, :, cols], dev_xp)
        send[i + 3] = rcopy(i + 3, pbuf.at[xm, top, cols], dbuf.at[1, :, cols], dev_xm)
        send[i + 4] = rcopy(i + 4, cbuf.at[0, :, cols], crecv.at[0, :, cols], dev_xp)
        send[i + 5] = rcopy(i + 5, cbuf.at[1, :, cols], crecv.at[1, :, cols], dev_xm)
        for n in range(6):
            recv[i + n] = send[i + n]
    for k in range(COLS):
        cols = slice(k * WIDE, (k + 1) * WIDE)
        part = jnp.dot(attended, wout[:, cols], preferred_element_type=f32).astype(bf16)
        pbuf[:, :, cols] = part.reshape(4, OWN, WIDE)
        start(R_MSG + 6 * k, R_MSG + 6 * k + 1)
    for k in range(COLS):
        start(R_MSG + 6 * k + 2, R_MSG + 6 * k + 3)
    for k in range(COLS):
        cols = slice(k * WIDE, (k + 1) * WIDE)
        i = R_MSG + 6 * k
        arrived(i, i + 1)
        cbuf[0, :, cols] = (
            r1buf[0, :, cols].astype(f32) + pbuf[xp, 0:32, cols].astype(f32)
        ).astype(bf16)
        cbuf[1, :, cols] = (
            r1buf[1, :, cols].astype(f32) + pbuf[xm, 32:64, cols].astype(f32)
        ).astype(bf16)
        start(i + 4, i + 5)
    for k in range(COLS):
        cols = slice(k * WIDE, (k + 1) * WIDE)
        i = R_MSG + 6 * k
        arrived(i + 2, i + 3, i + 4, i + 5)
        out[0:32, cols] = (
            pbuf[x, 0:32, cols].astype(f32)
            + crecv[0, :, cols].astype(f32)
            + dbuf[1, :, cols].astype(f32)
        ).astype(bf16)
        out[32:64, cols] = (
            pbuf[x, 32:64, cols].astype(f32)
            + crecv[1, :, cols].astype(f32)
            + dbuf[0, :, cols].astype(f32)
        ).astype(bf16)
    for i in range(N_MSG):
        send[i].wait_send()


def local(
    tokens,
    down_query,
    down_latent,
    down_rotary,
    query_gain,
    latent_gain,
    up_query,
    up_query_rotary,
    up_key,
    up_value,
    out_weight,
):
    sp = lax.axis_index("sp")
    x = lax.axis_index("tp")
    inverse = rope_base ** (-jnp.arange(0, ROPE, 2, dtype=f32) / ROPE)
    own = ((sp * RING + x) * OWN + jnp.arange(OWN, dtype=jnp.int32)).astype(f32)
    angles = own[:, None] * jnp.tile(inverse, 4)[None, :]
    sign = jnp.tile(jnp.repeat(jnp.array([-1.0, 1.0], f32), 32), 2)
    key_cos, key_sin = jnp.cos(angles), jnp.sin(angles) * sign[None, :]
    span = (sp * GROUP + jnp.arange(GROUP, dtype=jnp.int32)).astype(f32)
    angles = inverse[:, None] * span[None, :]
    query_cos, query_sin = jnp.cos(angles), jnp.sin(angles)

    vmem = pl.BlockSpec(memory_space=pltpu.VMEM)
    hbm = pl.BlockSpec(memory_space=pl.ANY)
    return pl.pallas_call(
        kernel,
        out_shape=jax.ShapeDtypeStruct((OWN, 4096), bf16),
        in_specs=[vmem, hbm, hbm, hbm, vmem, vmem, hbm, hbm, hbm, hbm, hbm, vmem, vmem, vmem, vmem],
        out_specs=vmem,
        scratch_shapes=[
            pltpu.VMEM((4096, 512), bf16),
            pltpu.VMEM((64, 4096), bf16),
            pltpu.VMEM((4096, 1024), bf16),
            pltpu.VMEM((1024, 512), bf16),
            pltpu.VMEM((1024, 256), bf16),
            pltpu.VMEM((512, 512), bf16),
            pltpu.VMEM((512, 512), bf16),
            pltpu.VMEM((512, 4096), bf16),
            pltpu.VMEM((16, 4, BLOCK, 128), bf16),
            pltpu.VMEM((4, OWN, 1024), bf16),
            pltpu.VMEM((2, HEADS * (NOPE + ROPE), GROUP), bf16),
            pltpu.VMEM((512, 512), bf16),
            pltpu.VMEM((HEADS, 2 * GROUP, 256), bf16),
            pltpu.VMEM((HEADS, VROWS, 2 * GROUP), bf16),
            pltpu.VMEM((HEADS, VROWS, 2 * GROUP), f32),
            pltpu.VMEM((HEADS, 1, 2 * GROUP), f32),
            pltpu.VMEM((HEADS, 256, 2 * GROUP), bf16),
            pltpu.VMEM((2, 2 * GROUP, 2 * GROUP), f32),
            pltpu.VMEM((2, 1, 2 * GROUP), f32),
            pltpu.VMEM((HEADS, VROWS, GROUP), f32),
            pltpu.VMEM((HEADS, VROWS, GROUP), f32),
            pltpu.VMEM((4, OWN, 4096), bf16),
            pltpu.VMEM((2, 32, 4096), bf16),
            pltpu.VMEM((2, 32, 4096), bf16),
            pltpu.VMEM((2, 32, 4096), bf16),
            pltpu.VMEM((2, 32, 4096), bf16),
            pltpu.SemaphoreType.DMA((14,)),
            pltpu.SemaphoreType.DMA((N_MSG,)),
            pltpu.SemaphoreType.DMA((N_MSG,)),
        ],
        compiler_params=pltpu.CompilerParams(
            collective_id=0, has_side_effects=True, vmem_limit_bytes=62 * 1024 * 1024
        ),
    )(
        tokens,
        down_query,
        down_latent,
        down_rotary.T,
        query_gain.reshape(1, -1),
        latent_gain.reshape(1, -1),
        up_query,
        up_query_rotary,
        up_key,
        up_value,
        out_weight,
        key_cos,
        key_sin,
        query_cos,
        query_sin,
    )


def solution(mesh):
    return jax.shard_map(
        local,
        mesh=mesh,
        in_specs=(
            P(("sp", "tp"), None),
            P(),
            P(),
            P(),
            P(),
            P(),
            P(None, "tp"),
            P(None, "tp"),
            P(None, "tp"),
            P(None, "tp"),
            P("tp", None),
        ),
        out_specs=P(("sp", "tp"), None),
        check_vma=False,
    )
```

```python
import functools

import jax
import jax.numpy as jnp
import numpy as np
from jax import lax
from jax.experimental import pallas as pl
from jax.experimental.pallas import tpu as pltpu
from jax.sharding import PartitionSpec as P

NOPE = 128
ROPE = 64
VDIM = 128
HEADS = 4
OWN = 64
GROUP = 256
BLOCK = 288
VROWS = 144
RING = 4

rope_base = 500000.0
norm_eps = 1e-06
masked_score = -1e30

f32 = jnp.float32
bf16 = jnp.bfloat16
MESH = pl.DeviceIdType.MESH

COLS = 4
N_MSG = 104

UNIT_OA = ((0, -1, 2, 1, 0, -1, 1, -1), (1, 0, 0, 1, -1, 2, 2, 2))
UNIT_OB = ((0, 0, 0, 1, 2, -1, 2, 2), (0, 1, -1, -1, 1, 1, -1, 2))


def pick(index, values):
    out = jnp.int32(values[0])
    for i, v in enumerate(values[1:], 1):
        out = jnp.where(index == i, jnp.int32(v), out)
    return out


def mod4(v):
    return lax.rem(v + 8, 4)


def kernel(
    tokens_in,
    down_query,
    down_latent,
    down_rotary,
    query_gain,
    latent_gain,
    up_query,
    up_query_rotary,
    up_key,
    up_value,
    out_weight,
    lane_rates,
    row_rates,
    out,
    tokens,
    lrate,
    rrate,
    lgain,
    qgain,
    wdl,
    wdr,
    wdq,
    wuq,
    wur,
    wuk,
    wuv,
    wout,
    lat,
    ql,
    qt,
    uvt,
    kbuf,
    vbuf,
    acc,
    best,
    qfull,
    sbuf,
    tops,
    xsend,
    xrecv,
    pbuf,
    r1buf,
    dbuf,
    cbuf,
    crecv,
    local_sem,
    ssem,
    rsem,
):
    sp = lax.axis_index("sp")
    x = lax.axis_index("tp")
    c = lax.rem(sp, 2)
    m = sp // 2
    y = lax.rem(m, 4)
    z = m // 4
    first = c == 0
    a = jnp.where(first, y, z)
    b = jnp.where(first, z, y)
    stride_a = jnp.where(first, 2, 8)
    stride_b = jnp.where(first, 8, 2)

    def at(aa, bb):
        return {"sp": aa * stride_a + bb * stride_b + c, "tp": x}

    xp, xm, x2 = mod4(x + 1), mod4(x - 1), mod4(x + 2)
    dev_xp = {"sp": sp, "tp": xp}
    dev_xm = {"sp": sp, "tp": xm}
    dev_ap, dev_am = at(mod4(a + 1), b), at(mod4(a - 1), b)
    dev_bp, dev_bm = at(a, mod4(b + 1)), at(a, mod4(b - 1))
    dev_core = {"sp": sp + 1 - 2 * c, "tp": x}

    copies = []

    def copy_in(src, dst):
        copies.append(pltpu.make_async_copy(src, dst, local_sem.at[len(copies)]))
        copies[-1].start()
        return copies[-1]

    K4 = 1024
    quarters = [pl.ds(k * K4, K4) for k in range(4)]
    load_lanes = copy_in(lane_rates, lrate)
    load_tokens = copy_in(tokens_in, tokens)
    load_latent = [copy_in(down_latent.at[r], wdl.at[r]) for r in quarters]
    load_rotary = copy_in(down_rotary, wdr)
    load_rows = copy_in(row_rates, rrate)
    load_lgain = copy_in(latent_gain, lgain)
    load_qgain = copy_in(query_gain, qgain)
    load_query = [copy_in(down_query.at[r], wdq.at[r]) for r in quarters]
    load_rest = [
        copy_in(up_query, wuq),
        copy_in(up_query_rotary, wur),
        copy_in(up_key, wuk),
        copy_in(up_value, wuv),
        copy_in(out_weight, wout),
    ]

    barrier = pltpu.get_barrier_semaphore()
    for dev in (dev_xp, dev_xm, dev_ap, dev_am, dev_bp, dev_bm, dev_core):
        pl.semaphore_signal(barrier, inc=1, device_id=dev, device_id_type=MESH)

    send, recv = [], []

    def add(src, dst, landed, dev):
        i = len(send)
        for refs, done in ((src, dst), send), ((landed, landed), recv):
            done.append(
                pltpu.make_async_remote_copy(
                    src_ref=refs[0],
                    dst_ref=refs[1],
                    send_sem=ssem.at[i],
                    recv_sem=rsem.at[i],
                    device_id=dev,
                    device_id_type=MESH,
                )
            )
        return i

    def pair(up, up_landed, dev_up, down, down_landed, dev_down):
        return (
            add(lat.at[up], lat.at[up], lat.at[up_landed], dev_up),
            add(lat.at[down], lat.at[down], lat.at[down_landed], dev_down),
        )

    def group(oa, ob):
        return mod4(b + ob) * 4 + mod4(a + oa)

    def line(ob, start=0, count=4):
        return pl.ds(mod4(b + ob) * 4 + start, count)

    def xs(o):
        return mod4(x + o)

    OFFS = (0, 1, -1, 2)
    s0 = group(0, 0)
    every, pre, post = pl.ds(0, 4), pl.ds(0, 2), pl.ds(2, 2)
    early, late = pl.ds(48, 240), pl.ds(0, 48)
    late_lo, late_hi = pl.ds(0, 32), pl.ds(32, 16)
    lo, hi = pl.ds(0, BLOCK // 2), pl.ds(BLOCK // 2, BLOCK // 2)
    own_block = (s0, x)

    X1 = pair(own_block, (s0, xm), dev_xp, own_block, (s0, xp), dev_xm)
    X2 = pair((s0, xm, lo), (s0, x2, lo), dev_xp, (s0, xp, hi), (s0, x2, hi), dev_xm)
    A1, B1 = {}, {}
    for o in OFFS:
        block = (s0, xs(o), early)
        A1[o] = pair(
            block, (group(-1, 0), *block[1:]), dev_ap, block, (group(1, 0), *block[1:]), dev_am
        )
        B1[0, o] = pair(
            block, (group(0, -1), *block[1:]), dev_bp, block, (group(0, 1), *block[1:]), dev_bm
        )
    A2 = pair(
        (group(-1, 0), pre, early),
        (group(2, 0), pre, early),
        dev_ap,
        (group(1, 0), post, early),
        (group(2, 0), post, early),
        dev_am,
    )
    B2, PB1 = {}, {}
    for o in OFFS:
        whole = (group(o, 0), every, early)
        if o != 0:
            B1[o] = pair(
                whole, (group(o, -1), *whole[1:]), dev_bp, whole, (group(o, 1), *whole[1:]), dev_bm
            )
        B2[o] = pair(
            (group(o, -1), pre, early),
            (group(o, 2), pre, early),
            dev_bp,
            (group(o, 1), post, early),
            (group(o, 2), post, early),
            dev_bm,
        )
        part = (group(o, 0), x, late)
        PB1[o] = pair(
            part, (group(o, -1), x, late), dev_bp, part, (group(o, 1), x, late), dev_bm
        )
    part = (s0, x, late)
    PA1 = pair(part, (group(-1, 0), x, late), dev_ap, part, (group(1, 0), x, late), dev_am)
    PA2 = pair(
        (group(-1, 0), x, late_lo),
        (group(2, 0), x, late_lo),
        dev_ap,
        (group(1, 0), x, late_hi),
        (group(2, 0), x, late_hi),
        dev_am,
    )
    PB2 = pair(
        (line(-1, 0, 2), x, late),
        (line(2, 0, 2), x, late),
        dev_bp,
        (line(1, 2, 2), x, late),
        (line(2, 2, 2), x, late),
        dev_bm,
    )
    XL1, XL2, XP1, XP2 = {}, {}, {}, {}
    for o in (1, -1, 2):
        g = group(o, 0)
        XL1[o] = pair((g, x, late), (g, xm, late), dev_xp, (g, x, late), (g, xp, late), dev_xm)
        XL2[o] = pair(
            (g, xm, late_lo), (g, x2, late_lo), dev_xp, (g, xp, late_hi), (g, x2, late_hi), dev_xm
        )
        g = line(o)
        XP1[o] = pair((g, x, late), (g, xm, late), dev_xp, (g, x, late), (g, xp, late), dev_xm)
        g, h = line(o, 0, 2), line(o, 2, 2)
        XP2[o] = pair((g, xm, late), (g, x2, late), dev_xp, (h, xp, late), (h, x2, late), dev_xm)
    q_lo, q_hi = pl.ds(0, OWN // 2), pl.ds(OWN // 2, OWN // 2)
    Q1 = (
        add(ql.at[x], ql.at[x], ql.at[xm], dev_xp),
        add(ql.at[x], ql.at[x], ql.at[xp], dev_xm),
    )
    Q2 = (
        add(ql.at[xm, q_lo], ql.at[xm, q_lo], ql.at[x2, q_lo], dev_xp),
        add(ql.at[xp, q_hi], ql.at[xp, q_hi], ql.at[x2, q_hi], dev_xm),
    )
    QX = (add(qt.at[c], qt.at[c], qt.at[1 - c], dev_core),)
    OX = (add(xsend, xrecv, xrecv, dev_core),)

    def start(*groups):
        for ids in groups:
            for i in ids:
                send[i].start()

    def arrived(*groups):
        for ids in groups:
            for i in ids:
                recv[i].wait_recv()

    def norm_rows(values, gain):
        return values * lax.rsqrt(jnp.mean(values * values, axis=-1, keepdims=True) + norm_eps) * gain

    load_lanes.wait()
    spot = lax.broadcasted_iota(jnp.int32, (OWN, 128), 0) + (sp * RING + x) * OWN
    angles = spot.astype(f32) * lrate[...]
    lane = lax.broadcasted_iota(jnp.int32, (OWN, 128), 1)
    key_cos = jnp.cos(angles)
    key_sin = jnp.sin(angles) * jnp.where(lax.rem(lane, 64) < 32, -1.0, 1.0)
    load_tokens.wait()
    latent = jnp.zeros((OWN, 512), f32)
    for k in range(4):
        load_latent[k].wait()
        cols = slice(k * K4, (k + 1) * K4)
        latent = latent + jnp.dot(tokens[:, cols], wdl[cols, :], preferred_element_type=f32)
    load_lgain.wait()
    latent = norm_rows(latent, lgain[...]).astype(bf16)
    for t in range(4):
        lat[s0, x, t * OWN : (t + 1) * OWN, :] = latent[:, t * 128 : (t + 1) * 128]
    load_rotary.wait()
    turned = lax.dot_general(
        tokens[...], wdr[...], (((1,), (1,)), ((), ())), preferred_element_type=f32
    )
    turned = jnp.concatenate([turned, turned], axis=-1)
    turned = turned * key_cos + pltpu.roll(turned, 32, 1) * key_sin
    lat[s0, x, 256:288, :] = jnp.where(lane[:32] < 64, turned[:32], turned[32:]).astype(bf16)
    pl.semaphore_wait(barrier, 7)
    start(X1, PA1, B1[0, 0], A1[0], PB1[0])

    query = jnp.zeros((OWN, 1024), f32)
    for k in range(4):
        load_query[k].wait()
        cols = slice(k * K4, (k + 1) * K4)
        query = query + jnp.dot(tokens[:, cols], wdq[cols, :], preferred_element_type=f32)
    load_qgain.wait()
    ql[x] = norm_rows(query, qgain[...]).astype(bf16)
    start(Q1)
    arrived(PA1)
    start(PA2, XL1[1], XL1[-1], PB1[1], PB1[-1])
    load_rows.wait()
    for load in load_rest:
        load.wait()
    uvt[...] = jnp.transpose(wuv[...].astype(f32)).astype(bf16)
    for h in range(HEADS):
        vbuf[h, VDIM:VROWS, :] = jnp.ones((VROWS - VDIM, 2 * GROUP), bf16)
    acc[...] = jnp.zeros_like(acc)
    best[...] = jnp.full(best.shape, masked_score, f32)
    spot = lax.broadcasted_iota(jnp.int32, (32, GROUP), 1) + sp * GROUP
    angles = spot.astype(f32) * rrate[...]
    cosine, sine = jnp.cos(angles), jnp.sin(angles)
    arrived(X1)
    start(X2, A1[1], A1[-1], B1[0, 1], B1[0, -1])
    arrived(PA2)
    start(XL1[2], PB1[2])
    arrived(Q1)
    start(Q2)
    arrived(XL1[1], XL1[-1])
    start(XL2[1], XL2[-1])
    arrived(PB1[0], PB1[1], PB1[-1], PB1[2])
    start(PB2, XP1[1], XP1[-1])
    arrived(X2)
    start(A1[2], B1[0, 2])
    arrived(XL1[2])
    start(XL2[2])
    arrived(Q2)
    factor = (NOPE + ROPE) ** (-0.5) * 1.4426950408889634
    rows = ql[...].reshape(GROUP, 1024)
    plain = jnp.dot(rows, wuq[...], preferred_element_type=f32) * factor
    qt[c, 0 : HEADS * NOPE, :] = jnp.transpose(plain).astype(bf16)
    turned = jnp.transpose(jnp.dot(rows, wur[...], preferred_element_type=f32) * factor)
    for h in range(HEADS):
        one = turned[h * ROPE : h * ROPE + 32]
        two = turned[h * ROPE + 32 : (h + 1) * ROPE]
        at_row = HEADS * NOPE + h * ROPE
        qt[c, at_row : at_row + 32, :] = (one * cosine - two * sine).astype(bf16)
        qt[c, at_row + 32 : at_row + 64, :] = (two * cosine + one * sine).astype(bf16)
    start(QX)

    UNIT = 2 * GROUP

    def sets_of(u):
        sets, spots = [], []
        for n in range(2):
            aa = mod4(a + pick(u, UNIT_OA[n]))
            bb = mod4(b + pick(u, UNIT_OB[n]))
            sets.append(bb * 4 + aa)
            spots.append(jnp.where(first, bb * 4 + aa, aa * 4 + bb))
        return sets, spots

    def expand(u):
        parts, rots = [], []
        for s in sets_of(u)[0]:
            tiles = [
                lat[s, :, t * OWN : (t + 1) * OWN, :].reshape(GROUP, 128) for t in range(4)
            ]
            parts.append(jnp.concatenate(tiles, axis=1))
            packed = lat[s, :, 256:288, :]
            swapped = pltpu.roll(packed.reshape(128, 128).astype(f32), 64, 1).astype(bf16)
            rots.append(
                jnp.concatenate([packed, swapped.reshape(4, 32, 128)], axis=1).reshape(GROUP, 128)
            )
        latents = jnp.concatenate(parts, axis=0)
        kbuf[:, 0:512] = jnp.dot(latents, wuk[...], preferred_element_type=f32).astype(bf16)
        kbuf[:, 512:640] = jnp.concatenate(rots, axis=0)
        values = lax.dot_general(
            uvt[...], latents, (((1,), (1,)), ((), ())), preferred_element_type=f32
        ).astype(bf16)
        for h in range(HEADS):
            vbuf[h, 0:VDIM, :] = values[h * VDIM : (h + 1) * VDIM]

    def attend(spots, masked):
        def score(h):
            keys = jnp.concatenate(
                [kbuf[:, h * NOPE : (h + 1) * NOPE], kbuf[:, 512:640]], axis=1
            )
            scores = jnp.dot(keys, qfull[h], preferred_element_type=f32)
            if masked:
                row = lax.broadcasted_iota(jnp.int32, (UNIT, UNIT), 0)
                col = lax.broadcasted_iota(jnp.int32, (UNIT, UNIT), 1)
                base_one = (2 * spots[0] + c) * GROUP
                base_two = (2 * spots[1] + c) * GROUP - GROUP
                place = row + jnp.where(row < GROUP, base_one, base_two)
                scores = jnp.where(place <= col + 2 * m * GROUP, scores, masked_score)
            sbuf[h % 2] = scores
            tops[h % 2] = jnp.max(scores, axis=0, keepdims=True)

        score(0)
        for h in range(HEADS):
            if h + 1 < HEADS:
                score(h + 1)
            old = best[h]
            new = jnp.maximum(old, tops[h % 2])
            weights = jnp.exp2(sbuf[h % 2] - new).astype(bf16)
            best[h] = new
            acc[h] = acc[h] * jnp.exp2(old - new) + jnp.dot(
                vbuf[h], weights, preferred_element_type=f32
            )

    def needed(u):
        spots = sets_of(u)[1]
        return jnp.logical_or(spots[0] <= m, spots[1] <= m)

    arrived(PB2)
    start(XP1[2])
    arrived(A1[0], A1[1], A1[-1], A1[2])
    start(A2, B1[1], B1[-1])
    arrived(XL2[1], XL2[-1])

    def unit(u, carry):

        @pl.when(u == 1)
        def _():
            arrived(XP1[2])
            start(XP2[2])
            arrived(XP2[1], XP2[-1])

        @pl.when(u == 2)
        def _():
            arrived(A2)
            start(B1[2])
            arrived(XL2[2])

        @pl.when(u == 4)
        def _():
            arrived(B2[0], XP2[2])

        @pl.when(u == 5)
        def _():
            arrived(B1[2])
            start(B2[2])

        @pl.when(u == 6)
        def _():
            arrived(B2[1])

        @pl.when(u == 7)
        def _():
            arrived(B2[-1], B2[2])

        spots = sets_of(u)[1]
        plain_unit = jnp.logical_and(spots[0] < m, spots[1] < m)
        some = needed(u)

        @pl.when(some)
        def _():
            expand(u)


        @pl.when(u == 0)
        def _():
            arrived(B1[0, 0], B1[0, 1], B1[0, -1], B1[0, 2])
            start(B2[0])
            arrived(XP1[1], XP1[-1])
            start(XP2[1], XP2[-1])
            arrived(QX)
            for h in range(HEADS):
                for j in range(2):
                    cols = slice(j * GROUP, (j + 1) * GROUP)
                    qfull[h, 0:NOPE, cols] = qt[j, h * NOPE : (h + 1) * NOPE, :]
                    at_row = HEADS * NOPE + h * ROPE
                    qfull[h, NOPE : NOPE + ROPE, cols] = qt[j, at_row : at_row + ROPE, :]
                qfull[h, NOPE + ROPE :, :] = jnp.zeros((ROPE, 2 * GROUP), bf16)

        @pl.when(u == 2)
        def _():
            arrived(B1[1])
            start(B2[1])

        @pl.when(u == 3)
        def _():
            arrived(B1[-1])
            start(B2[-1])


        @pl.when(plain_unit)
        def _():
            attend(spots, False)

        @pl.when(jnp.logical_and(some, jnp.logical_not(plain_unit)))
        def _():
            attend(spots, True)

        return carry

    lax.fori_loop(0, 8, unit, 0)

    mine_at = pl.ds(pl.multiple_of(c * GROUP, GROUP), GROUP)
    other_at = pl.ds(pl.multiple_of((1 - c) * GROUP, GROUP), GROUP)
    for h in range(HEADS):
        xsend[h, 0:136, :] = acc[h, 0:136, other_at]
        xsend[h, 136:144, :] = jnp.broadcast_to(best[h, :, other_at], (8, GROUP))
    start(OX)
    arrived(OX)
    heads = []
    for h in range(HEADS):
        mine, theirs = best[h, :, mine_at], xrecv[h, 136:137, :]
        top = jnp.maximum(mine, theirs)
        w_mine, w_theirs = jnp.exp2(mine - top), jnp.exp2(theirs - top)
        total = acc[h, 128:129, mine_at] * w_mine + xrecv[h, 128:129, :] * w_theirs
        summed = acc[h, 0:128, mine_at] * w_mine + xrecv[h, 0:128, :] * w_theirs
        heads.append(jnp.transpose(summed / total).astype(bf16))
    attended = jnp.concatenate(heads, axis=1)

    WIDE = 4096 // COLS
    top, low = pl.ds(0, 32), pl.ds(32, 32)
    R1, RD, RC = [], [], []
    for k in range(COLS):
        cols = pl.ds(k * WIDE, WIDE)

        def both(to_up, to_down, ref):
            up, down = ref.at[0, :, cols], ref.at[1, :, cols]
            return add(to_up, up, up, dev_xp), add(to_down, down, down, dev_xm)

        R1.append(both(pbuf.at[x2, top, cols], pbuf.at[x2, low, cols], r1buf))
        RD.append(both(pbuf.at[xp, low, cols], pbuf.at[xm, top, cols], dbuf))
        RC.append(both(cbuf.at[0, :, cols], cbuf.at[1, :, cols], crecv))
    assert len(send) == N_MSG, len(send)
    for k in range(COLS):
        cols = slice(k * WIDE, (k + 1) * WIDE)
        part = jnp.dot(attended, wout[:, cols], preferred_element_type=f32).astype(bf16)
        pbuf[:, :, cols] = part.reshape(4, OWN, WIDE)
        start(R1[k])
    start(*RD)
    for k in range(COLS):
        cols = slice(k * WIDE, (k + 1) * WIDE)
        arrived(R1[k])
        cbuf[0, :, cols] = (
            r1buf[0, :, cols].astype(f32) + pbuf[xp, 0:32, cols].astype(f32)
        ).astype(bf16)
        cbuf[1, :, cols] = (
            r1buf[1, :, cols].astype(f32) + pbuf[xm, 32:64, cols].astype(f32)
        ).astype(bf16)
        start(RC[k])
    for k in range(COLS):
        cols = slice(k * WIDE, (k + 1) * WIDE)
        arrived(RD[k], RC[k])
        out[0:32, cols] = (
            pbuf[x, 0:32, cols].astype(f32)
            + crecv[0, :, cols].astype(f32)
            + dbuf[1, :, cols].astype(f32)
        ).astype(bf16)
        out[32:64, cols] = (
            pbuf[x, 32:64, cols].astype(f32)
            + crecv[1, :, cols].astype(f32)
            + dbuf[0, :, cols].astype(f32)
        ).astype(bf16)
    for i in range(N_MSG):
        send[i].wait_send()


def local(
    tokens,
    down_query,
    down_latent,
    down_rotary,
    query_gain,
    latent_gain,
    up_query,
    up_query_rotary,
    up_key,
    up_value,
    out_weight,
):
    rates = (rope_base ** (-np.arange(0, ROPE, 2) / ROPE)).astype(np.float32)
    lane_rates = jnp.asarray(np.tile(rates, 4)[None, :])
    row_rates = jnp.asarray(np.repeat(rates[:, None], GROUP, axis=1))
    vmem = pl.BlockSpec(memory_space=pltpu.VMEM)
    hbm = pl.BlockSpec(memory_space=pl.ANY)
    return pl.pallas_call(
        kernel,
        out_shape=pltpu.VMEM((OWN, 4096), bf16),
        in_specs=[hbm] * 13,
        out_specs=vmem,
        scratch_shapes=[
            pltpu.VMEM((OWN, 4096), bf16),
            pltpu.VMEM((1, 128), f32),
            pltpu.VMEM((32, GROUP), f32),
            pltpu.VMEM((1, 512), f32),
            pltpu.VMEM((1, 1024), f32),
            pltpu.VMEM((4096, 512), bf16),
            pltpu.VMEM((64, 4096), bf16),
            pltpu.VMEM((4096, 1024), bf16),
            pltpu.VMEM((1024, 512), bf16),
            pltpu.VMEM((1024, 256), bf16),
            pltpu.VMEM((512, 512), bf16),
            pltpu.VMEM((512, 512), bf16),
            pltpu.VMEM((512, 4096), bf16),
            pltpu.VMEM((16, 4, BLOCK, 128), bf16),
            pltpu.VMEM((4, OWN, 1024), bf16),
            pltpu.VMEM((2, HEADS * (NOPE + ROPE), GROUP), bf16),
            pltpu.VMEM((512, 512), bf16),
            pltpu.VMEM((2 * GROUP, 640), bf16),
            pltpu.VMEM((HEADS, VROWS, 2 * GROUP), bf16),
            pltpu.VMEM((HEADS, VROWS, 2 * GROUP), f32),
            pltpu.VMEM((HEADS, 1, 2 * GROUP), f32),
            pltpu.VMEM((HEADS, 256, 2 * GROUP), bf16),
            pltpu.VMEM((2, 2 * GROUP, 2 * GROUP), f32),
            pltpu.VMEM((2, 1, 2 * GROUP), f32),
            pltpu.VMEM((HEADS, VROWS, GROUP), f32),
            pltpu.VMEM((HEADS, VROWS, GROUP), f32),
            pltpu.VMEM((4, OWN, 4096), bf16),
            pltpu.VMEM((2, 32, 4096), bf16),
            pltpu.VMEM((2, 32, 4096), bf16),
            pltpu.VMEM((2, 32, 4096), bf16),
            pltpu.VMEM((2, 32, 4096), bf16),
            pltpu.SemaphoreType.DMA((19,)),
            pltpu.SemaphoreType.DMA((N_MSG,)),
            pltpu.SemaphoreType.DMA((N_MSG,)),
        ],
        compiler_params=pltpu.CompilerParams(
            collective_id=0, has_side_effects=True, vmem_limit_bytes=62 * 1024 * 1024
        ),
    )(
        tokens,
        down_query,
        down_latent,
        down_rotary.T,
        query_gain.reshape(1, -1),
        latent_gain.reshape(1, -1),
        up_query,
        up_query_rotary,
        up_key,
        up_value,
        out_weight,
        lane_rates,
        row_rates,
    )


def solution(mesh):
    return jax.shard_map(
        local,
        mesh=mesh,
        in_specs=(
            P(("sp", "tp"), None),
            P(),
            P(),
            P(),
            P(),
            P(),
            P(None, "tp"),
            P(None, "tp"),
            P(None, "tp"),
            P(None, "tp"),
            P("tp", None),
        ),
        out_specs=P(("sp", "tp"), None),
        check_vma=False,
    )
```

```python
import functools

import jax
import jax.numpy as jnp
import numpy as np
from jax import lax
from jax.experimental import pallas as pl
from jax.experimental.pallas import tpu as pltpu
from jax.sharding import PartitionSpec as P

NOPE = 128
ROPE = 64
VDIM = 128
HEADS = 4
OWN = 64
GROUP = 256
BLOCK = 288
VROWS = 144
RING = 4

rope_base = 500000.0
norm_eps = 1e-06
masked_score = -1e30

f32 = jnp.float32
bf16 = jnp.bfloat16
MESH = pl.DeviceIdType.MESH

COLS = 4
N_MSG = 102 + 6 * (COLS - 4)

STEPS = 9
UNIT_OA = ((0, 1, 0, 2, 1, -1, 2, 1, 2), (0, -1, 0, 1, -1, 0, 2, -1, 2))
UNIT_OB = ((0, 0, 1, 0, -1, -1, 1, 2, 2), (0, 0, -1, 1, 1, 2, -1, 2, 2))


def pick(index, values):
    out = jnp.int32(values[0])
    for i, v in enumerate(values[1:], 1):
        out = jnp.where(index == i, jnp.int32(v), out)
    return out


def once(condition):
    def run(body):
        def trip(_, carry):
            body()
            return carry

        lax.fori_loop(0, jnp.where(condition, 1, 0), trip, 0)

    return run


def mod4(v):
    return jnp.where(v < 0, v + 4, jnp.where(v > 3, v - 4, v))


def kernel(
    tokens_in,
    down_query,
    down_latent,
    down_rotary,
    query_gain,
    latent_gain,
    up_query,
    up_query_rotary,
    up_key,
    up_value,
    out_weight,
    lane_rates,
    row_rates,
    out,
    tokens,
    lrate,
    rrate,
    lgain,
    qgain,
    wdl,
    wdr,
    wdq,
    wuq,
    wur,
    wuk,
    wuv,
    wout,
    lat,
    ql,
    qt,
    uvt,
    kbuf,
    vbuf,
    acc,
    best,
    qfull,
    sbuf,
    tops,
    xsend,
    xrecv,
    ssend,
    srecv,
    pbuf,
    r1buf,
    dbuf,
    cbuf,
    crecv,
    local_sem,
    ssem,
    rsem,
):
    sp = lax.axis_index("sp")
    x = lax.axis_index("tp")
    c = lax.rem(sp, 2)
    m = sp // 2
    y = lax.rem(m, 4)
    z = m // 4
    first = c == 0
    a = jnp.where(first, y, z)
    b = jnp.where(first, z, y)
    stride_a = jnp.where(first, 2, 8)
    stride_b = jnp.where(first, 8, 2)

    def at(aa, bb):
        return {"sp": aa * stride_a + bb * stride_b + c, "tp": x}

    xp, xm, x2 = mod4(x + 1), mod4(x - 1), mod4(x + 2)
    dev_xp = {"sp": sp, "tp": xp}
    dev_xm = {"sp": sp, "tp": xm}
    dev_ap, dev_am = at(mod4(a + 1), b), at(mod4(a - 1), b)
    dev_bp, dev_bm = at(a, mod4(b + 1)), at(a, mod4(b - 1))
    dev_core = {"sp": sp + 1 - 2 * c, "tp": x}

    copies = []

    def copy_in(src, dst):
        copies.append(pltpu.make_async_copy(src, dst, local_sem.at[len(copies)]))
        copies[-1].start()
        return copies[-1]

    K4 = 1024
    quarters = [pl.ds(k * K4, K4) for k in range(4)]
    load_lanes = copy_in(lane_rates, lrate)
    load_tokens = copy_in(tokens_in, tokens)
    load_latent = [copy_in(down_latent.at[r], wdl.at[r]) for r in quarters]
    load_rotary = copy_in(down_rotary, wdr)
    load_rows = copy_in(row_rates, rrate)
    load_lgain = copy_in(latent_gain, lgain)
    load_qgain = copy_in(query_gain, qgain)
    load_query = [copy_in(down_query.at[r], wdq.at[r]) for r in quarters]
    load_rest = [
        copy_in(up_query, wuq),
        copy_in(up_query_rotary, wur),
        copy_in(up_key, wuk),
        copy_in(up_value, wuv),
        copy_in(out_weight, wout),
    ]

    barrier = pltpu.get_barrier_semaphore()
    for dev in (dev_xp, dev_xm, dev_ap, dev_am, dev_bp, dev_bm, dev_core):
        pl.semaphore_signal(barrier, inc=1, device_id=dev, device_id_type=MESH)

    send, recv = [], []

    def add(src, dst, landed, dev):
        i = len(send)
        for refs, done in ((src, dst), send), ((landed, landed), recv):
            done.append(
                pltpu.make_async_remote_copy(
                    src_ref=refs[0],
                    dst_ref=refs[1],
                    send_sem=ssem.at[i],
                    recv_sem=rsem.at[i],
                    device_id=dev,
                    device_id_type=MESH,
                )
            )
        return i

    def pair(up, up_landed, dev_up, down, down_landed, dev_down):
        return (
            add(lat.at[up], lat.at[up], lat.at[up_landed], dev_up),
            add(lat.at[down], lat.at[down], lat.at[down_landed], dev_down),
        )

    def group(oa, ob):
        return mod4(b + ob) * 4 + mod4(a + oa)

    def xs(o):
        return mod4(x + o)

    OFFS = (0, 1, -1, 2)
    s0 = group(0, 0)
    lo, hi = pl.ds(0, BLOCK // 2), pl.ds(BLOCK // 2, BLOCK // 2)

    def block(oa, ob, o):
        return group(oa, ob), xs(o)

    X1 = [
        pair((s0, x, up), (s0, xm, up), dev_xp, (s0, x, down), (s0, xp, down), dev_xm)
        for up, down in ((lo, hi), (hi, lo))
    ]
    X2 = pair((s0, xm, lo), (s0, x2, lo), dev_xp, (s0, xp, hi), (s0, x2, hi), dev_xm)
    A1, A2, B1, B2 = {}, {}, {}, {}
    for o in OFFS:
        A1[o] = pair(
            block(0, 0, o), block(-1, 0, o), dev_ap, block(0, 0, o), block(1, 0, o), dev_am
        )
        for oa in OFFS:
            B1[oa, o] = pair(
                block(oa, 0, o), block(oa, -1, o), dev_bp, block(oa, 0, o), block(oa, 1, o), dev_bm
            )
    for n, (up, down) in enumerate(((0, 1), (2, -1))):
        A2[n] = pair(
            block(-1, 0, up), block(2, 0, up), dev_ap, block(1, 0, down), block(2, 0, down), dev_am
        )
        for oa in OFFS:
            B2[oa, n] = pair(
                block(oa, -1, up),
                block(oa, 2, up),
                dev_bp,
                block(oa, 1, down),
                block(oa, 2, down),
                dev_bm,
            )
    q_lo, q_hi = pl.ds(0, OWN // 2), pl.ds(OWN // 2, OWN // 2)
    Q1 = [
        (
            add(ql.at[x, up], ql.at[x, up], ql.at[xm, up], dev_xp),
            add(ql.at[x, down], ql.at[x, down], ql.at[xp, down], dev_xm),
        )
        for up, down in ((q_lo, q_hi), (q_hi, q_lo))
    ]
    Q2 = (
        add(ql.at[xm, q_lo], ql.at[xm, q_lo], ql.at[x2, q_lo], dev_xp),
        add(ql.at[xp, q_hi], ql.at[xp, q_hi], ql.at[x2, q_hi], dev_xm),
    )
    QX = (add(qt.at[c], qt.at[c], qt.at[1 - c], dev_core),)
    OX = [(add(xsend.at[h], xrecv.at[h], xrecv.at[h], dev_core),) for h in range(HEADS)]
    OS = (add(ssend, srecv, srecv, dev_core),)

    def start(*groups):
        for ids in groups:
            for i in ids:
                send[i].start()

    def arrived(*groups):
        for ids in groups:
            for i in ids:
                recv[i].wait_recv()

    def norm_rows(values, gain):
        return values * lax.rsqrt(jnp.mean(values * values, axis=-1, keepdims=True) + norm_eps) * gain

    load_lanes.wait()
    spot = lax.broadcasted_iota(jnp.int32, (OWN, 128), 0) + (sp * RING + x) * OWN
    angles = spot.astype(f32) * lrate[...]
    lane = lax.broadcasted_iota(jnp.int32, (OWN, 128), 1)
    key_cos = jnp.cos(angles)
    key_sin = jnp.sin(angles) * jnp.where(lax.rem(lane, 64) < 32, -1.0, 1.0)
    load_tokens.wait()
    latent = jnp.zeros((OWN, 512), f32)
    for k in range(4):
        load_latent[k].wait()
        cols = slice(k * K4, (k + 1) * K4)
        latent = latent + jnp.dot(tokens[:, cols], wdl[cols, :], preferred_element_type=f32)
    load_lgain.wait()
    latent = norm_rows(latent, lgain[...]).astype(bf16)
    for t in range(4):
        lat[s0, x, t * OWN : (t + 1) * OWN, :] = latent[:, t * 128 : (t + 1) * 128]
    load_rotary.wait()
    turned = lax.dot_general(
        tokens[...], wdr[...], (((1,), (1,)), ((), ())), preferred_element_type=f32
    )
    turned = jnp.concatenate([turned, turned], axis=-1)
    turned = turned * key_cos + pltpu.roll(turned, 32, 1) * key_sin
    lat[s0, x, 256:288, :] = jnp.where(lane[:32] < 64, turned[:32], turned[32:]).astype(bf16)
    pl.semaphore_wait(barrier, 7)
    start(*X1, A1[0], B1[0, 0])

    query = jnp.zeros((OWN, 1024), f32)
    for k in range(4):
        load_query[k].wait()
        cols = slice(k * K4, (k + 1) * K4)
        query = query + jnp.dot(tokens[:, cols], wdq[cols, :], preferred_element_type=f32)
    load_qgain.wait()
    ql[x] = norm_rows(query, qgain[...]).astype(bf16)
    start(*Q1)
    arrived(X1[0])
    start(X2)
    arrived(X1[1])
    start(A1[1], A1[-1], B1[0, 1], B1[0, -1])
    load_rows.wait()
    for load in load_rest:
        load.wait()
    uvt[...] = jnp.transpose(wuv[...].astype(f32)).astype(bf16)
    for h in range(HEADS):
        vbuf[h, VDIM:VROWS, :] = jnp.ones((VROWS - VDIM, 2 * GROUP), bf16)
    acc[...] = jnp.zeros_like(acc)
    best[...] = jnp.full(best.shape, masked_score, f32)
    spot = lax.broadcasted_iota(jnp.int32, (32, GROUP), 1) + sp * GROUP
    angles = spot.astype(f32) * rrate[...]
    cosine, sine = jnp.cos(angles), jnp.sin(angles)
    arrived(A1[0])
    start(B1[1, 0], B1[-1, 0])
    arrived(Q1[0])
    start(Q2)
    arrived(A1[1])
    start(A2[0], B1[1, 1], B1[-1, 1])
    arrived(B1[0, 0], B1[0, 1])
    start(B2[0, 0])
    arrived(X2)
    start(A1[2], B1[0, 2])
    arrived(A1[-1])
    start(B1[1, -1], B1[-1, -1])
    arrived(Q1[1], Q2)
    factor = (NOPE + ROPE) ** (-0.5) * 1.4426950408889634
    rows = ql[...].reshape(GROUP, 1024)
    plain = jnp.dot(rows, wuq[...], preferred_element_type=f32) * factor
    qt[c, 0 : HEADS * NOPE, :] = jnp.transpose(plain).astype(bf16)
    turned = jnp.transpose(jnp.dot(rows, wur[...], preferred_element_type=f32) * factor)
    for h in range(HEADS):
        one = turned[h * ROPE : h * ROPE + 32]
        two = turned[h * ROPE + 32 : (h + 1) * ROPE]
        at_row = HEADS * NOPE + h * ROPE
        qt[c, at_row : at_row + 32, :] = (one * cosine - two * sine).astype(bf16)
        qt[c, at_row + 32 : at_row + 64, :] = (two * cosine + one * sine).astype(bf16)
    start(QX)

    def set_of(u, n):
        aa, bb = mod4(a + pick(u, UNIT_OA[n])), mod4(b + pick(u, UNIT_OB[n]))
        spot = jnp.where(first, bb * 4 + aa, aa * 4 + bb)
        seen = spot <= m
        if n == 1:
            seen = jnp.logical_and(seen, jnp.logical_and(u > 0, u < STEPS - 1))
        return bb * 4 + aa, spot, seen

    def expand(sets):
        keys = len(sets) * GROUP
        parts, rots = [], []
        for s in sets:
            tiles = [
                lat[s, :, t * OWN : (t + 1) * OWN, :].reshape(GROUP, 128) for t in range(4)
            ]
            parts.append(jnp.concatenate(tiles, axis=1))
            packed = lat[s, :, 256:288, :]
            swapped = pltpu.roll(packed.reshape(128, 128).astype(f32), 64, 1).astype(bf16)
            rots.append(
                jnp.concatenate([packed, swapped.reshape(4, 32, 128)], axis=1).reshape(GROUP, 128)
            )
        latents = jnp.concatenate(parts, axis=0)
        kbuf[:keys, 0:512] = jnp.dot(latents, wuk[...], preferred_element_type=f32).astype(bf16)
        kbuf[:keys, 512:640] = jnp.concatenate(rots, axis=0)
        values = lax.dot_general(
            uvt[...], latents, (((1,), (1,)), ((), ())), preferred_element_type=f32
        ).astype(bf16)
        for h in range(HEADS):
            vbuf[h, 0:VDIM, :keys] = values[h * VDIM : (h + 1) * VDIM]

    def attend(keys, spot):
        def score(h):
            key = jnp.concatenate(
                [kbuf[:keys, h * NOPE : (h + 1) * NOPE], kbuf[:keys, 512:640]], axis=1
            )
            scores = jnp.dot(key, qfull[h], preferred_element_type=f32)
            if spot is not None:
                row = lax.broadcasted_iota(jnp.int32, (keys, 2 * GROUP), 0)
                col = lax.broadcasted_iota(jnp.int32, (keys, 2 * GROUP), 1)
                ahead = (2 * (spot - m) + c) * GROUP
                scores = jnp.where(row + ahead <= col, scores, masked_score)
            sbuf[h % 2, :keys] = scores
            tops[h % 2] = jnp.max(scores, axis=0, keepdims=True)

        score(0)
        for h in range(HEADS):
            if h + 1 < HEADS:
                score(h + 1)
            old = best[h]
            new = jnp.maximum(old, tops[h % 2])
            weights = jnp.exp2(sbuf[h % 2, :keys] - new).astype(bf16)
            best[h] = new
            acc[h] = acc[h] * jnp.exp2(old - new) + jnp.dot(
                vbuf[h, :, :keys], weights, preferred_element_type=f32
            )

    arrived(A2[0])
    start(B1[2, 0], B1[2, 1])
    arrived(B1[1, 0], B1[1, 1])
    start(B2[1, 0])
    def far_seen(oa):
        aa, bb = mod4(a + oa), mod4(b + 2)
        return jnp.where(first, bb * 4 + aa, aa * 4 + bb) <= m

    def step(u, carry):

        @once(u == 1)
        def _():
            arrived(A1[2])
            start(A2[1], B1[1, 2], B1[-1, 2])
            arrived(B1[-1, 0], B1[-1, 1])
            start(B2[-1, 0])

        @once(u == 2)
        def _():
            arrived(B1[0, -1], B1[0, 2])
            start(B2[0, 1])

        @once(u == 3)
        def _():
            arrived(A2[1])
            start(B1[2, -1], B1[2, 2])
            arrived(B1[1, -1], B1[1, 2])
            start(B2[1, 1])

        @once(u == 4)
        def _():
            arrived(B1[2, 0], B1[2, 1])
            start(B2[2, 0])
            arrived(B1[-1, -1], B1[-1, 2])
            start(B2[-1, 1])

        for oa, when in ((0, 5), (1, 7), (-1, 7), (2, 8)):

            @once(jnp.logical_and(u == when, far_seen(oa)))
            def _(oa=oa):
                arrived(B2[oa, 0], B2[oa, 1])

        set_one, spot_one, seen_one = set_of(u, 0)
        set_two, spot_two, seen_two = set_of(u, 1)
        two = jnp.logical_and(seen_one, seen_two)
        one = jnp.logical_and(jnp.logical_or(seen_one, seen_two), jnp.logical_not(two))
        single = jnp.where(seen_one, set_one, set_two)
        spot = jnp.where(seen_one, spot_one, spot_two)

        @pl.when(two)
        def _():
            expand((set_one, set_two))

        @pl.when(one)
        def _():
            expand((single,))


        @once(u == 0)
        def _():
            arrived(QX)
            for h in range(HEADS):
                for j in range(2):
                    cols = slice(j * GROUP, (j + 1) * GROUP)
                    qfull[h, 0:NOPE, cols] = qt[j, h * NOPE : (h + 1) * NOPE, :]
                    at_row = HEADS * NOPE + h * ROPE
                    qfull[h, NOPE : NOPE + ROPE, cols] = qt[j, at_row : at_row + ROPE, :]
                qfull[h, NOPE + ROPE :, :] = jnp.zeros((ROPE, 2 * GROUP), bf16)

        @once(u == 5)
        def _():
            arrived(B1[2, -1], B1[2, 2])
            start(B2[2, 1])


        @pl.when(two)
        def _():
            attend(2 * GROUP, None)

        @pl.when(one)
        def _():
            attend(GROUP, spot)

        return carry

    lax.fori_loop(0, STEPS, step, 0)

    mine_at = pl.ds(pl.multiple_of(c * GROUP, GROUP), GROUP)
    other_at = pl.ds(pl.multiple_of((1 - c) * GROUP, GROUP), GROUP)
    for h in range(HEADS):
        ssend[h, 0:1, :] = best[h, :, other_at]
        ssend[h, 1:2, :] = acc[h, 128:129, other_at]
    start(OS)
    for h in range(HEADS):
        xsend[h] = acc[h, 0:128, other_at].astype(bf16)
        start(OX[h])
    arrived(OS)
    heads = []
    for h in range(HEADS):
        mine, theirs = best[h, :, mine_at], srecv[h, 0:1, :]
        top = jnp.maximum(mine, theirs)
        w_mine, w_theirs = jnp.exp2(mine - top), jnp.exp2(theirs - top)
        total = acc[h, 128:129, mine_at] * w_mine + srecv[h, 1:2, :] * w_theirs
        arrived(OX[h])
        summed = acc[h, 0:128, mine_at] * w_mine + xrecv[h].astype(f32) * w_theirs
        heads.append(jnp.transpose(summed / total).astype(bf16))
    attended = jnp.concatenate(heads, axis=1)

    WIDE = 4096 // COLS
    top, low = pl.ds(0, 32), pl.ds(32, 32)
    R1, RD, RC = [], [], []
    for k in range(COLS):
        cols = pl.ds(k * WIDE, WIDE)

        def both(to_up, to_down, ref):
            up, down = ref.at[0, :, cols], ref.at[1, :, cols]
            return add(to_up, up, up, dev_xp), add(to_down, down, down, dev_xm)

        R1.append(both(pbuf.at[x2, top, cols], pbuf.at[x2, low, cols], r1buf))
        RD.append(both(pbuf.at[xp, low, cols], pbuf.at[xm, top, cols], dbuf))
        RC.append(both(cbuf.at[0, :, cols], cbuf.at[1, :, cols], crecv))
    assert len(send) == N_MSG, len(send)
    for k in range(COLS):
        cols = slice(k * WIDE, (k + 1) * WIDE)
        part = jnp.dot(attended, wout[:, cols], preferred_element_type=f32).astype(bf16)
        pbuf[:, :, cols] = part.reshape(4, OWN, WIDE)
        start(R1[k])
    start(*RD)
    for k in range(COLS):
        cols = slice(k * WIDE, (k + 1) * WIDE)
        arrived(R1[k])
        cbuf[0, :, cols] = (
            r1buf[0, :, cols].astype(f32) + pbuf[xp, 0:32, cols].astype(f32)
        ).astype(bf16)
        cbuf[1, :, cols] = (
            r1buf[1, :, cols].astype(f32) + pbuf[xm, 32:64, cols].astype(f32)
        ).astype(bf16)
        start(RC[k])
    for k in range(COLS):
        cols = slice(k * WIDE, (k + 1) * WIDE)
        arrived(RD[k], RC[k])
        out[0:32, cols] = (
            pbuf[x, 0:32, cols].astype(f32)
            + crecv[0, :, cols].astype(f32)
            + dbuf[1, :, cols].astype(f32)
        ).astype(bf16)
        out[32:64, cols] = (
            pbuf[x, 32:64, cols].astype(f32)
            + crecv[1, :, cols].astype(f32)
            + dbuf[0, :, cols].astype(f32)
        ).astype(bf16)
    for oa in OFFS:

        @pl.when(jnp.logical_not(far_seen(oa)))
        def _(oa=oa):
            arrived(B2[oa, 0], B2[oa, 1])

    for i in range(N_MSG):
        send[i].wait_send()


def local(
    tokens,
    down_query,
    down_latent,
    down_rotary,
    query_gain,
    latent_gain,
    up_query,
    up_query_rotary,
    up_key,
    up_value,
    out_weight,
):
    rates = (rope_base ** (-np.arange(0, ROPE, 2) / ROPE)).astype(np.float32)
    lane_rates = jnp.asarray(np.tile(rates, 4)[None, :])
    row_rates = jnp.asarray(np.repeat(rates[:, None], GROUP, axis=1))
    vmem = pl.BlockSpec(memory_space=pltpu.VMEM)
    hbm = pl.BlockSpec(memory_space=pl.ANY)
    return pl.pallas_call(
        kernel,
        out_shape=pltpu.VMEM((OWN, 4096), bf16),
        in_specs=[hbm] * 13,
        out_specs=vmem,
        scratch_shapes=[
            pltpu.VMEM((OWN, 4096), bf16),
            pltpu.VMEM((1, 128), f32),
            pltpu.VMEM((32, GROUP), f32),
            pltpu.VMEM((1, 512), f32),
            pltpu.VMEM((1, 1024), f32),
            pltpu.VMEM((4096, 512), bf16),
            pltpu.VMEM((64, 4096), bf16),
            pltpu.VMEM((4096, 1024), bf16),
            pltpu.VMEM((1024, 512), bf16),
            pltpu.VMEM((1024, 256), bf16),
            pltpu.VMEM((512, 512), bf16),
            pltpu.VMEM((512, 512), bf16),
            pltpu.VMEM((512, 4096), bf16),
            pltpu.VMEM((16, 4, BLOCK, 128), bf16),
            pltpu.VMEM((4, OWN, 1024), bf16),
            pltpu.VMEM((2, HEADS * (NOPE + ROPE), GROUP), bf16),
            pltpu.VMEM((512, 512), bf16),
            pltpu.VMEM((2 * GROUP, 640), bf16),
            pltpu.VMEM((HEADS, VROWS, 2 * GROUP), bf16),
            pltpu.VMEM((HEADS, VROWS, 2 * GROUP), f32),
            pltpu.VMEM((HEADS, 1, 2 * GROUP), f32),
            pltpu.VMEM((HEADS, 256, 2 * GROUP), bf16),
            pltpu.VMEM((2, 2 * GROUP, 2 * GROUP), f32),
            pltpu.VMEM((2, 1, 2 * GROUP), f32),
            pltpu.VMEM((HEADS, VDIM, GROUP), bf16),
            pltpu.VMEM((HEADS, VDIM, GROUP), bf16),
            pltpu.VMEM((HEADS, 8, GROUP), f32),
            pltpu.VMEM((HEADS, 8, GROUP), f32),
            pltpu.VMEM((4, OWN, 4096), bf16),
            pltpu.VMEM((2, 32, 4096), bf16),
            pltpu.VMEM((2, 32, 4096), bf16),
            pltpu.VMEM((2, 32, 4096), bf16),
            pltpu.VMEM((2, 32, 4096), bf16),
            pltpu.SemaphoreType.DMA((19,)),
            pltpu.SemaphoreType.DMA((N_MSG,)),
            pltpu.SemaphoreType.DMA((N_MSG,)),
        ],
        compiler_params=pltpu.CompilerParams(
            collective_id=0, has_side_effects=True, vmem_limit_bytes=62 * 1024 * 1024
        ),
    )(
        tokens,
        down_query,
        down_latent,
        down_rotary.T,
        query_gain.reshape(1, -1),
        latent_gain.reshape(1, -1),
        up_query,
        up_query_rotary,
        up_key,
        up_value,
        out_weight,
        lane_rates,
        row_rates,
    )


def solution(mesh):
    return jax.shard_map(
        local,
        mesh=mesh,
        in_specs=(
            P(("sp", "tp"), None),
            P(),
            P(),
            P(),
            P(),
            P(),
            P(None, "tp"),
            P(None, "tp"),
            P(None, "tp"),
            P(None, "tp"),
            P("tp", None),
        ),
        out_specs=P(("sp", "tp"), None),
        check_vma=False,
    )
```

```python
import functools

import jax
import jax.numpy as jnp
import numpy as np
from jax import lax
from jax.experimental import pallas as pl
from jax.experimental.pallas import tpu as pltpu
from jax.sharding import PartitionSpec as P

NOPE = 128
ROPE = 64
VDIM = 128
HEADS = 4
OWN = 64
GROUP = 256
BLOCK = 288
VROWS = 144
RING = 4

rope_base = 500000.0
norm_eps = 1e-06
masked_score = -1e30

f32 = jnp.float32
bf16 = jnp.bfloat16
MESH = pl.DeviceIdType.MESH

COLS = 4
N_MSG = 102 + 6 * (COLS - 4)

STEPS = 9
UNIT_OA = ((0, 1, 0, 2, 1, -1, 2, 1, 2), (0, -1, 0, 1, -1, 0, 2, -1, 2))
UNIT_OB = ((0, 0, 1, 0, -1, -1, 1, 2, 2), (0, 0, -1, 1, 1, 2, -1, 2, 2))


def pick(index, values):
    out = jnp.int32(values[0])
    for i, v in enumerate(values[1:], 1):
        out = jnp.where(index == i, jnp.int32(v), out)
    return out


def once(condition):
    def run(body):
        def trip(_, carry):
            body()
            return carry

        lax.fori_loop(0, jnp.where(condition, 1, 0), trip, 0)

    return run


def mod4(v):
    return jnp.where(v < 0, v + 4, jnp.where(v > 3, v - 4, v))


def kernel(
    tokens_in,
    down_query,
    down_latent,
    down_rotary,
    query_gain,
    latent_gain,
    up_query,
    up_query_rotary,
    up_key,
    up_value,
    out_weight,
    lane_rates,
    row_rates,
    out,
    tokens,
    lrate,
    rrate,
    lgain,
    qgain,
    wdl,
    wdr,
    wdq,
    wuq,
    wur,
    wuk,
    wuv,
    wout,
    lat,
    ql,
    qt,
    uvt,
    kbuf,
    vbuf,
    acc,
    best,
    qfull,
    sbuf,
    tops,
    xsend,
    xrecv,
    ssend,
    srecv,
    pbuf,
    r1buf,
    dbuf,
    cbuf,
    crecv,
    local_sem,
    ssem,
    rsem,
):
    sp = lax.axis_index("sp")
    x = lax.axis_index("tp")
    c = lax.rem(sp, 2)
    m = sp // 2
    y = lax.rem(m, 4)
    z = m // 4
    first = c == 0
    a = jnp.where(first, y, z)
    b = jnp.where(first, z, y)
    stride_a = jnp.where(first, 2, 8)
    stride_b = jnp.where(first, 8, 2)

    def at(aa, bb):
        return {"sp": aa * stride_a + bb * stride_b + c, "tp": x}

    xp, xm, x2 = mod4(x + 1), mod4(x - 1), mod4(x + 2)
    dev_xp = {"sp": sp, "tp": xp}
    dev_xm = {"sp": sp, "tp": xm}
    dev_ap, dev_am = at(mod4(a + 1), b), at(mod4(a - 1), b)
    dev_bp, dev_bm = at(a, mod4(b + 1)), at(a, mod4(b - 1))
    dev_core = {"sp": sp + 1 - 2 * c, "tp": x}

    copies = []

    def copy_in(src, dst):
        copies.append(pltpu.make_async_copy(src, dst, local_sem.at[len(copies)]))
        copies[-1].start()
        return copies[-1]

    K4 = 1024
    quarters = [pl.ds(k * K4, K4) for k in range(4)]
    load_lanes = copy_in(lane_rates, lrate)
    load_tokens = copy_in(tokens_in, tokens)
    load_latent = [copy_in(down_latent.at[r], wdl.at[r]) for r in quarters]
    load_rotary = copy_in(down_rotary, wdr)
    load_rows = copy_in(row_rates, rrate)
    load_lgain = copy_in(latent_gain, lgain)
    load_qgain = copy_in(query_gain, qgain)
    load_query = [copy_in(down_query.at[r], wdq.at[r]) for r in quarters]
    load_rest = [
        copy_in(up_query, wuq),
        copy_in(up_query_rotary, wur),
        copy_in(up_key, wuk),
        copy_in(up_value, wuv),
        copy_in(out_weight, wout),
    ]

    barrier = pltpu.get_barrier_semaphore()
    for dev in (dev_xp, dev_xm, dev_ap, dev_am, dev_bp, dev_bm, dev_core):
        pl.semaphore_signal(barrier, inc=1, device_id=dev, device_id_type=MESH)

    send, recv = [], []

    def add(src, dst, landed, dev):
        i = len(send)
        for refs, done in ((src, dst), send), ((landed, landed), recv):
            done.append(
                pltpu.make_async_remote_copy(
                    src_ref=refs[0],
                    dst_ref=refs[1],
                    send_sem=ssem.at[i],
                    recv_sem=rsem.at[i],
                    device_id=dev,
                    device_id_type=MESH,
                )
            )
        return i

    def pair(up, up_landed, dev_up, down, down_landed, dev_down):
        return (
            add(lat.at[up], lat.at[up], lat.at[up_landed], dev_up),
            add(lat.at[down], lat.at[down], lat.at[down_landed], dev_down),
        )

    def group(oa, ob):
        return mod4(b + ob) * 4 + mod4(a + oa)

    def xs(o):
        return mod4(x + o)

    OFFS = (0, 1, -1, 2)
    s0 = group(0, 0)
    lo, hi = pl.ds(0, BLOCK // 2), pl.ds(BLOCK // 2, BLOCK // 2)

    def block(oa, ob, o):
        return group(oa, ob), xs(o)

    X1 = [
        pair((s0, x, up), (s0, xm, up), dev_xp, (s0, x, down), (s0, xp, down), dev_xm)
        for up, down in ((lo, hi), (hi, lo))
    ]
    X2 = pair((s0, xm, lo), (s0, x2, lo), dev_xp, (s0, xp, hi), (s0, x2, hi), dev_xm)
    A1, A2, B1, B2 = {}, {}, {}, {}
    for o in OFFS:
        A1[o] = pair(
            block(0, 0, o), block(-1, 0, o), dev_ap, block(0, 0, o), block(1, 0, o), dev_am
        )
        for oa in OFFS:
            B1[oa, o] = pair(
                block(oa, 0, o), block(oa, -1, o), dev_bp, block(oa, 0, o), block(oa, 1, o), dev_bm
            )
    for n, (up, down) in enumerate(((0, 1), (2, -1))):
        A2[n] = pair(
            block(-1, 0, up), block(2, 0, up), dev_ap, block(1, 0, down), block(2, 0, down), dev_am
        )
        for oa in OFFS:
            B2[oa, n] = pair(
                block(oa, -1, up),
                block(oa, 2, up),
                dev_bp,
                block(oa, 1, down),
                block(oa, 2, down),
                dev_bm,
            )
    q_lo, q_hi = pl.ds(0, OWN // 2), pl.ds(OWN // 2, OWN // 2)
    Q1 = [
        (
            add(ql.at[x, up], ql.at[x, up], ql.at[xm, up], dev_xp),
            add(ql.at[x, down], ql.at[x, down], ql.at[xp, down], dev_xm),
        )
        for up, down in ((q_lo, q_hi), (q_hi, q_lo))
    ]
    Q2 = (
        add(ql.at[xm, q_lo], ql.at[xm, q_lo], ql.at[x2, q_lo], dev_xp),
        add(ql.at[xp, q_hi], ql.at[xp, q_hi], ql.at[x2, q_hi], dev_xm),
    )
    QX = (add(qt.at[c], qt.at[c], qt.at[1 - c], dev_core),)
    OX = [(add(xsend.at[h], xrecv.at[h], xrecv.at[h], dev_core),) for h in range(HEADS)]
    OS = (add(ssend, srecv, srecv, dev_core),)

    def start(*groups):
        for ids in groups:
            for i in ids:
                send[i].start()

    def arrived(*groups):
        for ids in groups:
            for i in ids:
                recv[i].wait_recv()

    def norm_rows(values, gain):
        return values * lax.rsqrt(jnp.mean(values * values, axis=-1, keepdims=True) + norm_eps) * gain

    load_lanes.wait()
    spot = lax.broadcasted_iota(jnp.int32, (OWN, 128), 0) + (sp * RING + x) * OWN
    angles = spot.astype(f32) * lrate[...]
    lane = lax.broadcasted_iota(jnp.int32, (OWN, 128), 1)
    key_cos = jnp.cos(angles)
    key_sin = jnp.sin(angles) * jnp.where(lax.rem(lane, 64) < 32, -1.0, 1.0)
    load_tokens.wait()
    latent = jnp.zeros((OWN, 512), f32)
    for k in range(4):
        load_latent[k].wait()
        cols = slice(k * K4, (k + 1) * K4)
        latent = latent + jnp.dot(tokens[:, cols], wdl[cols, :], preferred_element_type=f32)
    load_lgain.wait()
    latent = norm_rows(latent, lgain[...]).astype(bf16)
    for t in range(4):
        lat[s0, x, t * OWN : (t + 1) * OWN, :] = latent[:, t * 128 : (t + 1) * 128]
    load_rotary.wait()
    turned = lax.dot_general(
        tokens[...], wdr[...], (((1,), (1,)), ((), ())), preferred_element_type=f32
    )
    turned = jnp.concatenate([turned, turned], axis=-1)
    turned = turned * key_cos + pltpu.roll(turned, 32, 1) * key_sin
    lat[s0, x, 256:288, :] = jnp.where(lane[:32] < 64, turned[:32], turned[32:]).astype(bf16)
    pl.semaphore_wait(barrier, 7)
    start(*X1, A1[0], B1[0, 0])

    query = jnp.zeros((OWN, 1024), f32)
    for k in range(4):
        load_query[k].wait()
        cols = slice(k * K4, (k + 1) * K4)
        query = query + jnp.dot(tokens[:, cols], wdq[cols, :], preferred_element_type=f32)
    load_qgain.wait()
    ql[x] = norm_rows(query, qgain[...]).astype(bf16)
    start(*Q1)
    arrived(X1[0])
    start(X2)
    arrived(X1[1])
    start(A1[1], A1[-1], B1[0, 1], B1[0, -1])
    load_rows.wait()
    for load in load_rest:
        load.wait()
    uvt[...] = jnp.transpose(wuv[...].astype(f32)).astype(bf16)
    for h in range(HEADS):
        vbuf[h, VDIM:VROWS, :] = jnp.ones((VROWS - VDIM, 2 * GROUP), bf16)
    acc[...] = jnp.zeros_like(acc)
    best[...] = jnp.full(best.shape, masked_score, f32)
    spot = lax.broadcasted_iota(jnp.int32, (32, GROUP), 1) + sp * GROUP
    angles = spot.astype(f32) * rrate[...]
    cosine, sine = jnp.cos(angles), jnp.sin(angles)
    arrived(A1[0])
    start(B1[1, 0], B1[-1, 0])
    arrived(Q1[0])
    start(Q2)
    arrived(A1[1])
    start(A2[0], B1[1, 1], B1[-1, 1])
    arrived(B1[0, 0], B1[0, 1])
    start(B2[0, 0])
    arrived(X2)
    start(A1[2], B1[0, 2])
    arrived(A1[-1])
    start(B1[1, -1], B1[-1, -1])
    arrived(Q1[1], Q2)
    factor = (NOPE + ROPE) ** (-0.5) * 1.4426950408889634
    rows = ql[...].reshape(GROUP, 1024)
    plain = jnp.dot(rows, wuq[...], preferred_element_type=f32) * factor
    qt[c, 0 : HEADS * NOPE, :] = jnp.transpose(plain).astype(bf16)
    turned = jnp.transpose(jnp.dot(rows, wur[...], preferred_element_type=f32) * factor)
    for h in range(HEADS):
        one = turned[h * ROPE : h * ROPE + 32]
        two = turned[h * ROPE + 32 : (h + 1) * ROPE]
        at_row = HEADS * NOPE + h * ROPE
        qt[c, at_row : at_row + 32, :] = (one * cosine - two * sine).astype(bf16)
        qt[c, at_row + 32 : at_row + 64, :] = (two * cosine + one * sine).astype(bf16)
    start(QX)

    def set_of(u, n):
        aa, bb = mod4(a + pick(u, UNIT_OA[n])), mod4(b + pick(u, UNIT_OB[n]))
        spot = jnp.where(first, bb * 4 + aa, aa * 4 + bb)
        seen = spot <= m
        if n == 1:
            seen = jnp.logical_and(seen, jnp.logical_and(u > 0, u < STEPS - 1))
        return bb * 4 + aa, spot, seen

    def attend(sets, spot):
        keys = len(sets) * GROUP
        parts, rots = [], []
        for s in sets:
            tiles = [
                lat[s, :, t * OWN : (t + 1) * OWN, :].reshape(GROUP, 128) for t in range(4)
            ]
            parts.append(jnp.concatenate(tiles, axis=1))
            packed = lat[s, :, 256:288, :]
            swapped = pltpu.roll(packed.reshape(128, 128).astype(f32), 64, 1).astype(bf16)
            rots.append(
                jnp.concatenate([packed, swapped.reshape(4, 32, 128)], axis=1).reshape(GROUP, 128)
            )
        latents = jnp.concatenate(parts, axis=0)
        kbuf[:keys, 0:512] = jnp.dot(latents, wuk[...], preferred_element_type=f32).astype(bf16)
        kbuf[:keys, 512:640] = jnp.concatenate(rots, axis=0)

        def score(h):
            key = jnp.concatenate(
                [kbuf[:keys, h * NOPE : (h + 1) * NOPE], kbuf[:keys, 512:640]], axis=1
            )
            scores = jnp.dot(key, qfull[h], preferred_element_type=f32)
            if spot is not None:
                row = lax.broadcasted_iota(jnp.int32, (keys, 2 * GROUP), 0)
                col = lax.broadcasted_iota(jnp.int32, (keys, 2 * GROUP), 1)
                ahead = (2 * (spot - m) + c) * GROUP
                scores = jnp.where(row + ahead <= col, scores, masked_score)
            sbuf[h % 2, :keys] = scores
            tops[h % 2] = jnp.max(scores, axis=0, keepdims=True)

        score(0)
        values = lax.dot_general(
            uvt[...], latents, (((1,), (1,)), ((), ())), preferred_element_type=f32
        ).astype(bf16)
        for h in range(HEADS):
            vbuf[h, 0:VDIM, :keys] = values[h * VDIM : (h + 1) * VDIM]
        for h in range(HEADS):
            if h + 1 < HEADS:
                score(h + 1)
            old = best[h]
            new = jnp.maximum(old, tops[h % 2])
            weights = jnp.exp2(sbuf[h % 2, :keys] - new).astype(bf16)
            best[h] = new
            acc[h] = acc[h] * jnp.exp2(old - new) + jnp.dot(
                vbuf[h, :, :keys], weights, preferred_element_type=f32
            )

    arrived(A2[0])
    start(B1[2, 0], B1[2, 1])
    arrived(B1[1, 0], B1[1, 1])
    start(B2[1, 0])
    arrived(QX)
    for h in range(HEADS):
        for j in range(2):
            cols = slice(j * GROUP, (j + 1) * GROUP)
            qfull[h, 0:NOPE, cols] = qt[j, h * NOPE : (h + 1) * NOPE, :]
            at_row = HEADS * NOPE + h * ROPE
            qfull[h, NOPE : NOPE + ROPE, cols] = qt[j, at_row : at_row + ROPE, :]
        qfull[h, NOPE + ROPE :, :] = jnp.zeros((ROPE, 2 * GROUP), bf16)

    def far_seen(oa):
        aa, bb = mod4(a + oa), mod4(b + 2)
        return jnp.where(first, bb * 4 + aa, aa * 4 + bb) <= m

    def step(u, carry):

        @once(u == 1)
        def _():
            arrived(A1[2])
            start(A2[1], B1[1, 2], B1[-1, 2])
            arrived(B1[-1, 0], B1[-1, 1])
            start(B2[-1, 0])

        @once(u == 2)
        def _():
            arrived(B1[0, -1], B1[0, 2])
            start(B2[0, 1])

        @once(u == 3)
        def _():
            arrived(A2[1])
            start(B1[2, -1], B1[2, 2])
            arrived(B1[1, -1], B1[1, 2])
            start(B2[1, 1])

        @once(u == 4)
        def _():
            arrived(B1[2, 0], B1[2, 1])
            start(B2[2, 0])
            arrived(B1[-1, -1], B1[-1, 2])
            start(B2[-1, 1])

        @once(u == 6)
        def _():
            arrived(B1[2, -1], B1[2, 2])
            start(B2[2, 1])

        for oa, when in ((0, 5), (1, 7), (-1, 7), (2, 8)):

            @once(jnp.logical_and(u == when, far_seen(oa)))
            def _(oa=oa):
                arrived(B2[oa, 0], B2[oa, 1])

        set_one, spot_one, seen_one = set_of(u, 0)
        set_two, spot_two, seen_two = set_of(u, 1)
        two = jnp.logical_and(seen_one, seen_two)
        one = jnp.logical_and(jnp.logical_or(seen_one, seen_two), jnp.logical_not(two))
        single = jnp.where(seen_one, set_one, set_two)
        spot = jnp.where(seen_one, spot_one, spot_two)

        @pl.when(two)
        def _():
            attend((set_one, set_two), None)

        @pl.when(one)
        def _():
            attend((single,), spot)

        return carry

    lax.fori_loop(0, STEPS, step, 0)

    mine_at = pl.ds(pl.multiple_of(c * GROUP, GROUP), GROUP)
    other_at = pl.ds(pl.multiple_of((1 - c) * GROUP, GROUP), GROUP)
    for h in range(HEADS):
        ssend[h, 0:1, :] = best[h, :, other_at]
        ssend[h, 1:2, :] = acc[h, 128:129, other_at]
    start(OS)
    for h in range(HEADS):
        xsend[h] = acc[h, 0:128, other_at].astype(bf16)
        start(OX[h])
    arrived(OS)
    heads = []
    for h in range(HEADS):
        mine, theirs = best[h, :, mine_at], srecv[h, 0:1, :]
        top = jnp.maximum(mine, theirs)
        w_mine, w_theirs = jnp.exp2(mine - top), jnp.exp2(theirs - top)
        total = acc[h, 128:129, mine_at] * w_mine + srecv[h, 1:2, :] * w_theirs
        arrived(OX[h])
        summed = acc[h, 0:128, mine_at] * w_mine + xrecv[h].astype(f32) * w_theirs
        heads.append(jnp.transpose(summed / total).astype(bf16))
    attended = jnp.concatenate(heads, axis=1)

    WIDE = 4096 // COLS
    top, low = pl.ds(0, 32), pl.ds(32, 32)
    R1, RD, RC = [], [], []
    for k in range(COLS):
        cols = pl.ds(k * WIDE, WIDE)

        def both(to_up, to_down, ref):
            up, down = ref.at[0, :, cols], ref.at[1, :, cols]
            return add(to_up, up, up, dev_xp), add(to_down, down, down, dev_xm)

        R1.append(both(pbuf.at[x2, top, cols], pbuf.at[x2, low, cols], r1buf))
        RD.append(both(pbuf.at[xp, low, cols], pbuf.at[xm, top, cols], dbuf))
        RC.append(both(cbuf.at[0, :, cols], cbuf.at[1, :, cols], crecv))
    assert len(send) == N_MSG, len(send)
    for k in range(COLS):
        cols = slice(k * WIDE, (k + 1) * WIDE)
        part = jnp.dot(attended, wout[:, cols], preferred_element_type=f32).astype(bf16)
        pbuf[:, :, cols] = part.reshape(4, OWN, WIDE)
        start(R1[k])
    start(*RD)
    for k in range(COLS):
        cols = slice(k * WIDE, (k + 1) * WIDE)
        arrived(R1[k])
        cbuf[0, :, cols] = (
            r1buf[0, :, cols].astype(f32) + pbuf[xp, 0:32, cols].astype(f32)
        ).astype(bf16)
        cbuf[1, :, cols] = (
            r1buf[1, :, cols].astype(f32) + pbuf[xm, 32:64, cols].astype(f32)
        ).astype(bf16)
        start(RC[k])
    for k in range(COLS):
        cols = slice(k * WIDE, (k + 1) * WIDE)
        arrived(RD[k], RC[k])
        out[0:32, cols] = (
            pbuf[x, 0:32, cols].astype(f32)
            + crecv[0, :, cols].astype(f32)
            + dbuf[1, :, cols].astype(f32)
        ).astype(bf16)
        out[32:64, cols] = (
            pbuf[x, 32:64, cols].astype(f32)
            + crecv[1, :, cols].astype(f32)
            + dbuf[0, :, cols].astype(f32)
        ).astype(bf16)
    for oa in OFFS:

        @pl.when(jnp.logical_not(far_seen(oa)))
        def _(oa=oa):
            arrived(B2[oa, 0], B2[oa, 1])

    for i in range(N_MSG):
        send[i].wait_send()


def local(
    tokens,
    down_query,
    down_latent,
    down_rotary,
    query_gain,
    latent_gain,
    up_query,
    up_query_rotary,
    up_key,
    up_value,
    out_weight,
):
    rates = (rope_base ** (-np.arange(0, ROPE, 2) / ROPE)).astype(np.float32)
    lane_rates = jnp.asarray(np.tile(rates, 4)[None, :])
    row_rates = jnp.asarray(np.repeat(rates[:, None], GROUP, axis=1))
    vmem = pl.BlockSpec(memory_space=pltpu.VMEM)
    hbm = pl.BlockSpec(memory_space=pl.ANY)
    return pl.pallas_call(
        kernel,
        out_shape=pltpu.VMEM((OWN, 4096), bf16),
        in_specs=[hbm] * 13,
        out_specs=vmem,
        scratch_shapes=[
            pltpu.VMEM((OWN, 4096), bf16),
            pltpu.VMEM((1, 128), f32),
            pltpu.VMEM((32, GROUP), f32),
            pltpu.VMEM((1, 512), f32),
            pltpu.VMEM((1, 1024), f32),
            pltpu.VMEM((4096, 512), bf16),
            pltpu.VMEM((64, 4096), bf16),
            pltpu.VMEM((4096, 1024), bf16),
            pltpu.VMEM((1024, 512), bf16),
            pltpu.VMEM((1024, 256), bf16),
            pltpu.VMEM((512, 512), bf16),
            pltpu.VMEM((512, 512), bf16),
            pltpu.VMEM((512, 4096), bf16),
            pltpu.VMEM((16, 4, BLOCK, 128), bf16),
            pltpu.VMEM((4, OWN, 1024), bf16),
            pltpu.VMEM((2, HEADS * (NOPE + ROPE), GROUP), bf16),
            pltpu.VMEM((512, 512), bf16),
            pltpu.VMEM((2 * GROUP, 640), bf16),
            pltpu.VMEM((HEADS, VROWS, 2 * GROUP), bf16),
            pltpu.VMEM((HEADS, VROWS, 2 * GROUP), f32),
            pltpu.VMEM((HEADS, 1, 2 * GROUP), f32),
            pltpu.VMEM((HEADS, 256, 2 * GROUP), bf16),
            pltpu.VMEM((2, 2 * GROUP, 2 * GROUP), f32),
            pltpu.VMEM((2, 1, 2 * GROUP), f32),
            pltpu.VMEM((HEADS, VDIM, GROUP), bf16),
            pltpu.VMEM((HEADS, VDIM, GROUP), bf16),
            pltpu.VMEM((HEADS, 8, GROUP), f32),
            pltpu.VMEM((HEADS, 8, GROUP), f32),
            pltpu.VMEM((4, OWN, 4096), bf16),
            pltpu.VMEM((2, 32, 4096), bf16),
            pltpu.VMEM((2, 32, 4096), bf16),
            pltpu.VMEM((2, 32, 4096), bf16),
            pltpu.VMEM((2, 32, 4096), bf16),
            pltpu.SemaphoreType.DMA((19,)),
            pltpu.SemaphoreType.DMA((N_MSG,)),
            pltpu.SemaphoreType.DMA((N_MSG,)),
        ],
        compiler_params=pltpu.CompilerParams(
            collective_id=0, has_side_effects=True, vmem_limit_bytes=62 * 1024 * 1024
        ),
    )(
        tokens,
        down_query,
        down_latent,
        down_rotary.T,
        query_gain.reshape(1, -1),
        latent_gain.reshape(1, -1),
        up_query,
        up_query_rotary,
        up_key,
        up_value,
        out_weight,
        lane_rates,
        row_rates,
    )


def solution(mesh):
    return jax.shard_map(
        local,
        mesh=mesh,
        in_specs=(
            P(("sp", "tp"), None),
            P(),
            P(),
            P(),
            P(),
            P(),
            P(None, "tp"),
            P(None, "tp"),
            P(None, "tp"),
            P(None, "tp"),
            P("tp", None),
        ),
        out_specs=P(("sp", "tp"), None),
        check_vma=False,
    )
```

```python
import functools

import jax
import jax.numpy as jnp
import numpy as np
from jax import lax
from jax.experimental import pallas as pl
from jax.experimental.pallas import tpu as pltpu
from jax.sharding import PartitionSpec as P

NOPE = 128
ROPE = 64
VDIM = 128
HEADS = 4
OWN = 64
GROUP = 256
BLOCK = 288
VROWS = 144
RING = 4

rope_base = 500000.0
norm_eps = 1e-06
masked_score = -1e30

f32 = jnp.float32
bf16 = jnp.bfloat16
MESH = pl.DeviceIdType.MESH

COLS = 4
N_MSG = 103 + 6 * (COLS - 4)

STEPS = 9
UNIT_OA = ((0, 1, 0, 2, 1, -1, 2, 1, 2), (0, -1, 0, 1, -1, 0, 2, -1, 2))
UNIT_OB = ((0, 0, 1, 0, -1, -1, 1, 2, 2), (0, 0, -1, 1, 1, 2, -1, 2, 2))


def pick(index, values):
    out = jnp.int32(values[0])
    for i, v in enumerate(values[1:], 1):
        out = jnp.where(index == i, jnp.int32(v), out)
    return out


def once(condition):
    def run(body):
        def trip(_, carry):
            body()
            return carry

        lax.fori_loop(0, jnp.where(condition, 1, 0), trip, 0)

    return run


def mod4(v):
    return jnp.where(v < 0, v + 4, jnp.where(v > 3, v - 4, v))


def kernel(
    tokens_in,
    down_query,
    down_latent,
    down_rotary,
    query_gain,
    latent_gain,
    up_query,
    up_query_rotary,
    up_key,
    up_value,
    out_weight,
    lane_rates,
    row_rates,
    out,
    tokens,
    lrate,
    rrate,
    lgain,
    qgain,
    wdl,
    wdr,
    wdq,
    wuq,
    wur,
    wuk,
    wuv,
    wout,
    lat,
    ql,
    qt,
    uvt,
    kbuf,
    vbuf,
    acc,
    best,
    qfull,
    sbuf,
    tops,
    xsend,
    xrecv,
    ssend,
    srecv,
    pbuf,
    r1buf,
    dbuf,
    cbuf,
    crecv,
    local_sem,
    ssem,
    rsem,
):
    sp = lax.axis_index("sp")
    x = lax.axis_index("tp")
    c = lax.rem(sp, 2)
    m = sp // 2
    y = lax.rem(m, 4)
    z = m // 4
    first = c == 0
    a = jnp.where(first, y, z)
    b = jnp.where(first, z, y)
    stride_a = jnp.where(first, 2, 8)
    stride_b = jnp.where(first, 8, 2)

    def at(aa, bb):
        return {"sp": aa * stride_a + bb * stride_b + c, "tp": x}

    xp, xm, x2 = mod4(x + 1), mod4(x - 1), mod4(x + 2)
    dev_xp = {"sp": sp, "tp": xp}
    dev_xm = {"sp": sp, "tp": xm}
    dev_ap, dev_am = at(mod4(a + 1), b), at(mod4(a - 1), b)
    dev_bp, dev_bm = at(a, mod4(b + 1)), at(a, mod4(b - 1))
    dev_core = {"sp": sp + 1 - 2 * c, "tp": x}

    copies = []

    def copy_in(src, dst):
        copies.append(pltpu.make_async_copy(src, dst, local_sem.at[len(copies)]))
        copies[-1].start()
        return copies[-1]

    K4 = 1024
    quarters = [pl.ds(k * K4, K4) for k in range(4)]
    load_lanes = copy_in(lane_rates, lrate)
    load_tokens = copy_in(tokens_in, tokens)
    load_latent = [copy_in(down_latent.at[r], wdl.at[r]) for r in quarters]
    load_rotary = copy_in(down_rotary, wdr)
    load_rows = copy_in(row_rates, rrate)
    load_lgain = copy_in(latent_gain, lgain)
    load_qgain = copy_in(query_gain, qgain)
    load_query = [copy_in(down_query.at[r], wdq.at[r]) for r in quarters]
    load_rest = [
        copy_in(up_query, wuq),
        copy_in(up_query_rotary, wur),
        copy_in(up_key, wuk),
        copy_in(up_value, wuv),
        copy_in(out_weight, wout),
    ]

    barrier = pltpu.get_barrier_semaphore()
    for dev in (dev_xp, dev_xm, dev_ap, dev_am, dev_bp, dev_bm, dev_core):
        pl.semaphore_signal(barrier, inc=1, device_id=dev, device_id_type=MESH)

    send, recv = [], []

    def add(src, dst, landed, dev):
        i = len(send)
        for refs, done in ((src, dst), send), ((landed, landed), recv):
            done.append(
                pltpu.make_async_remote_copy(
                    src_ref=refs[0],
                    dst_ref=refs[1],
                    send_sem=ssem.at[i],
                    recv_sem=rsem.at[i],
                    device_id=dev,
                    device_id_type=MESH,
                )
            )
        return i

    def pair(up, up_landed, dev_up, down, down_landed, dev_down):
        return (
            add(lat.at[up], lat.at[up], lat.at[up_landed], dev_up),
            add(lat.at[down], lat.at[down], lat.at[down_landed], dev_down),
        )

    def group(oa, ob):
        return mod4(b + ob) * 4 + mod4(a + oa)

    def xs(o):
        return mod4(x + o)

    OFFS = (0, 1, -1, 2)
    s0 = group(0, 0)
    lo, hi = pl.ds(0, BLOCK // 2), pl.ds(BLOCK // 2, BLOCK // 2)

    def block(oa, ob, o):
        return group(oa, ob), xs(o)

    X1 = [
        pair((s0, x, up), (s0, xm, up), dev_xp, (s0, x, down), (s0, xp, down), dev_xm)
        for up, down in ((lo, hi), (hi, lo))
    ]
    X2 = pair((s0, xm, lo), (s0, x2, lo), dev_xp, (s0, xp, hi), (s0, x2, hi), dev_xm)
    A1, A2, B1, B2 = {}, {}, {}, {}
    for o in OFFS:
        A1[o] = pair(
            block(0, 0, o), block(-1, 0, o), dev_ap, block(0, 0, o), block(1, 0, o), dev_am
        )
        for oa in OFFS:
            B1[oa, o] = pair(
                block(oa, 0, o), block(oa, -1, o), dev_bp, block(oa, 0, o), block(oa, 1, o), dev_bm
            )
    for n, (up, down) in enumerate(((0, 1), (2, -1))):
        A2[n] = pair(
            block(-1, 0, up), block(2, 0, up), dev_ap, block(1, 0, down), block(2, 0, down), dev_am
        )
        for oa in OFFS:
            B2[oa, n] = pair(
                block(oa, -1, up),
                block(oa, 2, up),
                dev_bp,
                block(oa, 1, down),
                block(oa, 2, down),
                dev_bm,
            )
    q_lo, q_hi = pl.ds(0, OWN // 2), pl.ds(OWN // 2, OWN // 2)
    Q1 = [
        (
            add(ql.at[x, up], ql.at[x, up], ql.at[xm, up], dev_xp),
            add(ql.at[x, down], ql.at[x, down], ql.at[xp, down], dev_xm),
        )
        for up, down in ((q_lo, q_hi), (q_hi, q_lo))
    ]
    Q2 = (
        add(ql.at[xm, q_lo], ql.at[xm, q_lo], ql.at[x2, q_lo], dev_xp),
        add(ql.at[xp, q_hi], ql.at[xp, q_hi], ql.at[x2, q_hi], dev_xm),
    )
    QX = []
    for n in range(2):
        half = pl.ds(n * 2 * OWN, 2 * OWN)
        mine = qt.at[c, :, half]
        QX.append((add(mine, mine, qt.at[1 - c, :, half], dev_core),))
    OX = [(add(xsend.at[h], xrecv.at[h], xrecv.at[h], dev_core),) for h in range(HEADS)]
    OS = (add(ssend, srecv, srecv, dev_core),)

    def start(*groups):
        for ids in groups:
            for i in ids:
                send[i].start()

    def arrived(*groups):
        for ids in groups:
            for i in ids:
                recv[i].wait_recv()

    def token_of(col):
        place = col
        for r, o in enumerate(OFFS):
            inside = jnp.logical_and(col >= r * OWN, col < (r + 1) * OWN)
            place = jnp.where(inside, col + (xs(o) - r) * OWN, place)
        return place

    def norm_rows(values, gain):
        return values * lax.rsqrt(jnp.mean(values * values, axis=-1, keepdims=True) + norm_eps) * gain

    load_lanes.wait()
    spot = lax.broadcasted_iota(jnp.int32, (OWN, 128), 0) + (sp * RING + x) * OWN
    angles = spot.astype(f32) * lrate[...]
    lane = lax.broadcasted_iota(jnp.int32, (OWN, 128), 1)
    key_cos = jnp.cos(angles)
    key_sin = jnp.sin(angles) * jnp.where(lax.rem(lane, 64) < 32, -1.0, 1.0)
    load_tokens.wait()
    latent = jnp.zeros((OWN, 512), f32)
    for k in range(4):
        load_latent[k].wait()
        cols = slice(k * K4, (k + 1) * K4)
        latent = latent + jnp.dot(tokens[:, cols], wdl[cols, :], preferred_element_type=f32)
    load_lgain.wait()
    latent = norm_rows(latent, lgain[...]).astype(bf16)
    for t in range(4):
        lat[s0, x, t * OWN : (t + 1) * OWN, :] = latent[:, t * 128 : (t + 1) * 128]
    load_rotary.wait()
    turned = lax.dot_general(
        tokens[...], wdr[...], (((1,), (1,)), ((), ())), preferred_element_type=f32
    )
    turned = jnp.concatenate([turned, turned], axis=-1)
    turned = turned * key_cos + pltpu.roll(turned, 32, 1) * key_sin
    lat[s0, x, 256:288, :] = jnp.where(lane[:32] < 64, turned[:32], turned[32:]).astype(bf16)
    pl.semaphore_wait(barrier, 7)
    start(*X1, A1[0], B1[0, 0])

    query = jnp.zeros((OWN, 1024), f32)
    for k in range(4):
        load_query[k].wait()
        cols = slice(k * K4, (k + 1) * K4)
        query = query + jnp.dot(tokens[:, cols], wdq[cols, :], preferred_element_type=f32)
    load_qgain.wait()
    ql[x] = norm_rows(query, qgain[...]).astype(bf16)
    start(Q1[0])
    arrived(X1[0])
    start(X2, Q1[1])
    arrived(X1[1])
    start(A1[1], A1[-1], B1[0, 1], B1[0, -1])
    load_rows.wait()
    for load in load_rest:
        load.wait()
    uvt[...] = jnp.transpose(wuv[...])
    for h in range(HEADS):
        vbuf[h, VDIM:VROWS, :] = jnp.ones((VROWS - VDIM, 2 * GROUP), bf16)
    acc[...] = jnp.zeros_like(acc)
    best[...] = jnp.full(best.shape, masked_score, f32)
    spot = token_of(lax.broadcasted_iota(jnp.int32, (32, GROUP), 1)) + sp * GROUP
    angles = spot.astype(f32) * rrate[...]
    cosine, sine = jnp.cos(angles), jnp.sin(angles)
    arrived(A1[0])
    start(B1[1, 0], B1[-1, 0])
    arrived(Q1[0])
    start(Q2)
    arrived(A1[1])
    start(A2[0], B1[1, 1], B1[-1, 1])
    arrived(B1[0, 0], B1[0, 1])
    start(B2[0, 0])
    arrived(X2)
    start(A1[2], B1[0, 2])
    arrived(A1[-1])
    start(B1[1, -1], B1[-1, -1])
    factor = (NOPE + ROPE) ** (-0.5) * 1.4426950408889634

    def make_queries(n):
        half = slice(n * 2 * OWN, (n + 1) * 2 * OWN)
        rows = jnp.concatenate([ql[xs(OFFS[2 * n])], ql[xs(OFFS[2 * n + 1])]], axis=0)
        plain = jnp.dot(rows, wuq[...], preferred_element_type=f32) * factor
        qt[c, 0 : HEADS * NOPE, half] = jnp.transpose(plain.astype(bf16))
        turned = jnp.transpose(jnp.dot(rows, wur[...], preferred_element_type=f32) * factor)
        for h in range(HEADS):
            one = turned[h * ROPE : h * ROPE + 32]
            two = turned[h * ROPE + 32 : (h + 1) * ROPE]
            at_row = HEADS * NOPE + h * ROPE
            qt[c, at_row : at_row + 32, half] = (
                one * cosine[:, half] - two * sine[:, half]
            ).astype(bf16)
            qt[c, at_row + 32 : at_row + 64, half] = (
                two * cosine[:, half] + one * sine[:, half]
            ).astype(bf16)
        start(QX[n])

    arrived(Q1[1])
    make_queries(0)
    arrived(Q2)
    make_queries(1)

    def set_of(u, n):
        aa, bb = mod4(a + pick(u, UNIT_OA[n])), mod4(b + pick(u, UNIT_OB[n]))
        spot = jnp.where(first, bb * 4 + aa, aa * 4 + bb)
        seen = spot <= m
        if n == 1:
            seen = jnp.logical_and(seen, jnp.logical_and(u > 0, u < STEPS - 1))
        return bb * 4 + aa, spot, seen

    def attend(sets, spot):
        keys = len(sets) * GROUP
        parts, rots = [], []
        for s in sets:
            tiles = [
                lat[s, :, t * OWN : (t + 1) * OWN, :].reshape(GROUP, 128) for t in range(4)
            ]
            parts.append(jnp.concatenate(tiles, axis=1))
            packed = lat[s, :, 256:288, :]
            swapped = pltpu.roll(packed.reshape(128, 128).astype(f32), 64, 1).astype(bf16)
            rots.append(
                jnp.concatenate([packed, swapped.reshape(4, 32, 128)], axis=1).reshape(GROUP, 128)
            )
        latents = jnp.concatenate(parts, axis=0)
        kbuf[:keys, 0:512] = jnp.dot(latents, wuk[...], preferred_element_type=f32).astype(bf16)
        kbuf[:keys, 512:640] = jnp.concatenate(rots, axis=0)

        def score(h):
            key = jnp.concatenate(
                [kbuf[:keys, h * NOPE : (h + 1) * NOPE], kbuf[:keys, 512:640]], axis=1
            )
            scores = jnp.dot(key, qfull[h], preferred_element_type=f32)
            if spot is not None:
                row = lax.broadcasted_iota(jnp.int32, (keys, 2 * GROUP), 0)
                col = lax.broadcasted_iota(jnp.int32, (1, 2 * GROUP), 1)
                col = jnp.where(col < GROUP, token_of(col), token_of(col - GROUP) + GROUP)
                ahead = (2 * (spot - m) + c) * GROUP
                scores = jnp.where(row <= col - ahead, scores, masked_score)
            sbuf[h % 2, :keys] = scores
            tops[h % 2] = jnp.max(scores, axis=0, keepdims=True)

        score(0)
        values = lax.dot_general(
            uvt[...], latents, (((1,), (1,)), ((), ())), preferred_element_type=f32
        ).astype(bf16)
        for h in range(HEADS):
            vbuf[h, 0:VDIM, :keys] = values[h * VDIM : (h + 1) * VDIM]
        for h in range(HEADS):
            if h + 1 < HEADS:
                score(h + 1)
            old = best[h]
            new = jnp.maximum(old, tops[h % 2])
            weights = jnp.exp2(sbuf[h % 2, :keys] - new).astype(bf16)
            best[h] = new
            acc[h] = acc[h] * jnp.exp2(old - new) + jnp.dot(
                vbuf[h, :, :keys], weights, preferred_element_type=f32
            )

    arrived(A2[0])
    start(B1[2, 0], B1[2, 1])
    arrived(B1[1, 0], B1[1, 1])
    start(B2[1, 0])
    arrived(*QX)
    for h in range(HEADS):
        for j in range(2):
            cols = slice(j * GROUP, (j + 1) * GROUP)
            qfull[h, 0:NOPE, cols] = qt[j, h * NOPE : (h + 1) * NOPE, :]
            at_row = HEADS * NOPE + h * ROPE
            qfull[h, NOPE : NOPE + ROPE, cols] = qt[j, at_row : at_row + ROPE, :]
        qfull[h, NOPE + ROPE :, :] = jnp.zeros((ROPE, 2 * GROUP), bf16)

    def far_seen(oa):
        aa, bb = mod4(a + oa), mod4(b + 2)
        return jnp.where(first, bb * 4 + aa, aa * 4 + bb) <= m

    def step(u, carry):

        @once(u == 1)
        def _():
            arrived(A1[2])
            start(A2[1], B1[1, 2], B1[-1, 2])
            arrived(B1[-1, 0], B1[-1, 1])
            start(B2[-1, 0])

        @once(u == 2)
        def _():
            arrived(B1[0, -1], B1[0, 2])
            start(B2[0, 1])

        @once(u == 3)
        def _():
            arrived(A2[1])
            start(B1[2, -1], B1[2, 2])
            arrived(B1[1, -1], B1[1, 2])
            start(B2[1, 1])

        @once(u == 4)
        def _():
            arrived(B1[2, 0], B1[2, 1])
            start(B2[2, 0])
            arrived(B1[-1, -1], B1[-1, 2])
            start(B2[-1, 1])

        @once(u == 6)
        def _():
            arrived(B1[2, -1], B1[2, 2])
            start(B2[2, 1])

        for oa, when in ((0, 5), (1, 7), (-1, 7), (2, 8)):

            @once(jnp.logical_and(u == when, far_seen(oa)))
            def _(oa=oa):
                arrived(B2[oa, 0], B2[oa, 1])

        set_one, spot_one, seen_one = set_of(u, 0)
        set_two, spot_two, seen_two = set_of(u, 1)
        two = jnp.logical_and(seen_one, seen_two)
        one = jnp.logical_and(jnp.logical_or(seen_one, seen_two), jnp.logical_not(two))
        single = jnp.where(seen_one, set_one, set_two)
        spot = jnp.where(seen_one, spot_one, spot_two)

        @pl.when(two)
        def _():
            attend((set_one, set_two), None)

        @pl.when(one)
        def _():
            attend((single,), spot)

        return carry

    lax.fori_loop(0, STEPS, step, 0)

    mine_at = pl.ds(pl.multiple_of(c * GROUP, GROUP), GROUP)
    other_at = pl.ds(pl.multiple_of((1 - c) * GROUP, GROUP), GROUP)
    for h in range(HEADS):
        ssend[h, 0:1, :] = best[h, :, other_at]
        ssend[h, 1:2, :] = acc[h, 128:129, other_at]
    start(OS)
    for h in range(HEADS):
        xsend[h] = acc[h, 0:128, other_at].astype(bf16)
        start(OX[h])
    arrived(OS)
    heads = []
    for h in range(HEADS):
        mine, theirs = best[h, :, mine_at], srecv[h, 0:1, :]
        top = jnp.maximum(mine, theirs)
        w_mine, w_theirs = jnp.exp2(mine - top), jnp.exp2(theirs - top)
        total = acc[h, 128:129, mine_at] * w_mine + srecv[h, 1:2, :] * w_theirs
        arrived(OX[h])
        summed = acc[h, 0:128, mine_at] * w_mine + xrecv[h].astype(f32) * w_theirs
        heads.append(jnp.transpose((summed * (1.0 / total)).astype(bf16)))
    attended = jnp.concatenate(heads, axis=1)

    WIDE = 4096 // COLS
    top, low = pl.ds(0, 32), pl.ds(32, 32)
    R1, RD, RC = [], [], []
    for k in range(COLS):
        cols = pl.ds(k * WIDE, WIDE)

        def both(to_up, to_down, ref):
            up, down = ref.at[0, :, cols], ref.at[1, :, cols]
            return add(to_up, up, up, dev_xp), add(to_down, down, down, dev_xm)

        R1.append(both(pbuf.at[3, top, cols], pbuf.at[3, low, cols], r1buf))
        RD.append(both(pbuf.at[1, low, cols], pbuf.at[2, top, cols], dbuf))
        RC.append(both(cbuf.at[0, :, cols], cbuf.at[1, :, cols], crecv))
    assert len(send) == N_MSG, len(send)
    for k in range(COLS):
        cols = slice(k * WIDE, (k + 1) * WIDE)
        part = jnp.dot(attended, wout[:, cols], preferred_element_type=f32).astype(bf16)
        pbuf[:, :, cols] = part.reshape(4, OWN, WIDE)
        start(R1[k])
    start(*RD)
    for k in range(COLS):
        cols = slice(k * WIDE, (k + 1) * WIDE)
        arrived(R1[k])
        cbuf[0, :, cols] = (
            r1buf[0, :, cols].astype(f32) + pbuf[1, 0:32, cols].astype(f32)
        ).astype(bf16)
        cbuf[1, :, cols] = (
            r1buf[1, :, cols].astype(f32) + pbuf[2, 32:64, cols].astype(f32)
        ).astype(bf16)
        start(RC[k])
    for k in range(COLS):
        cols = slice(k * WIDE, (k + 1) * WIDE)
        arrived(RD[k], RC[k])
        out[0:32, cols] = (
            pbuf[0, 0:32, cols].astype(f32)
            + crecv[0, :, cols].astype(f32)
            + dbuf[1, :, cols].astype(f32)
        ).astype(bf16)
        out[32:64, cols] = (
            pbuf[0, 32:64, cols].astype(f32)
            + crecv[1, :, cols].astype(f32)
            + dbuf[0, :, cols].astype(f32)
        ).astype(bf16)
    for oa in OFFS:

        @pl.when(jnp.logical_not(far_seen(oa)))
        def _(oa=oa):
            arrived(B2[oa, 0], B2[oa, 1])

    for i in range(N_MSG):
        send[i].wait_send()


def local(
    tokens,
    down_query,
    down_latent,
    down_rotary,
    query_gain,
    latent_gain,
    up_query,
    up_query_rotary,
    up_key,
    up_value,
    out_weight,
):
    rates = (rope_base ** (-np.arange(0, ROPE, 2) / ROPE)).astype(np.float32)
    lane_rates = jnp.asarray(np.tile(rates, 4)[None, :])
    row_rates = jnp.asarray(np.repeat(rates[:, None], GROUP, axis=1))
    vmem = pl.BlockSpec(memory_space=pltpu.VMEM)
    hbm = pl.BlockSpec(memory_space=pl.ANY)
    return pl.pallas_call(
        kernel,
        out_shape=pltpu.VMEM((OWN, 4096), bf16),
        in_specs=[hbm] * 13,
        out_specs=vmem,
        scratch_shapes=[
            pltpu.VMEM((OWN, 4096), bf16),
            pltpu.VMEM((1, 128), f32),
            pltpu.VMEM((32, GROUP), f32),
            pltpu.VMEM((1, 512), f32),
            pltpu.VMEM((1, 1024), f32),
            pltpu.VMEM((4096, 512), bf16),
            pltpu.VMEM((64, 4096), bf16),
            pltpu.VMEM((4096, 1024), bf16),
            pltpu.VMEM((1024, 512), bf16),
            pltpu.VMEM((1024, 256), bf16),
            pltpu.VMEM((512, 512), bf16),
            pltpu.VMEM((512, 512), bf16),
            pltpu.VMEM((512, 4096), bf16),
            pltpu.VMEM((16, 4, BLOCK, 128), bf16),
            pltpu.VMEM((4, OWN, 1024), bf16),
            pltpu.VMEM((2, HEADS * (NOPE + ROPE), GROUP), bf16),
            pltpu.VMEM((512, 512), bf16),
            pltpu.VMEM((2 * GROUP, 640), bf16),
            pltpu.VMEM((HEADS, VROWS, 2 * GROUP), bf16),
            pltpu.VMEM((HEADS, VROWS, 2 * GROUP), f32),
            pltpu.VMEM((HEADS, 1, 2 * GROUP), f32),
            pltpu.VMEM((HEADS, 256, 2 * GROUP), bf16),
            pltpu.VMEM((2, 2 * GROUP, 2 * GROUP), f32),
            pltpu.VMEM((2, 1, 2 * GROUP), f32),
            pltpu.VMEM((HEADS, VDIM, GROUP), bf16),
            pltpu.VMEM((HEADS, VDIM, GROUP), bf16),
            pltpu.VMEM((HEADS, 8, GROUP), f32),
            pltpu.VMEM((HEADS, 8, GROUP), f32),
            pltpu.VMEM((4, OWN, 4096), bf16),
            pltpu.VMEM((2, 32, 4096), bf16),
            pltpu.VMEM((2, 32, 4096), bf16),
            pltpu.VMEM((2, 32, 4096), bf16),
            pltpu.VMEM((2, 32, 4096), bf16),
            pltpu.SemaphoreType.DMA((19,)),
            pltpu.SemaphoreType.DMA((N_MSG,)),
            pltpu.SemaphoreType.DMA((N_MSG,)),
        ],
        compiler_params=pltpu.CompilerParams(
            collective_id=0, has_side_effects=True, vmem_limit_bytes=62 * 1024 * 1024
        ),
    )(
        tokens,
        down_query,
        down_latent,
        down_rotary.T,
        query_gain.reshape(1, -1),
        latent_gain.reshape(1, -1),
        up_query,
        up_query_rotary,
        up_key,
        up_value,
        out_weight,
        lane_rates,
        row_rates,
    )


def solution(mesh):
    return jax.shard_map(
        local,
        mesh=mesh,
        in_specs=(
            P(("sp", "tp"), None),
            P(),
            P(),
            P(),
            P(),
            P(),
            P(None, "tp"),
            P(None, "tp"),
            P(None, "tp"),
            P(None, "tp"),
            P("tp", None),
        ),
        out_specs=P(("sp", "tp"), None),
        check_vma=False,
    )
```

```python
import functools

import jax
import jax.numpy as jnp
import numpy as np
from jax import lax
from jax.experimental import pallas as pl
from jax.experimental.pallas import tpu as pltpu
from jax.sharding import PartitionSpec as P

NOPE = 128
ROPE = 64
VDIM = 128
HEADS = 4
OWN = 64
GROUP = 256
BLOCK = 288
VROWS = 144
RING = 4

rope_base = 500000.0
norm_eps = 1e-06
masked_score = -1e30

f32 = jnp.float32
bf16 = jnp.bfloat16
MESH = pl.DeviceIdType.MESH

COLS = 4
N_MSG = 103 + 6 * (COLS - 4)

STEPS = 9
UNIT_OA = ((0, 1, 0, 2, 1, -1, 2, 1, 2), (0, -1, 0, 1, -1, 0, 2, -1, 2))
UNIT_OB = ((0, 0, 1, 0, -1, -1, 1, 2, 2), (0, 0, -1, 1, 1, 2, -1, 2, 2))


def pick(index, values):
    out = jnp.int32(values[0])
    for i, v in enumerate(values[1:], 1):
        out = jnp.where(index == i, jnp.int32(v), out)
    return out


def once(condition):
    def run(body):
        def trip(_, carry):
            body()
            return carry

        lax.fori_loop(0, jnp.where(condition, 1, 0), trip, 0)

    return run


def mod4(v):
    return jnp.where(v < 0, v + 4, jnp.where(v > 3, v - 4, v))


def kernel(
    tokens_in,
    down_query,
    down_latent,
    down_rotary,
    query_gain,
    latent_gain,
    up_query,
    up_query_rotary,
    up_key,
    up_value,
    out_weight,
    lane_rates,
    row_rates,
    out,
    tokens,
    lrate,
    rrate,
    lgain,
    qgain,
    wdl,
    wdr,
    wdq,
    wuq,
    wur,
    wuk,
    wuv,
    wout,
    lat,
    ql,
    qt,
    uvt,
    kbuf,
    vbuf,
    acc,
    best,
    qfull,
    sbuf,
    tops,
    xsend,
    xrecv,
    ssend,
    srecv,
    pbuf,
    r1buf,
    dbuf,
    cbuf,
    crecv,
    local_sem,
    ssem,
    rsem,
):
    sp = lax.axis_index("sp")
    x = lax.axis_index("tp")
    c = lax.rem(sp, 2)
    m = sp // 2
    y = lax.rem(m, 4)
    z = m // 4
    first = c == 0
    a = jnp.where(first, y, z)
    b = jnp.where(first, z, y)
    stride_a = jnp.where(first, 2, 8)
    stride_b = jnp.where(first, 8, 2)

    def at(aa, bb):
        return {"sp": aa * stride_a + bb * stride_b + c, "tp": x}

    xp, xm, x2 = mod4(x + 1), mod4(x - 1), mod4(x + 2)
    dev_xp = {"sp": sp, "tp": xp}
    dev_xm = {"sp": sp, "tp": xm}
    dev_ap, dev_am = at(mod4(a + 1), b), at(mod4(a - 1), b)
    dev_bp, dev_bm = at(a, mod4(b + 1)), at(a, mod4(b - 1))
    dev_core = {"sp": sp + 1 - 2 * c, "tp": x}

    copies = []

    def copy_in(src, dst):
        copies.append(pltpu.make_async_copy(src, dst, local_sem.at[len(copies)]))
        copies[-1].start()
        return copies[-1]

    K4 = 1024
    quarters = [pl.ds(k * K4, K4) for k in range(4)]
    load_lanes = copy_in(lane_rates, lrate)
    load_tokens = copy_in(tokens_in, tokens)
    load_latent = [copy_in(down_latent.at[r], wdl.at[r]) for r in quarters]
    load_rotary = copy_in(down_rotary, wdr)
    load_rows = copy_in(row_rates, rrate)
    load_lgain = copy_in(latent_gain, lgain)
    load_qgain = copy_in(query_gain, qgain)
    load_query = [copy_in(down_query.at[r], wdq.at[r]) for r in quarters]
    load_rest = [
        copy_in(up_query, wuq),
        copy_in(up_query_rotary, wur),
        copy_in(up_key, wuk),
        copy_in(up_value, wuv),
        copy_in(out_weight, wout),
    ]

    barrier = pltpu.get_barrier_semaphore()
    for dev in (dev_xp, dev_xm, dev_ap, dev_am, dev_bp, dev_bm, dev_core):
        pl.semaphore_signal(barrier, inc=1, device_id=dev, device_id_type=MESH)

    send, recv = [], []

    def add(src, dst, landed, dev):
        i = len(send)
        for refs, done in ((src, dst), send), ((landed, landed), recv):
            done.append(
                pltpu.make_async_remote_copy(
                    src_ref=refs[0],
                    dst_ref=refs[1],
                    send_sem=ssem.at[i],
                    recv_sem=rsem.at[i],
                    device_id=dev,
                    device_id_type=MESH,
                )
            )
        return i

    def pair(up, up_landed, dev_up, down, down_landed, dev_down):
        return (
            add(lat.at[up], lat.at[up], lat.at[up_landed], dev_up),
            add(lat.at[down], lat.at[down], lat.at[down_landed], dev_down),
        )

    def group(oa, ob):
        return mod4(b + ob) * 4 + mod4(a + oa)

    def xs(o):
        return mod4(x + o)

    OFFS = (0, 1, -1, 2)
    s0 = group(0, 0)
    lo, hi = pl.ds(0, BLOCK // 2), pl.ds(BLOCK // 2, BLOCK // 2)

    def block(oa, ob, o):
        return group(oa, ob), xs(o)

    X1 = [
        pair((s0, x, up), (s0, xm, up), dev_xp, (s0, x, down), (s0, xp, down), dev_xm)
        for up, down in ((lo, hi), (hi, lo))
    ]
    X2 = pair((s0, xm, lo), (s0, x2, lo), dev_xp, (s0, xp, hi), (s0, x2, hi), dev_xm)
    A1, A2, B1, B2 = {}, {}, {}, {}
    for o in OFFS:
        A1[o] = pair(
            block(0, 0, o), block(-1, 0, o), dev_ap, block(0, 0, o), block(1, 0, o), dev_am
        )
        for oa in OFFS:
            B1[oa, o] = pair(
                block(oa, 0, o), block(oa, -1, o), dev_bp, block(oa, 0, o), block(oa, 1, o), dev_bm
            )
    for n, (up, down) in enumerate(((0, 1), (2, -1))):
        A2[n] = pair(
            block(-1, 0, up), block(2, 0, up), dev_ap, block(1, 0, down), block(2, 0, down), dev_am
        )
        for oa in OFFS:
            B2[oa, n] = pair(
                block(oa, -1, up),
                block(oa, 2, up),
                dev_bp,
                block(oa, 1, down),
                block(oa, 2, down),
                dev_bm,
            )
    q_lo, q_hi = pl.ds(0, OWN // 2), pl.ds(OWN // 2, OWN // 2)
    Q1 = [
        (
            add(ql.at[x, up], ql.at[x, up], ql.at[xm, up], dev_xp),
            add(ql.at[x, down], ql.at[x, down], ql.at[xp, down], dev_xm),
        )
        for up, down in ((q_lo, q_hi), (q_hi, q_lo))
    ]
    Q2 = (
        add(ql.at[xm, q_lo], ql.at[xm, q_lo], ql.at[x2, q_lo], dev_xp),
        add(ql.at[xp, q_hi], ql.at[xp, q_hi], ql.at[x2, q_hi], dev_xm),
    )
    QX = []
    for n in range(2):
        half = pl.ds(n * 2 * OWN, 2 * OWN)
        mine = qt.at[c, :, half]
        QX.append((add(mine, mine, qt.at[1 - c, :, half], dev_core),))
    OX = [(add(xsend.at[h], xrecv.at[h], xrecv.at[h], dev_core),) for h in range(HEADS)]
    OS = (add(ssend, srecv, srecv, dev_core),)

    def start(*groups):
        for ids in groups:
            for i in ids:
                send[i].start()

    def arrived(*groups):
        for ids in groups:
            for i in ids:
                recv[i].wait_recv()

    def token_of(col):
        place = col
        for r, o in enumerate(OFFS):
            inside = jnp.logical_and(col >= r * OWN, col < (r + 1) * OWN)
            place = jnp.where(inside, col + (xs(o) - r) * OWN, place)
        return place

    def norm_rows(values, gain):
        return values * lax.rsqrt(jnp.mean(values * values, axis=-1, keepdims=True) + norm_eps) * gain

    load_lanes.wait()
    spot = lax.broadcasted_iota(jnp.int32, (OWN, 128), 0) + (sp * RING + x) * OWN
    angles = spot.astype(f32) * lrate[...]
    lane = lax.broadcasted_iota(jnp.int32, (OWN, 128), 1)
    key_cos = jnp.cos(angles)
    key_sin = jnp.sin(angles) * jnp.where(lax.rem(lane, 64) < 32, -1.0, 1.0)
    load_tokens.wait()
    latent = jnp.zeros((OWN, 512), f32)
    for k in range(4):
        load_latent[k].wait()
        cols = slice(k * K4, (k + 1) * K4)
        latent = latent + jnp.dot(tokens[:, cols], wdl[cols, :], preferred_element_type=f32)
    load_lgain.wait()
    latent = norm_rows(latent, lgain[...]).astype(bf16)
    for t in range(4):
        lat[s0, x, t * OWN : (t + 1) * OWN, :] = latent[:, t * 128 : (t + 1) * 128]
    load_rotary.wait()
    turned = lax.dot_general(
        tokens[...], wdr[...], (((1,), (1,)), ((), ())), preferred_element_type=f32
    )
    turned = jnp.concatenate([turned, turned], axis=-1)
    turned = turned * key_cos + pltpu.roll(turned, 32, 1) * key_sin
    lat[s0, x, 256:288, :] = jnp.where(lane[:32] < 64, turned[:32], turned[32:]).astype(bf16)
    pl.semaphore_wait(barrier, 7)
    start(*X1, A1[0], B1[0, 0])

    query = jnp.zeros((OWN, 1024), f32)
    for k in range(4):
        load_query[k].wait()
        cols = slice(k * K4, (k + 1) * K4)
        query = query + jnp.dot(tokens[:, cols], wdq[cols, :], preferred_element_type=f32)
    load_qgain.wait()
    ql[x] = norm_rows(query, qgain[...]).astype(bf16)
    start(Q1[0])
    arrived(X1[0])
    start(X2, Q1[1])
    arrived(X1[1])
    start(A1[1], A1[-1], B1[0, 1], B1[0, -1])
    load_rows.wait()
    for load in load_rest:
        load.wait()
    uvt[...] = jnp.transpose(wuv[...])
    for h in range(HEADS):
        vbuf[h, VDIM:VROWS, :] = jnp.ones((VROWS - VDIM, 2 * GROUP), bf16)
    acc[...] = jnp.zeros_like(acc)
    best[...] = jnp.full(best.shape, masked_score, f32)
    spot = token_of(lax.broadcasted_iota(jnp.int32, (32, GROUP), 1)) + sp * GROUP
    angles = spot.astype(f32) * rrate[...]
    cosine, sine = jnp.cos(angles), jnp.sin(angles)
    arrived(A1[0])
    start(B1[1, 0], B1[-1, 0])
    arrived(Q1[0])
    start(Q2)
    arrived(A1[1])
    start(A2[0], B1[1, 1], B1[-1, 1])
    arrived(B1[0, 0], B1[0, 1])
    start(B2[0, 0])
    arrived(X2)
    start(A1[2], B1[0, 2])
    arrived(A1[-1])
    start(B1[1, -1], B1[-1, -1])
    factor = (NOPE + ROPE) ** (-0.5) * 1.4426950408889634

    def make_queries(n):
        half = slice(n * 2 * OWN, (n + 1) * 2 * OWN)
        rows = jnp.concatenate([ql[xs(OFFS[2 * n])], ql[xs(OFFS[2 * n + 1])]], axis=0)
        plain = jnp.dot(rows, wuq[...], preferred_element_type=f32) * factor
        qt[c, 0 : HEADS * NOPE, half] = jnp.transpose(plain.astype(bf16))
        turned = jnp.transpose(jnp.dot(rows, wur[...], preferred_element_type=f32) * factor)
        for h in range(HEADS):
            one = turned[h * ROPE : h * ROPE + 32]
            two = turned[h * ROPE + 32 : (h + 1) * ROPE]
            at_row = HEADS * NOPE + h * ROPE
            qt[c, at_row : at_row + 32, half] = (
                one * cosine[:, half] - two * sine[:, half]
            ).astype(bf16)
            qt[c, at_row + 32 : at_row + 64, half] = (
                two * cosine[:, half] + one * sine[:, half]
            ).astype(bf16)
        start(QX[n])

    arrived(Q1[1])
    make_queries(0)
    arrived(Q2)
    make_queries(1)

    def set_of(u, n):
        aa, bb = mod4(a + pick(u, UNIT_OA[n])), mod4(b + pick(u, UNIT_OB[n]))
        spot = jnp.where(first, bb * 4 + aa, aa * 4 + bb)
        seen = spot <= m
        if n == 1:
            seen = jnp.logical_and(seen, jnp.logical_and(u > 0, u < STEPS - 1))
        return bb * 4 + aa, spot, seen

    def attend(sets, spot):
        keys = len(sets) * GROUP
        parts, rots = [], []
        for s in sets:
            tiles = [
                lat[s, :, t * OWN : (t + 1) * OWN, :].reshape(GROUP, 128) for t in range(4)
            ]
            parts.append(jnp.concatenate(tiles, axis=1))
            packed = lat[s, :, 256:288, :]
            swapped = pltpu.roll(packed.reshape(128, 128).astype(f32), 64, 1).astype(bf16)
            rots.append(
                jnp.concatenate([packed, swapped.reshape(4, 32, 128)], axis=1).reshape(GROUP, 128)
            )
        latents = jnp.concatenate(parts, axis=0)
        kbuf[:keys, 0:512] = jnp.dot(latents, wuk[...], preferred_element_type=f32).astype(bf16)
        kbuf[:keys, 512:640] = jnp.concatenate(rots, axis=0)

        def score(h):
            key = jnp.concatenate(
                [kbuf[:keys, h * NOPE : (h + 1) * NOPE], kbuf[:keys, 512:640]], axis=1
            )
            scores = jnp.dot(key, qfull[h], preferred_element_type=f32)
            if spot is not None:
                row = lax.broadcasted_iota(jnp.int32, (keys, 2 * GROUP), 0)
                col = lax.broadcasted_iota(jnp.int32, (1, 2 * GROUP), 1)
                col = jnp.where(col < GROUP, token_of(col), token_of(col - GROUP) + GROUP)
                ahead = (2 * (spot - m) + c) * GROUP
                scores = jnp.where(row <= col - ahead, scores, masked_score)
            sbuf[h % 2, :keys] = scores
            tops[h % 2] = jnp.max(scores, axis=0, keepdims=True)

        score(0)
        values = lax.dot_general(
            uvt[...], latents, (((1,), (1,)), ((), ())), preferred_element_type=f32
        ).astype(bf16)
        for h in range(HEADS):
            vbuf[h, 0:VDIM, :keys] = values[h * VDIM : (h + 1) * VDIM]
        for h in range(HEADS):
            if h + 1 < HEADS:
                score(h + 1)
            old = best[h]
            new = jnp.maximum(old, tops[h % 2])
            weights = jnp.exp2(sbuf[h % 2, :keys] - new).astype(bf16)
            best[h] = new
            acc[h] = acc[h] * jnp.exp2(old - new) + jnp.dot(
                vbuf[h, :, :keys], weights, preferred_element_type=f32
            )

    def pass_second():
        arrived(A2[0])
        start(B1[2, 0], B1[2, 1])
        arrived(B1[1, 0], B1[1, 1])
        start(B2[1, 0])

    once(jnp.logical_not(first))(pass_second)

    arrived(*QX)
    for h in range(HEADS):
        for j in range(2):
            cols = slice(j * GROUP, (j + 1) * GROUP)
            qfull[h, 0:NOPE, cols] = qt[j, h * NOPE : (h + 1) * NOPE, :]
            at_row = HEADS * NOPE + h * ROPE
            qfull[h, NOPE : NOPE + ROPE, cols] = qt[j, at_row : at_row + ROPE, :]
        qfull[h, NOPE + ROPE :, :] = jnp.zeros((ROPE, 2 * GROUP), bf16)

    def far_seen(oa):
        aa, bb = mod4(a + oa), mod4(b + 2)
        return jnp.where(first, bb * 4 + aa, aa * 4 + bb) <= m

    def step(u, carry):

        @once(u == 1)
        def _():
            arrived(A1[2])
            start(A2[1], B1[1, 2], B1[-1, 2])
            once(first)(pass_second)
            arrived(B1[-1, 0], B1[-1, 1])
            start(B2[-1, 0])

        @once(u == 2)
        def _():
            arrived(B1[0, -1], B1[0, 2])
            start(B2[0, 1])

        @once(u == 3)
        def _():
            arrived(A2[1])
            start(B1[2, -1], B1[2, 2])
            arrived(B1[1, -1], B1[1, 2])
            start(B2[1, 1])

        @once(u == 4)
        def _():
            arrived(B1[2, 0], B1[2, 1])
            start(B2[2, 0])
            arrived(B1[-1, -1], B1[-1, 2])
            start(B2[-1, 1])

        @once(u == 6)
        def _():
            arrived(B1[2, -1], B1[2, 2])
            start(B2[2, 1])

        for oa, when in ((0, 5), (1, 7), (-1, 7), (2, 8)):

            @once(jnp.logical_and(u == when, far_seen(oa)))
            def _(oa=oa):
                arrived(B2[oa, 0], B2[oa, 1])

        set_one, spot_one, seen_one = set_of(u, 0)
        set_two, spot_two, seen_two = set_of(u, 1)
        two = jnp.logical_and(seen_one, seen_two)
        one = jnp.logical_and(jnp.logical_or(seen_one, seen_two), jnp.logical_not(two))
        single = jnp.where(seen_one, set_one, set_two)
        spot = jnp.where(seen_one, spot_one, spot_two)

        @pl.when(two)
        def _():
            attend((set_one, set_two), None)

        @pl.when(one)
        def _():
            attend((single,), spot)

        return carry

    lax.fori_loop(0, STEPS, step, 0)

    mine_at = pl.ds(pl.multiple_of(c * GROUP, GROUP), GROUP)
    other_at = pl.ds(pl.multiple_of((1 - c) * GROUP, GROUP), GROUP)
    for h in range(HEADS):
        ssend[h, 0:1, :] = best[h, :, other_at]
        ssend[h, 1:2, :] = acc[h, 128:129, other_at]
    start(OS)
    for h in range(HEADS):
        xsend[h] = acc[h, 0:128, other_at].astype(bf16)
        start(OX[h])
    arrived(OS)
    heads = []
    for h in range(HEADS):
        mine, theirs = best[h, :, mine_at], srecv[h, 0:1, :]
        top = jnp.maximum(mine, theirs)
        w_mine, w_theirs = jnp.exp2(mine - top), jnp.exp2(theirs - top)
        total = acc[h, 128:129, mine_at] * w_mine + srecv[h, 1:2, :] * w_theirs
        arrived(OX[h])
        summed = acc[h, 0:128, mine_at] * w_mine + xrecv[h].astype(f32) * w_theirs
        heads.append(jnp.transpose((summed * (1.0 / total)).astype(bf16)))
    attended = jnp.concatenate(heads, axis=1)

    WIDE = 4096 // COLS
    top, low = pl.ds(0, 32), pl.ds(32, 32)
    R1, RD, RC = [], [], []
    for k in range(COLS):
        cols = pl.ds(k * WIDE, WIDE)

        def both(to_up, to_down, ref):
            up, down = ref.at[0, :, cols], ref.at[1, :, cols]
            return add(to_up, up, up, dev_xp), add(to_down, down, down, dev_xm)

        R1.append(both(pbuf.at[3, top, cols], pbuf.at[3, low, cols], r1buf))
        RD.append(both(pbuf.at[1, low, cols], pbuf.at[2, top, cols], dbuf))
        RC.append(both(cbuf.at[0, :, cols], cbuf.at[1, :, cols], crecv))
    assert len(send) == N_MSG, len(send)
    for k in range(COLS):
        cols = slice(k * WIDE, (k + 1) * WIDE)
        part = jnp.dot(attended, wout[:, cols], preferred_element_type=f32).astype(bf16)
        pbuf[:, :, cols] = part.reshape(4, OWN, WIDE)
        start(R1[k])
    start(*RD)
    for k in range(COLS):
        cols = slice(k * WIDE, (k + 1) * WIDE)
        arrived(R1[k])
        cbuf[0, :, cols] = (
            r1buf[0, :, cols].astype(f32) + pbuf[1, 0:32, cols].astype(f32)
        ).astype(bf16)
        cbuf[1, :, cols] = (
            r1buf[1, :, cols].astype(f32) + pbuf[2, 32:64, cols].astype(f32)
        ).astype(bf16)
        start(RC[k])
    for k in range(COLS):
        cols = slice(k * WIDE, (k + 1) * WIDE)
        arrived(RD[k], RC[k])
        out[0:32, cols] = (
            pbuf[0, 0:32, cols].astype(f32)
            + crecv[0, :, cols].astype(f32)
            + dbuf[1, :, cols].astype(f32)
        ).astype(bf16)
        out[32:64, cols] = (
            pbuf[0, 32:64, cols].astype(f32)
            + crecv[1, :, cols].astype(f32)
            + dbuf[0, :, cols].astype(f32)
        ).astype(bf16)
    for oa in OFFS:

        @pl.when(jnp.logical_not(far_seen(oa)))
        def _(oa=oa):
            arrived(B2[oa, 0], B2[oa, 1])

    for i in range(N_MSG):
        send[i].wait_send()


def local(
    tokens,
    down_query,
    down_latent,
    down_rotary,
    query_gain,
    latent_gain,
    up_query,
    up_query_rotary,
    up_key,
    up_value,
    out_weight,
):
    rates = (rope_base ** (-np.arange(0, ROPE, 2) / ROPE)).astype(np.float32)
    lane_rates = jnp.asarray(np.tile(rates, 4)[None, :])
    row_rates = jnp.asarray(np.repeat(rates[:, None], GROUP, axis=1))
    vmem = pl.BlockSpec(memory_space=pltpu.VMEM)
    hbm = pl.BlockSpec(memory_space=pl.ANY)
    return pl.pallas_call(
        kernel,
        out_shape=pltpu.VMEM((OWN, 4096), bf16),
        in_specs=[hbm] * 13,
        out_specs=vmem,
        scratch_shapes=[
            pltpu.VMEM((OWN, 4096), bf16),
            pltpu.VMEM((1, 128), f32),
            pltpu.VMEM((32, GROUP), f32),
            pltpu.VMEM((1, 512), f32),
            pltpu.VMEM((1, 1024), f32),
            pltpu.VMEM((4096, 512), bf16),
            pltpu.VMEM((64, 4096), bf16),
            pltpu.VMEM((4096, 1024), bf16),
            pltpu.VMEM((1024, 512), bf16),
            pltpu.VMEM((1024, 256), bf16),
            pltpu.VMEM((512, 512), bf16),
            pltpu.VMEM((512, 512), bf16),
            pltpu.VMEM((512, 4096), bf16),
            pltpu.VMEM((16, 4, BLOCK, 128), bf16),
            pltpu.VMEM((4, OWN, 1024), bf16),
            pltpu.VMEM((2, HEADS * (NOPE + ROPE), GROUP), bf16),
            pltpu.VMEM((512, 512), bf16),
            pltpu.VMEM((2 * GROUP, 640), bf16),
            pltpu.VMEM((HEADS, VROWS, 2 * GROUP), bf16),
            pltpu.VMEM((HEADS, VROWS, 2 * GROUP), f32),
            pltpu.VMEM((HEADS, 1, 2 * GROUP), f32),
            pltpu.VMEM((HEADS, 256, 2 * GROUP), bf16),
            pltpu.VMEM((2, 2 * GROUP, 2 * GROUP), f32),
            pltpu.VMEM((2, 1, 2 * GROUP), f32),
            pltpu.VMEM((HEADS, VDIM, GROUP), bf16),
            pltpu.VMEM((HEADS, VDIM, GROUP), bf16),
            pltpu.VMEM((HEADS, 8, GROUP), f32),
            pltpu.VMEM((HEADS, 8, GROUP), f32),
            pltpu.VMEM((4, OWN, 4096), bf16),
            pltpu.VMEM((2, 32, 4096), bf16),
            pltpu.VMEM((2, 32, 4096), bf16),
            pltpu.VMEM((2, 32, 4096), bf16),
            pltpu.VMEM((2, 32, 4096), bf16),
            pltpu.SemaphoreType.DMA((19,)),
            pltpu.SemaphoreType.DMA((N_MSG,)),
            pltpu.SemaphoreType.DMA((N_MSG,)),
        ],
        compiler_params=pltpu.CompilerParams(
            collective_id=0, has_side_effects=True, vmem_limit_bytes=62 * 1024 * 1024
        ),
    )(
        tokens,
        down_query,
        down_latent,
        down_rotary.T,
        query_gain.reshape(1, -1),
        latent_gain.reshape(1, -1),
        up_query,
        up_query_rotary,
        up_key,
        up_value,
        out_weight,
        lane_rates,
        row_rates,
    )


def solution(mesh):
    return jax.shard_map(
        local,
        mesh=mesh,
        in_specs=(
            P(("sp", "tp"), None),
            P(),
            P(),
            P(),
            P(),
            P(),
            P(None, "tp"),
            P(None, "tp"),
            P(None, "tp"),
            P(None, "tp"),
            P("tp", None),
        ),
        out_specs=P(("sp", "tp"), None),
        check_vma=False,
    )
```

```python
import functools

import jax
import jax.numpy as jnp
import numpy as np
from jax import lax
from jax.experimental import pallas as pl
from jax.experimental.pallas import tpu as pltpu
from jax.sharding import PartitionSpec as P

NOPE = 128
ROPE = 64
VDIM = 128
HEADS = 4
OWN = 64
GROUP = 256
BLOCK = 288
VROWS = 144
RING = 4

rope_base = 500000.0
norm_eps = 1e-06
masked_score = -1e30

f32 = jnp.float32
bf16 = jnp.bfloat16
MESH = pl.DeviceIdType.MESH

COLS = 4
N_MSG = 103 + 6 * (COLS - 4)

STEPS = 9
UNIT_OA = ((0, 1, 0, 2, 1, -1, 2, 1, 2), (0, -1, 0, 1, -1, 0, 2, -1, 2))
UNIT_OB = ((0, 0, 1, 0, -1, -1, 1, 2, 2), (0, 0, -1, 1, 1, 2, -1, 2, 2))


def pick(index, values):
    out = jnp.int32(values[0])
    for i, v in enumerate(values[1:], 1):
        out = jnp.where(index == i, jnp.int32(v), out)
    return out


def once(condition):
    def run(body):
        def trip(_, carry):
            body()
            return carry

        lax.fori_loop(0, jnp.where(condition, 1, 0), trip, 0)

    return run


def mod4(v):
    return jnp.where(v < 0, v + 4, jnp.where(v > 3, v - 4, v))


def kernel(
    tokens_in,
    down_query,
    down_latent,
    down_rotary,
    query_gain,
    latent_gain,
    up_query,
    up_query_rotary,
    up_key,
    up_value,
    out_weight,
    lane_rates,
    row_rates,
    out,
    tokens,
    lrate,
    rrate,
    lgain,
    qgain,
    wdl,
    wdr,
    wdq,
    wuq,
    wur,
    wuk,
    wuv,
    wout,
    lat,
    ql,
    qt,
    uvt,
    kbuf,
    vbuf,
    acc,
    best,
    qfull,
    sbuf,
    tops,
    xsend,
    xrecv,
    ssend,
    srecv,
    pbuf,
    r1buf,
    dbuf,
    cbuf,
    crecv,
    local_sem,
    ssem,
    rsem,
):
    sp = lax.axis_index("sp")
    x = lax.axis_index("tp")
    c = lax.rem(sp, 2)
    m = sp // 2
    y = lax.rem(m, 4)
    z = m // 4
    first = c == 0
    a = jnp.where(first, y, z)
    b = jnp.where(first, z, y)
    stride_a = jnp.where(first, 2, 8)
    stride_b = jnp.where(first, 8, 2)

    def at(aa, bb):
        return {"sp": aa * stride_a + bb * stride_b + c, "tp": x}

    xp, xm, x2 = mod4(x + 1), mod4(x - 1), mod4(x + 2)
    dev_xp = {"sp": sp, "tp": xp}
    dev_xm = {"sp": sp, "tp": xm}
    dev_ap, dev_am = at(mod4(a + 1), b), at(mod4(a - 1), b)
    dev_bp, dev_bm = at(a, mod4(b + 1)), at(a, mod4(b - 1))
    dev_core = {"sp": sp + 1 - 2 * c, "tp": x}

    copies = []

    def copy_in(src, dst):
        copies.append(pltpu.make_async_copy(src, dst, local_sem.at[len(copies)]))
        copies[-1].start()
        return copies[-1]

    K4 = 1024
    quarters = [pl.ds(k * K4, K4) for k in range(4)]
    load_lanes = copy_in(lane_rates, lrate)
    load_tokens = copy_in(tokens_in, tokens)
    load_latent = [copy_in(down_latent.at[r], wdl.at[r]) for r in quarters]
    load_rotary = copy_in(down_rotary, wdr)
    load_rows = copy_in(row_rates, rrate)
    load_lgain = copy_in(latent_gain, lgain)
    load_qgain = copy_in(query_gain, qgain)
    load_query = [copy_in(down_query.at[r], wdq.at[r]) for r in quarters]
    load_rest = [
        copy_in(up_query, wuq),
        copy_in(up_query_rotary, wur),
        copy_in(up_key, wuk),
        copy_in(up_value, wuv),
        copy_in(out_weight, wout),
    ]

    barrier = pltpu.get_barrier_semaphore()
    for dev in (dev_xp, dev_xm, dev_ap, dev_am, dev_bp, dev_bm, dev_core):
        pl.semaphore_signal(barrier, inc=1, device_id=dev, device_id_type=MESH)

    send, recv = [], []

    def add(src, dst, landed, dev):
        i = len(send)
        for refs, done in ((src, dst), send), ((landed, landed), recv):
            done.append(
                pltpu.make_async_remote_copy(
                    src_ref=refs[0],
                    dst_ref=refs[1],
                    send_sem=ssem.at[i],
                    recv_sem=rsem.at[i],
                    device_id=dev,
                    device_id_type=MESH,
                )
            )
        return i

    def pair(up, up_landed, dev_up, down, down_landed, dev_down):
        return (
            add(lat.at[up], lat.at[up], lat.at[up_landed], dev_up),
            add(lat.at[down], lat.at[down], lat.at[down_landed], dev_down),
        )

    def group(oa, ob):
        return mod4(b + ob) * 4 + mod4(a + oa)

    def xs(o):
        return mod4(x + o)

    OFFS = (0, 1, -1, 2)
    s0 = group(0, 0)
    lo, hi = pl.ds(0, BLOCK // 2), pl.ds(BLOCK // 2, BLOCK // 2)

    def block(oa, ob, o):
        return group(oa, ob), xs(o)

    X1 = [
        pair((s0, x, up), (s0, xm, up), dev_xp, (s0, x, down), (s0, xp, down), dev_xm)
        for up, down in ((lo, hi), (hi, lo))
    ]
    X2 = pair((s0, xm, lo), (s0, x2, lo), dev_xp, (s0, xp, hi), (s0, x2, hi), dev_xm)
    A1, A2, B1, B2 = {}, {}, {}, {}
    for o in OFFS:
        A1[o] = pair(
            block(0, 0, o), block(-1, 0, o), dev_ap, block(0, 0, o), block(1, 0, o), dev_am
        )
        for oa in OFFS:
            B1[oa, o] = pair(
                block(oa, 0, o), block(oa, -1, o), dev_bp, block(oa, 0, o), block(oa, 1, o), dev_bm
            )
    for n, (up, down) in enumerate(((0, 1), (2, -1))):
        A2[n] = pair(
            block(-1, 0, up), block(2, 0, up), dev_ap, block(1, 0, down), block(2, 0, down), dev_am
        )
        for oa in OFFS:
            B2[oa, n] = pair(
                block(oa, -1, up),
                block(oa, 2, up),
                dev_bp,
                block(oa, 1, down),
                block(oa, 2, down),
                dev_bm,
            )
    q_lo, q_hi = pl.ds(0, OWN // 2), pl.ds(OWN // 2, OWN // 2)
    Q1 = [
        (
            add(ql.at[x, up], ql.at[x, up], ql.at[xm, up], dev_xp),
            add(ql.at[x, down], ql.at[x, down], ql.at[xp, down], dev_xm),
        )
        for up, down in ((q_lo, q_hi), (q_hi, q_lo))
    ]
    Q2 = (
        add(ql.at[xm, q_lo], ql.at[xm, q_lo], ql.at[x2, q_lo], dev_xp),
        add(ql.at[xp, q_hi], ql.at[xp, q_hi], ql.at[x2, q_hi], dev_xm),
    )
    QX = []
    for n in range(2):
        half = pl.ds(n * 2 * OWN, 2 * OWN)
        mine = qt.at[c, :, half]
        QX.append((add(mine, mine, qt.at[1 - c, :, half], dev_core),))
    OX = [(add(xsend.at[h], xrecv.at[h], xrecv.at[h], dev_core),) for h in range(HEADS)]
    OS = (add(ssend, srecv, srecv, dev_core),)

    def start(*groups):
        for ids in groups:
            for i in ids:
                send[i].start()

    def arrived(*groups):
        for ids in groups:
            for i in ids:
                recv[i].wait_recv()

    def token_of(col):
        place = col
        for r, o in enumerate(OFFS):
            inside = jnp.logical_and(col >= r * OWN, col < (r + 1) * OWN)
            place = jnp.where(inside, col + (xs(o) - r) * OWN, place)
        return place

    def norm_rows(values, gain):
        return values * lax.rsqrt(jnp.mean(values * values, axis=-1, keepdims=True) + norm_eps) * gain

    load_lanes.wait()
    spot = lax.broadcasted_iota(jnp.int32, (OWN, 128), 0) + (sp * RING + x) * OWN
    angles = spot.astype(f32) * lrate[...]
    lane = lax.broadcasted_iota(jnp.int32, (OWN, 128), 1)
    key_cos = jnp.cos(angles)
    key_sin = jnp.sin(angles) * jnp.where(lax.rem(lane, 64) < 32, -1.0, 1.0)
    load_tokens.wait()
    latent = jnp.zeros((OWN, 512), f32)
    for k in range(4):
        load_latent[k].wait()
        cols = slice(k * K4, (k + 1) * K4)
        latent = latent + jnp.dot(tokens[:, cols], wdl[cols, :], preferred_element_type=f32)
    load_lgain.wait()
    latent = norm_rows(latent, lgain[...]).astype(bf16)
    for t in range(4):
        lat[s0, x, t * OWN : (t + 1) * OWN, :] = latent[:, t * 128 : (t + 1) * 128]
    load_rotary.wait()
    turned = lax.dot_general(
        tokens[...], wdr[...], (((1,), (1,)), ((), ())), preferred_element_type=f32
    )
    turned = jnp.concatenate([turned, turned], axis=-1)
    turned = turned * key_cos + pltpu.roll(turned, 32, 1) * key_sin
    lat[s0, x, 256:288, :] = jnp.where(lane[:32] < 64, turned[:32], turned[32:]).astype(bf16)
    pl.semaphore_wait(barrier, 7)
    start(*X1, A1[0], B1[0, 0])

    query = jnp.zeros((OWN, 1024), f32)
    for k in range(4):
        load_query[k].wait()
        cols = slice(k * K4, (k + 1) * K4)
        query = query + jnp.dot(tokens[:, cols], wdq[cols, :], preferred_element_type=f32)
    load_qgain.wait()
    ql[x] = norm_rows(query, qgain[...]).astype(bf16)
    start(Q1[0])
    arrived(X1[0])
    start(X2, Q1[1])
    arrived(X1[1])
    start(A1[1], A1[-1], B1[0, 1], B1[0, -1])
    load_rows.wait()
    for load in load_rest:
        load.wait()
    uvt[...] = jnp.transpose(wuv[...])
    for h in range(HEADS):
        vbuf[h, VDIM:VROWS, :] = jnp.ones((VROWS - VDIM, 2 * GROUP), bf16)
    acc[...] = jnp.zeros_like(acc)
    best[...] = jnp.full(best.shape, masked_score, f32)
    spot = token_of(lax.broadcasted_iota(jnp.int32, (32, GROUP), 1)) + sp * GROUP
    angles = spot.astype(f32) * rrate[...]
    cosine, sine = jnp.cos(angles), jnp.sin(angles)
    arrived(A1[0])
    start(B1[1, 0], B1[-1, 0])
    arrived(Q1[0])
    start(Q2)
    arrived(A1[1])
    start(A2[0], B1[1, 1], B1[-1, 1])
    arrived(B1[0, 0], B1[0, 1])
    start(B2[0, 0])
    arrived(X2)
    start(A1[2], B1[0, 2])
    arrived(A1[-1])
    start(B1[1, -1], B1[-1, -1])
    factor = (NOPE + ROPE) ** (-0.5) * 1.4426950408889634

    def make_queries(n):
        half = slice(n * 2 * OWN, (n + 1) * 2 * OWN)
        rows = jnp.concatenate([ql[xs(OFFS[2 * n])], ql[xs(OFFS[2 * n + 1])]], axis=0)
        plain = jnp.dot(rows, wuq[...], preferred_element_type=f32) * factor
        qt[c, 0 : HEADS * NOPE, half] = jnp.transpose(plain.astype(bf16))
        turned = jnp.transpose(jnp.dot(rows, wur[...], preferred_element_type=f32) * factor)
        for h in range(HEADS):
            one = turned[h * ROPE : h * ROPE + 32]
            two = turned[h * ROPE + 32 : (h + 1) * ROPE]
            at_row = HEADS * NOPE + h * ROPE
            qt[c, at_row : at_row + 32, half] = (
                one * cosine[:, half] - two * sine[:, half]
            ).astype(bf16)
            qt[c, at_row + 32 : at_row + 64, half] = (
                two * cosine[:, half] + one * sine[:, half]
            ).astype(bf16)
        start(QX[n])

    arrived(Q1[1])
    make_queries(0)
    arrived(Q2)
    make_queries(1)

    def set_of(u, n):
        aa, bb = mod4(a + pick(u, UNIT_OA[n])), mod4(b + pick(u, UNIT_OB[n]))
        spot = jnp.where(first, bb * 4 + aa, aa * 4 + bb)
        seen = spot <= m
        if n == 1:
            seen = jnp.logical_and(seen, jnp.logical_and(u > 0, u < STEPS - 1))
        return bb * 4 + aa, spot, seen

    def attend(sets, spot):
        keys = len(sets) * GROUP
        parts, rots = [], []
        for s in sets:
            tiles = [
                lat[s, :, t * OWN : (t + 1) * OWN, :].reshape(GROUP, 128) for t in range(4)
            ]
            parts.append(jnp.concatenate(tiles, axis=1))
            packed = lat[s, :, 256:288, :]
            swapped = pltpu.roll(packed.reshape(128, 128).astype(f32), 64, 1).astype(bf16)
            rots.append(
                jnp.concatenate([packed, swapped.reshape(4, 32, 128)], axis=1).reshape(GROUP, 128)
            )
        latents = jnp.concatenate(parts, axis=0)
        kbuf[:keys, 0:512] = jnp.dot(latents, wuk[...], preferred_element_type=f32).astype(bf16)
        kbuf[:keys, 512:640] = jnp.concatenate(rots, axis=0)

        def score(h):
            key = jnp.concatenate(
                [kbuf[:keys, h * NOPE : (h + 1) * NOPE], kbuf[:keys, 512:640]], axis=1
            )
            scores = jnp.dot(key, qfull[h], preferred_element_type=f32)
            if spot is not None:
                row = lax.broadcasted_iota(jnp.int32, (keys, 2 * GROUP), 0)
                col = lax.broadcasted_iota(jnp.int32, (1, 2 * GROUP), 1)
                col = jnp.where(col < GROUP, token_of(col), token_of(col - GROUP) + GROUP)
                ahead = (2 * (spot - m) + c) * GROUP
                scores = jnp.where(row <= col - ahead, scores, masked_score)
            sbuf[h % 2, :keys] = scores
            tops[h % 2] = jnp.max(scores, axis=0, keepdims=True)

        score(0)
        values = lax.dot_general(
            uvt[...], latents, (((1,), (1,)), ((), ())), preferred_element_type=f32
        ).astype(bf16)
        for h in range(HEADS):
            vbuf[h, 0:VDIM, :keys] = values[h * VDIM : (h + 1) * VDIM]
        for h in range(HEADS):
            if h + 1 < HEADS:
                score(h + 1)
            old = best[h]
            new = jnp.maximum(old, tops[h % 2])
            weights = jnp.exp2(sbuf[h % 2, :keys] - new).astype(bf16)
            best[h] = new
            acc[h] = acc[h] * jnp.exp2(old - new) + jnp.dot(
                vbuf[h, :, :keys], weights, preferred_element_type=f32
            )

    def pass_second():
        arrived(A2[0])
        start(B1[2, 0], B1[2, 1])
        arrived(B1[1, 0], B1[1, 1])
        start(B2[1, 0])

    once(jnp.logical_not(first))(pass_second)

    arrived(*QX)
    for h in range(HEADS):
        for j in range(2):
            cols = slice(j * GROUP, (j + 1) * GROUP)
            qfull[h, 0:NOPE, cols] = qt[j, h * NOPE : (h + 1) * NOPE, :]
            at_row = HEADS * NOPE + h * ROPE
            qfull[h, NOPE : NOPE + ROPE, cols] = qt[j, at_row : at_row + ROPE, :]
        qfull[h, NOPE + ROPE :, :] = jnp.zeros((ROPE, 2 * GROUP), bf16)

    def far_seen(oa):
        aa, bb = mod4(a + oa), mod4(b + 2)
        return jnp.where(first, bb * 4 + aa, aa * 4 + bb) <= m

    def step(u, carry):

        @once(u == 1)
        def _():
            arrived(A1[2])
            start(A2[1], B1[1, 2], B1[-1, 2])
            once(first)(pass_second)
            arrived(B1[-1, 0], B1[-1, 1])
            start(B2[-1, 0])

        @once(u == 2)
        def _():
            arrived(B1[0, -1], B1[0, 2])
            start(B2[0, 1])

        @once(u == 3)
        def _():
            arrived(A2[1])
            start(B1[2, -1], B1[2, 2])
            arrived(B1[1, -1], B1[1, 2])
            start(B2[1, 1])

        @once(u == 4)
        def _():
            arrived(B1[2, 0], B1[2, 1])
            start(B2[2, 0])
            arrived(B1[-1, -1], B1[-1, 2])
            start(B2[-1, 1])

        @once(u == 6)
        def _():
            arrived(B1[2, -1], B1[2, 2])
            start(B2[2, 1])

        for oa, when in ((0, 5), (1, 7), (-1, 7), (2, 8)):

            @once(jnp.logical_and(u == when, far_seen(oa)))
            def _(oa=oa):
                arrived(B2[oa, 0], B2[oa, 1])

        set_one, spot_one, seen_one = set_of(u, 0)
        set_two, spot_two, seen_two = set_of(u, 1)
        two = jnp.logical_and(seen_one, seen_two)
        one = jnp.logical_and(jnp.logical_or(seen_one, seen_two), jnp.logical_not(two))
        single = jnp.where(seen_one, set_one, set_two)
        spot = jnp.where(seen_one, spot_one, spot_two)

        @pl.when(two)
        def _():
            attend((set_one, set_two), None)

        @pl.when(one)
        def _():
            attend((single,), spot)

        return carry

    lax.fori_loop(0, STEPS, step, 0)

    mine_at = pl.ds(pl.multiple_of(c * GROUP, GROUP), GROUP)
    other_at = pl.ds(pl.multiple_of((1 - c) * GROUP, GROUP), GROUP)
    for h in range(HEADS):
        ssend[h, 0:1, :] = best[h, :, other_at]
        ssend[h, 1:2, :] = acc[h, 128:129, other_at]
    start(OS)
    for h in range(HEADS):
        xsend[h] = acc[h, 0:128, other_at].astype(bf16)
        start(OX[h])
    arrived(OS)
    heads = []
    for h in range(HEADS):
        mine, theirs = best[h, :, mine_at], srecv[h, 0:1, :]
        top = jnp.maximum(mine, theirs)
        w_mine, w_theirs = jnp.exp2(mine - top), jnp.exp2(theirs - top)
        total = acc[h, 128:129, mine_at] * w_mine + srecv[h, 1:2, :] * w_theirs
        arrived(OX[h])
        summed = acc[h, 0:128, mine_at] * w_mine + xrecv[h].astype(f32) * w_theirs
        heads.append(jnp.transpose((summed * (1.0 / total)).astype(bf16)))
    attended = jnp.concatenate(heads, axis=1)

    WIDE = 4096 // COLS
    top, low = pl.ds(0, 32), pl.ds(32, 32)
    R1, RD, RC = [], [], []
    for k in range(COLS):
        cols = pl.ds(k * WIDE, WIDE)

        def both(to_up, to_down, ref):
            up, down = ref.at[0, :, cols], ref.at[1, :, cols]
            return add(to_up, up, up, dev_xp), add(to_down, down, down, dev_xm)

        R1.append(both(pbuf.at[3, top, cols], pbuf.at[3, low, cols], r1buf))
        RD.append(both(pbuf.at[1, low, cols], pbuf.at[2, top, cols], dbuf))
        RC.append(both(cbuf.at[0, :, cols], cbuf.at[1, :, cols], crecv))
    assert len(send) == N_MSG, len(send)
    for k in range(COLS):
        cols = slice(k * WIDE, (k + 1) * WIDE)
        part = jnp.dot(attended, wout[:, cols], preferred_element_type=f32).astype(bf16)
        pbuf[:, :, cols] = part.reshape(4, OWN, WIDE)
        start(R1[k])
    start(*RD)
    for k in range(COLS):
        cols = slice(k * WIDE, (k + 1) * WIDE)
        arrived(R1[k])
        cbuf[0, :, cols] = (
            r1buf[0, :, cols].astype(f32) + pbuf[1, 0:32, cols].astype(f32)
        ).astype(bf16)
        cbuf[1, :, cols] = (
            r1buf[1, :, cols].astype(f32) + pbuf[2, 32:64, cols].astype(f32)
        ).astype(bf16)
        start(RC[k])
    for oa in OFFS:

        @pl.when(jnp.logical_not(far_seen(oa)))
        def _(oa=oa):
            arrived(B2[oa, 0], B2[oa, 1])

    tail = [i for ids in (*RD, *RC) for i in ids]
    for i in range(N_MSG):
        if i not in tail:
            send[i].wait_send()

    for k in range(COLS):
        cols = slice(k * WIDE, (k + 1) * WIDE)
        arrived(RD[k], RC[k])
        out[0:32, cols] = (
            pbuf[0, 0:32, cols].astype(f32)
            + crecv[0, :, cols].astype(f32)
            + dbuf[1, :, cols].astype(f32)
        ).astype(bf16)
        out[32:64, cols] = (
            pbuf[0, 32:64, cols].astype(f32)
            + crecv[1, :, cols].astype(f32)
            + dbuf[0, :, cols].astype(f32)
        ).astype(bf16)
    for i in tail:
        send[i].wait_send()


def local(
    tokens,
    down_query,
    down_latent,
    down_rotary,
    query_gain,
    latent_gain,
    up_query,
    up_query_rotary,
    up_key,
    up_value,
    out_weight,
):
    rates = (rope_base ** (-np.arange(0, ROPE, 2) / ROPE)).astype(np.float32)
    lane_rates = jnp.asarray(np.tile(rates, 4)[None, :])
    row_rates = jnp.asarray(np.repeat(rates[:, None], GROUP, axis=1))
    vmem = pl.BlockSpec(memory_space=pltpu.VMEM)
    hbm = pl.BlockSpec(memory_space=pl.ANY)
    return pl.pallas_call(
        kernel,
        out_shape=pltpu.VMEM((OWN, 4096), bf16),
        in_specs=[hbm] * 13,
        out_specs=vmem,
        scratch_shapes=[
            pltpu.VMEM((OWN, 4096), bf16),
            pltpu.VMEM((1, 128), f32),
            pltpu.VMEM((32, GROUP), f32),
            pltpu.VMEM((1, 512), f32),
            pltpu.VMEM((1, 1024), f32),
            pltpu.VMEM((4096, 512), bf16),
            pltpu.VMEM((64, 4096), bf16),
            pltpu.VMEM((4096, 1024), bf16),
            pltpu.VMEM((1024, 512), bf16),
            pltpu.VMEM((1024, 256), bf16),
            pltpu.VMEM((512, 512), bf16),
            pltpu.VMEM((512, 512), bf16),
            pltpu.VMEM((512, 4096), bf16),
            pltpu.VMEM((16, 4, BLOCK, 128), bf16),
            pltpu.VMEM((4, OWN, 1024), bf16),
            pltpu.VMEM((2, HEADS * (NOPE + ROPE), GROUP), bf16),
            pltpu.VMEM((512, 512), bf16),
            pltpu.VMEM((2 * GROUP, 640), bf16),
            pltpu.VMEM((HEADS, VROWS, 2 * GROUP), bf16),
            pltpu.VMEM((HEADS, VROWS, 2 * GROUP), f32),
            pltpu.VMEM((HEADS, 1, 2 * GROUP), f32),
            pltpu.VMEM((HEADS, 256, 2 * GROUP), bf16),
            pltpu.VMEM((2, 2 * GROUP, 2 * GROUP), f32),
            pltpu.VMEM((2, 1, 2 * GROUP), f32),
            pltpu.VMEM((HEADS, VDIM, GROUP), bf16),
            pltpu.VMEM((HEADS, VDIM, GROUP), bf16),
            pltpu.VMEM((HEADS, 8, GROUP), f32),
            pltpu.VMEM((HEADS, 8, GROUP), f32),
            pltpu.VMEM((4, OWN, 4096), bf16),
            pltpu.VMEM((2, 32, 4096), bf16),
            pltpu.VMEM((2, 32, 4096), bf16),
            pltpu.VMEM((2, 32, 4096), bf16),
            pltpu.VMEM((2, 32, 4096), bf16),
            pltpu.SemaphoreType.DMA((19,)),
            pltpu.SemaphoreType.DMA((N_MSG,)),
            pltpu.SemaphoreType.DMA((N_MSG,)),
        ],
        compiler_params=pltpu.CompilerParams(
            collective_id=0, has_side_effects=True, vmem_limit_bytes=62 * 1024 * 1024
        ),
    )(
        tokens,
        down_query,
        down_latent,
        down_rotary.T,
        query_gain.reshape(1, -1),
        latent_gain.reshape(1, -1),
        up_query,
        up_query_rotary,
        up_key,
        up_value,
        out_weight,
        lane_rates,
        row_rates,
    )


def solution(mesh):
    return jax.shard_map(
        local,
        mesh=mesh,
        in_specs=(
            P(("sp", "tp"), None),
            P(),
            P(),
            P(),
            P(),
            P(),
            P(None, "tp"),
            P(None, "tp"),
            P(None, "tp"),
            P(None, "tp"),
            P("tp", None),
        ),
        out_specs=P(("sp", "tp"), None),
        check_vma=False,
    )
```
